32 devices in a mesh: grp: 2 (over y), sp: 4 (over z), tp: 4 (over x, core).
Axes of the slice: x: 2, y: 2, z: 4, core: 2. Of those that a mesh axis runs over, the one named last changes fastest.
Arguments:
- residual_in: bfloat16 [2048, 2048], P(('grp', 'sp', 'tp')), parts along dimension 0, may hold values from -1.1953125 to 1.1953125
- query_small: bfloat16 [2048, 1024], P(('grp', 'sp'), 'tp'), parts along dimension 0, may hold values from -6 to 6
- query_large: bfloat16 [2048, 1024], P(('grp', 'sp'), 'tp'), parts along dimension 0, may hold values from -6 to 6
- key_small: bfloat16 [64, 2048], P(None, ('grp', 'sp')), parts along dimension 1, may hold values from -6 to 6
- key_large: bfloat16 [128, 2048], P(None, ('grp', 'sp')), parts along dimension 1, may hold values from -6 to 6
- value_small: bfloat16 [64, 2048], P(None, ('grp', 'sp')), parts along dimension 1, may hold values from -6 to 6
- value_large: bfloat16 [128, 2048], P(None, ('grp', 'sp')), parts along dimension 1, may hold values from -6 to 6
- forget_small: float32 [16, 2048], P('tp', ('grp', 'sp')), parts along dimension 1, may hold values from -148 to 0, as said below
- forget_large: float32 [8, 2048], P('tp', ('grp', 'sp')), parts along dimension 1, may hold values from -148 to 0, as said below
- project_small: bfloat16 [1024, 2048], P('tp'), may hold values from -0.125 to 0.125
- project_large: bfloat16 [1024, 2048], P('tp'), may hold values from -0.125 to 0.125
- norm_gain: bfloat16 [2048], replicated, may hold values from 0.099609375 to 1.8984375
- expert_gate: bfloat16 [16, 2048, 512], P(('sp', 'tp')), may hold values from -0.125 to 0.125
- expert_up: bfloat16 [16, 2048, 512], P(('sp', 'tp')), may hold values from -0.125 to 0.125
- expert_down: bfloat16 [16, 512, 2048], P(('sp', 'tp')), may hold values from -0.25 to 0.25
- routing: int32 [2048, 2], P(('grp', 'sp', 'tp')), parts along dimension 0, may hold values from 0 to 15, all different within a row; in each aligned block of 64 rows (0 to 63, 64 to 127, ...) at most 16 rows name the same one
- route_weight: float32 [2048, 2], P(('grp', 'sp', 'tp')), parts along dimension 0, may hold values from 0.2 to 1
Outputs:
- layer_out: bfloat16 [2048, 2048], P(('grp', 'sp', 'tp')), parts along dimension 0
The draws below stay inside these ranges and needn't reach their ends.
There are 2 independent parts, one for each index of `grp`. The reference program is written for one: setup_inputs(seed, part) draws one part's arguments, and reference() takes and returns one part's arrays. A program takes and returns all parts, laid end to end along the dimension named above; an argument that names none is the same for every part. Nothing has to cross between parts.
Inputs may be any that keep to these rules, and one draw needn't show every extreme that they name: `forget_small`: each row never rises from one position to the next. `forget_large`: each row never rises from one position to the next. `routing`: each row names 2 different experts; in the rows of one device no expert is named by more than 16 rows, and in some devices' rows some expert is named by exactly 16.
All inputs are finite; a program needn't handle non-finite values.
Results may differ from the reference program's by a relative error of at most 0.018.
Values may be sent and summed in bfloat16 or wider, within the bound.
A program may use at most 64 MiB of HBM per device.

```python
import math
import jax
import jax.numpy as jnp
import numpy as np
from jax import lax

D = 2048
HS_N = 16
DHS = 64
HL_N = 8
DHL = 128
FF = 512
TOP = 2
TOK_DEV = 256
SEQUENCE_TOKENS = 1024
ROWS = 64
EXPERTS = 16
CAP = 16
N_TP = 4


def query_draw(key, salt, number_heads, head_size):
    drawn = 1.5 * jax.random.truncated_normal(jax.random.fold_in(key, salt), -4.0, 4.0, (SEQUENCE_TOKENS, number_heads * head_size), jnp.float32)
    return drawn


def key_draw(key, salt, head_size):
    drawn = 1.5 * jax.random.truncated_normal(jax.random.fold_in(key, salt), -4.0, 4.0, (head_size, SEQUENCE_TOKENS), jnp.float32)
    return drawn


def gate_draw(key, salt, number_heads):
    root_random_key = jax.random.fold_in(key, salt)
    fast_share = 0.5
    is_fast = jax.random.uniform(jax.random.fold_in(root_random_key, 1), (number_heads,)) < fast_share
    slow_total = jnp.exp(jax.random.uniform(jax.random.fold_in(root_random_key, 2), (number_heads,), jnp.float32, math.log(0.3), math.log(0.8)))
    fast_rate = jnp.exp(-jax.random.uniform(jax.random.fold_in(root_random_key, 3), (number_heads,), jnp.float32, math.log(30.0), math.log(100.0)))
    rate = jnp.where(is_fast, fast_rate, slow_total / SEQUENCE_TOKENS)
    block_count = SEQUENCE_TOKENS // TOK_DEV
    block_factor = jnp.exp(jax.random.uniform(jax.random.fold_in(root_random_key, 4), (number_heads, block_count), jnp.float32, math.log(0.35), math.log(2.8)))
    block_factor = jnp.repeat(block_factor, TOK_DEV, axis=1)
    rough = jax.random.uniform(jax.random.fold_in(root_random_key, 5), (number_heads, SEQUENCE_TOKENS), jnp.float32, 0.5, 1.5)
    logarithm_gate = -rate[:, None] * block_factor * rough
    spike_position = jax.random.randint(jax.random.fold_in(root_random_key, 6), (number_heads, 2), 0, SEQUENCE_TOKENS)
    spike_penalty = -jnp.log(1.0 - jax.random.uniform(jax.random.fold_in(root_random_key, 7), (number_heads, 2), jnp.float32, 0.2, 0.4))
    per_head_rows = jnp.broadcast_to(jnp.arange(number_heads)[:, None], (number_heads, 2))
    logarithm_gate = logarithm_gate.at[per_head_rows, spike_position].add(-spike_penalty)
    return jnp.cumsum(logarithm_gate, axis=1)


def draw_query_small(key, part):
    return query_draw(key, 11, HS_N, DHS).astype(jnp.bfloat16)


def draw_query_large(key, part):
    return query_draw(key, 12, HL_N, DHL).astype(jnp.bfloat16)


def draw_key_small(key, part):
    return key_draw(key, 13, DHS).astype(jnp.bfloat16)


def draw_key_large(key, part):
    return key_draw(key, 14, DHL).astype(jnp.bfloat16)


def draw_forget_small(key, part):
    return gate_draw(key, 15, HS_N)


def draw_forget_large(key, part):
    return gate_draw(key, 16, HL_N)


def block_levels(rng, shape, pieces, low, largest):
    def one(dim, parts):
        heights = jax.random.uniform(jax.random.fold_in(jax.random.fold_in(rng, 6), dim), (parts,), jnp.float32, low / len(pieces), largest / len(pieces))
        return jnp.repeat(jnp.exp(heights), shape[dim] // parts).reshape((-1,) + (1,) * (len(shape) - dim - 1))

    factor_of = one(*pieces[0])
    for cut in pieces[1:]:
        factor_of = factor_of * one(*cut)
    return factor_of


def assign_block(rng, own, number, rows, number_of, top, bound, skew):
    order = jax.random.permutation(rng, number_of)
    packed, ordinary = shares(number_of, rows * top, bound, skew, True), shares(number_of, rows * top, bound, skew, False)
    places = jnp.arange(number_of)

    def named(sizes, rotation):
        used = int((sizes > 0).sum())
        fixed = max(1, used // 4)
        shifted = fixed + (places - fixed + rotation * (used - fixed)) % max(1, number_of - fixed)
        return jnp.zeros((number_of,), jnp.int32).at[order[jnp.where(places < fixed, places, shifted)]].set(jnp.asarray(sizes, jnp.int32))

    sizes = jnp.where(number % 4 == 0, named(packed, number // 4), named(ordinary, number - number // 4 - 1))
    mixed = jax.random.permutation(jax.random.fold_in(own, 3), number_of)
    giver, taker = mixed[0:number_of // 2 * 2:2], mixed[1:number_of // 2 * 2:2]
    room = jnp.minimum(sizes[giver] - 1, bound - sizes[taker]) // 2
    room = jnp.where((giver == order[0]) | (taker == order[0]) | (sizes[taker] == 0), 0, jnp.maximum(room, 0))
    shifted = jax.random.randint(jax.random.fold_in(own, 4), (number_of // 2,), 0, 1 << 20) % (room + 1)
    sizes = sizes.at[giver].add(-shifted).at[taker].add(shifted)
    labels = jnp.searchsorted(jnp.cumsum(sizes), jnp.arange(rows * top), side="right").astype(jnp.int32)
    grid = labels.reshape(top, rows).T
    grid = grid[jax.random.permutation(jax.random.fold_in(own, 1), rows)]
    rotation = jax.random.randint(jax.random.fold_in(own, 2), (rows, 1), 0, top)
    return jnp.take_along_axis(grid, (jnp.arange(top)[None, :] + rotation) % top, axis=1)


def shares(amount, total, bound, slope, full):
    portions = [(1 << 20) // math.isqrt(rank ** slope) + 1 for rank in range(1, amount + 1)]
    largest = bound if full else min(bound, max(-(-total // amount), total * portions[0] // sum(portions)))
    least = 1 if total - largest >= amount - 1 else 0
    holding, surplus = [largest] + [least] * (amount - 1), total - largest - least * (amount - 1)
    while surplus > 0:
        candidates = [i for i in range(1, amount) if holding[i] < largest] or [i for i in range(1, amount) if holding[i] < bound]
        mass, budget = sum([portions[i] for i in candidates]), surplus
        for i in candidates:
            extra = min(bound - holding[i], max(1, budget * portions[i] // mass), surplus)
            holding[i] = holding[i] + extra
            surplus = surplus - extra
    return np.array(holding)


def gaussian(key, extent, spread, limit, pieces=(), kind=jnp.bfloat16):
    level = block_levels(key, extent, pieces, -0.22, 0.18) if pieces else 1.0
    values = jax.random.normal(key, extent, jnp.float32) * spread * level
    return jnp.minimum(jnp.maximum(values, -limit), limit).astype(kind)


def setup_inputs(seed: int = 0, part: int = 0) -> dict:
    seeds = jax.random.split(jax.random.key(seed), 18)
    own_keys = jax.random.split(jax.random.fold_in(seeds[17], part), 18)
    residual_in = gaussian(own_keys[0], (SEQUENCE_TOKENS, D), 0.2, 1.1953125, ((0, 16),))
    query_small = draw_query_small(jax.random.fold_in(jax.random.fold_in(seeds[17], part), 71), part)
    query_large = draw_query_large(jax.random.fold_in(jax.random.fold_in(seeds[17], part), 71), part)
    key_small = draw_key_small(jax.random.fold_in(jax.random.fold_in(seeds[17], part), 71), part)
    key_large = draw_key_large(jax.random.fold_in(jax.random.fold_in(seeds[17], part), 71), part)
    value_small = gaussian(own_keys[5], (DHS, SEQUENCE_TOKENS), 1.0, 6.0, ((1, 4),))
    value_large = gaussian(own_keys[6], (DHL, SEQUENCE_TOKENS), 1.0, 6.0, ((1, 4),))
    forget_small = draw_forget_small(jax.random.fold_in(jax.random.fold_in(seeds[17], part), 71), part)
    forget_large = draw_forget_large(jax.random.fold_in(jax.random.fold_in(seeds[17], part), 71), part)
    project_small = gaussian(seeds[9], (HS_N * DHS, D), (HS_N * DHS + HL_N * DHL) ** -0.5, 0.125, ((0, 4),))
    project_large = gaussian(seeds[10], (HL_N * DHL, D), (HS_N * DHS + HL_N * DHL) ** -0.5, 0.125, ((0, 4),))
    norm_gain = jnp.clip(1.0 + 0.18 * jax.random.normal(seeds[11], (D,), jnp.float32), 0.099609375, 1.8984375).astype(jnp.bfloat16)
    expert_gate = gaussian(seeds[12], (EXPERTS, D, FF), D ** -0.5, 0.125, ((0, 16),))
    expert_up = gaussian(seeds[13], (EXPERTS, D, FF), D ** -0.5, 0.125, ((0, 16),))
    expert_down = gaussian(seeds[14], (EXPERTS, FF, D), FF ** -0.5, 0.25, ((0, 16),))
    routing_keys = jax.random.split(jax.random.fold_in(own_keys[15], 1), SEQUENCE_TOKENS // ROWS)
    routing_turns = jax.random.permutation(jax.random.fold_in(own_keys[15], 3), SEQUENCE_TOKENS // ROWS)
    routing = jax.vmap(lambda own, number: assign_block(jax.random.fold_in(own_keys[15], 2), own, number, ROWS, EXPERTS, TOP, CAP, 2))(routing_keys, routing_turns).reshape((SEQUENCE_TOKENS, TOP))
    route_weight = jnp.clip(0.2 + 0.8 * jax.random.uniform(own_keys[16], (SEQUENCE_TOKENS, TOP), jnp.float32) ** block_levels(own_keys[16], (SEQUENCE_TOKENS, TOP), ((0, 16),), -0.2, 0.2), 0.2, 1.0)
    return dict(residual_in=residual_in, query_small=query_small, query_large=query_large, key_small=key_small, key_large=key_large, value_small=value_small, value_large=value_large, forget_small=forget_small, forget_large=forget_large, project_small=project_small, project_large=project_large, norm_gain=norm_gain, expert_gate=expert_gate, expert_up=expert_up, expert_down=expert_down, routing=routing, route_weight=route_weight)


def attend(queries, keys_in, values_in, gates_in):
    number_heads = gates_in.shape[0]
    head_size = keys_in.shape[0]
    length = keys_in.shape[1]
    block_len = 512 if length % 512 == 0 else length
    results = []
    for block_index in range(length // block_len):
        first_row = block_index * block_len
        last_row = first_row + block_len
        query_rows = queries[first_row:last_row].reshape(block_len, number_heads, head_size).astype(jnp.float32)
        key_rows = keys_in[:, :last_row].astype(jnp.float32)
        value_rows = values_in[:, :last_row].astype(jnp.float32)
        scores = jnp.einsum('qhd,dk->hqk', query_rows, key_rows) * head_size ** (-0.5)
        scores = scores + gates_in[:, first_row:last_row, None] - gates_in[:, None, :last_row]
        causal = (jnp.arange(first_row, last_row)[:, None] >= jnp.arange(last_row)[None, :])[None]
        scores = jnp.where(causal, scores, -jnp.inf)
        row_top = lax.optimization_barrier(jnp.max(scores, axis=2, keepdims=True))
        weights = jnp.exp(scores - row_top)
        row_total = lax.optimization_barrier(jnp.sum(weights, axis=2))
        rounded = lax.optimization_barrier(weights.astype(jnp.bfloat16)).astype(jnp.float32)
        mixed = jnp.einsum('hqk,dk->qhd', rounded, value_rows) / row_total.T[:, :, None]
        results.append(mixed.reshape(block_len, number_heads * head_size).astype(jnp.bfloat16))
    return jnp.concatenate(results, axis=0)

def reference(residual_in, query_small, query_large, key_small, key_large, value_small, value_large, forget_small, forget_large, project_small, project_large, norm_gain, expert_gate, expert_up, expert_down, routing, route_weight):
    attn_small = attend(query_small, key_small, value_small, forget_small)
    attn_large = attend(query_large, key_large, value_large, forget_large)
    width_small = attn_small.shape[1] // N_TP
    width_large = attn_large.shape[1] // N_TP
    projected = jnp.zeros((SEQUENCE_TOKENS, D), jnp.float32)
    for member in range(N_TP):
        part_small = attn_small[:, member * width_small:(member + 1) * width_small]
        part_large = attn_large[:, member * width_large:(member + 1) * width_large]
        partial_value = jnp.dot(part_small, project_small[member * width_small:(member + 1) * width_small], preferred_element_type=jnp.float32)
        partial_value = partial_value + jnp.dot(part_large, project_large[member * width_large:(member + 1) * width_large], preferred_element_type=jnp.float32)
        projected = projected + lax.optimization_barrier(partial_value.astype(jnp.bfloat16)).astype(jnp.float32)
    resid = residual_in.astype(jnp.float32) + projected
    scale = lax.rsqrt(lax.optimization_barrier(jnp.mean(resid * resid, axis=1, keepdims=True)) + 1e-06)
    normed = (resid * scale * norm_gain.astype(jnp.float32)).astype(jnp.bfloat16)
    flat_route = routing.reshape(-1)
    flat_weight = route_weight.reshape(-1)
    per_expert = SEQUENCE_TOKENS // ROWS * CAP

    def one_expert(running, inputs):
        expert_id, weight_gate, weight_up, weight_down = inputs
        matches = flat_route == expert_id
        chosen = jnp.nonzero(matches, size=per_expert, fill_value=0)[0].astype(jnp.int32)
        valid = jnp.arange(per_expert) < jnp.sum(matches.astype(jnp.int32))
        token_ids = (chosen // TOP).astype(jnp.int32)
        rows_in = normed[token_ids]
        gate_part = jnp.dot(rows_in, weight_gate, preferred_element_type=jnp.float32)
        up_part = jnp.dot(rows_in, weight_up, preferred_element_type=jnp.float32)
        hidden = (jax.nn.silu(gate_part) * up_part).astype(jnp.bfloat16)
        result = jnp.dot(hidden, weight_down, preferred_element_type=jnp.float32).astype(jnp.bfloat16)
        factor = jnp.where(valid, flat_weight[chosen], jnp.zeros((), flat_weight.dtype))
        update = lax.optimization_barrier(result).astype(jnp.float32) * factor[:, None]
        return (running.at[token_ids].add(update), None)
    moe_sum, _ = lax.scan(one_expert, jnp.zeros((SEQUENCE_TOKENS, D), jnp.float32), (jnp.arange(EXPERTS, dtype=jnp.int32), expert_gate, expert_up, expert_down))
    return (resid + moe_sum).astype(jnp.bfloat16)
```

```python
import functools
import math

import jax
import jax.numpy as jnp
from jax import lax
from jax.experimental import pallas as pl
from jax.experimental.pallas import tpu as pltpu
from jax.sharding import PartitionSpec as P

MESH = pl.DeviceIdType.MESH
F32 = jnp.float32
BF16 = jnp.bfloat16


def layer_kernel(
    dims,
    residual_in,
    query_small,
    query_large,
    key_small,
    key_large,
    value_small,
    value_large,
    forget_small,
    forget_large,
    norm_gain,
    routing,
    route_weight,
    project_small,
    project_large,
    expert_gate,
    expert_up,
    expert_down,
    out,
    kv,
    gates,
    turned_q_small,
    turned_q_large,
    top_ref,
    total_ref,
    acc_small,
    acc_large,
    attn_t,
    attn,
    proj_w,
    gate_w,
    up_w,
    down_w,
    proj_f32,
    pair_out,
    pair_in,
    cross_out,
    cross_in,
    resid_ref,
    pick_ref,
    outgoing,
    arrived,
    scale_out,
    scale_in,
    result,
    returned,
    weight_sem,
    kv_send,
    kv_recv,
    gate_send,
    gate_recv,
    fwd_send,
    fwd_recv,
    pair_send,
    pair_recv,
    cross_send,
    cross_recv,
    disp_send,
    disp_recv,
    back_send,
    back_recv,
):
    n_sp, n_tp, cap, col_len = dims
    experts = n_sp * n_tp
    seq = lax.axis_index("sp")
    ten = lax.axis_index("tp")
    me = seq * n_tp + ten
    parity = lax.rem(ten, 2)
    partner = ten + 1 - 2 * parity
    tokens = query_small.shape[0]
    size_small, size_large = key_small.shape[0], key_large.shape[0]
    heads_small, heads_large = forget_small.shape[0], forget_large.shape[0]
    width_small = heads_small * size_small
    rows, width = residual_in.shape
    half_small, half_large = size_small // 2, size_large // 2
    cols = width // col_len
    half_groups = n_tp // 2

    loads = [
        pltpu.make_async_copy(project_small, proj_w.at[pl.ds(0, width_small)], weight_sem.at[0]),
        pltpu.make_async_copy(
            project_large,
            proj_w.at[pl.ds(width_small, heads_large * size_large)],
            weight_sem.at[1],
        ),
        pltpu.make_async_copy(expert_gate.at[0], gate_w, weight_sem.at[2]),
        pltpu.make_async_copy(expert_up.at[0], up_w, weight_sem.at[3]),
        pltpu.make_async_copy(expert_down.at[0], down_w, weight_sem.at[4]),
    ]
    for load in loads:
        load.start()

    barrier = pltpu.get_barrier_semaphore()

    def greet(i, carry):
        peer = lax.rem(me + i, experts)
        pl.semaphore_signal(
            barrier,
            inc=1,
            device_id={"sp": lax.div(peer, n_tp), "tp": lax.rem(peer, n_tp)},
            device_id_type=MESH,
        )
        return carry

    lax.fori_loop(1, experts, greet, 0)

    for half in range(2):
        base = 0
        for source, piece in (
            (key_small, half_small),
            (key_large, half_large),
            (value_small, half_small),
            (value_large, half_large),
        ):
            kv[seq, half, base : base + piece, :] = source[half * piece : (half + 1) * piece, :]
            base += piece
    gates[seq, :heads_small, :] = forget_small[...]
    gates[seq, heads_small : heads_small + heads_large, :] = forget_large[...]
    gate_rows = gates.shape[1]
    if gate_rows > heads_small + heads_large:
        gates[seq, heads_small + heads_large :, :] = jnp.zeros(
            (gate_rows - heads_small - heads_large, tokens), F32
        )

    pl.semaphore_wait(barrier, experts - 1)

    def kv_copy(source, target, slot):
        return pltpu.make_async_remote_copy(
            src_ref=kv.at[source, parity],
            dst_ref=kv.at[source, parity],
            send_sem=kv_send.at[slot],
            recv_sem=kv_recv.at[source],
            device_id={"sp": target, "tp": ten},
            device_id_type=MESH,
        )

    def gate_copy(source, target, slot):
        return pltpu.make_async_remote_copy(
            src_ref=gates.at[source],
            dst_ref=gates.at[source],
            send_sem=gate_send.at[slot],
            recv_sem=gate_recv.at[source],
            device_id={"sp": target, "tp": ten},
            device_id_type=MESH,
        )

    def fwd_copy(source, half):
        return pltpu.make_async_remote_copy(
            src_ref=kv.at[source, half],
            dst_ref=kv.at[source, half],
            send_sem=fwd_send.at[source],
            recv_sem=fwd_recv.at[source],
            device_id={"sp": seq, "tp": partner},
            device_id_type=MESH,
        )

    def send_kv(target, carry):
        gate_copy(seq, target, target).start()
        kv_copy(seq, target, target).start()
        return carry

    lax.fori_loop(seq + 1, n_sp, send_kv, 0)

    lanes = lax.broadcasted_iota(jnp.int32, (rows, experts), 1)
    same = lax.broadcasted_iota(jnp.int32, (rows, rows), 0) == lax.broadcasted_iota(
        jnp.int32, (rows, rows), 1
    )

    def column(ref, k):
        return jnp.sum(
            jnp.where(same, ref[k : k + 1, :].astype(F32), 0.0), axis=1, keepdims=True
        )

    top_count = routing.shape[0]
    routes = [column(routing, k) for k in range(top_count)]
    hot = [(routes[k] == lanes.astype(F32)).astype(F32) for k in range(top_count)]
    named = sum(hot).astype(BF16)
    below = (
        lax.broadcasted_iota(jnp.int32, (rows, rows), 0)
        > lax.broadcasted_iota(jnp.int32, (rows, rows), 1)
    ).astype(F32)
    earlier = jnp.dot(below.astype(BF16), named, preferred_element_type=F32)
    places = lax.broadcasted_iota(jnp.int32, (rows, experts * cap), 1).astype(F32)
    for k in range(top_count):
        slot = jnp.sum(earlier * hot[k], axis=1, keepdims=True)
        place = routes[k] * cap + slot
        pick_ref[k * rows : (k + 1) * rows, :] = (places == place).astype(F32).astype(BF16)

    extra_rows = turned_q_small.shape[1] - size_small

    def fold(size):
        power = 2.0 ** math.floor(math.log2(size**-0.5))
        return power, size**-0.5 / power

    extra_row = lax.broadcasted_iota(jnp.int32, (extra_rows, tokens), 0)
    for kind in range(2):
        heads, size, offset, source, q_ref = (
            (heads_small, size_small, 0, query_small, turned_q_small),
            (heads_large, size_large, heads_small, query_large, turned_q_large),
        )[kind]
        turned = (source[...] * fold(size)[0]).astype(BF16).T
        for h in range(heads):
            chosen = (lax.rem(extra_row, gate_rows) == offset + h) & (extra_row < 3 * gate_rows)
            q_ref[h, :size, :] = turned[h * size : (h + 1) * size, :]
            q_ref[h, size:, :] = jnp.where(chosen, 1.0, 0.0).astype(BF16)
    key_base = (0, half_small)
    value_base = (half_small + half_large, 2 * half_small + half_large)

    def attend(block, diagonal):
        block_gates = gates[block]
        if diagonal:
            k_pos = lax.broadcasted_iota(jnp.int32, (tokens, tokens), 0)
            q_pos = lax.broadcasted_iota(jnp.int32, (tokens, tokens), 1)
            seen = q_pos >= k_pos
        for kind in range(2):
            heads, size, half, offset, q_ref, acc = (
                (heads_small, size_small, half_small, 0, turned_q_small, acc_small),
                (heads_large, size_large, half_large, heads_small, turned_q_large, acc_large),
            )[kind]
            kb, vb = key_base[kind], value_base[kind]
            rest = fold(size)[1]
            shift = block_gates * (-1.0 / rest)
            first = shift.astype(BF16).astype(F32)
            second = (shift - first).astype(BF16).astype(F32)
            pieces = [first, second, shift - first - second]
            if extra_rows > 3 * gate_rows:
                pieces.append(jnp.zeros((extra_rows - 3 * gate_rows, tokens), F32))
            keys = jnp.concatenate(
                [
                    kv[block, 0, kb : kb + half, :],
                    kv[block, 1, kb : kb + half, :],
                    jnp.concatenate(pieces, axis=0).astype(BF16),
                ],
                axis=0,
            ).T
            values = jnp.concatenate(
                [kv[block, 0, vb : vb + half, :], kv[block, 1, vb : vb + half, :]], axis=0
            )
            for h in range(heads):
                g = slice(offset + h, offset + h + 1)
                scores = jnp.dot(keys, q_ref[h], preferred_element_type=F32)
                if diagonal:
                    scores = jnp.where(seen, scores, -jnp.inf)
                block_top = jnp.max(scores, axis=0, keepdims=True)
                top = block_top if diagonal else jnp.maximum(top_ref[g, :], block_top)
                below_top = scores - top
                weights = jnp.exp(below_top if rest == 1.0 else below_top * rest)
                total = jnp.sum(weights, axis=0, keepdims=True)
                mixed = jnp.dot(values, weights.astype(BF16), preferred_element_type=F32)
                if not diagonal:
                    factor = jnp.exp((top_ref[g, :] - top) * rest)
                    total = total_ref[g, :] * factor + total
                    mixed = acc[h] * factor + mixed
                top_ref[g, :] = top
                total_ref[g, :] = total
                acc[h] = mixed

    def pass_on(block):
        kv_copy(block, seq, block).wait_recv()
        fwd_copy(block, parity).start()

    attend(seq, True)

    @pl.when(seq > 0)
    def _():
        pass_on(seq - 1)

    def earlier_block(i, carry):
        block = seq - 1 - i

        @pl.when(block > 0)
        def _():
            pass_on(block - 1)

        fwd_copy(block, 1 - parity).wait_recv()
        gate_copy(block, seq, block).wait_recv()
        attend(block, False)
        return carry

    lax.fori_loop(0, seq, earlier_block, 0)

    for h in range(heads_small):
        attn_t[h * size_small : (h + 1) * size_small, :] = (
            acc_small[h] * (1.0 / total_ref[h : h + 1, :])
        ).astype(BF16)
    for h in range(heads_large):
        first = width_small + h * size_large
        g = heads_small + h
        attn_t[first : first + size_large, :] = (
            acc_large[h] * (1.0 / total_ref[g : g + 1, :])
        ).astype(BF16)
    attn[...] = attn_t[...].T

    def row_ds(group, par):
        return pl.ds(pl.multiple_of((2 * group + par) * rows, rows), rows)

    def pair_copy(c):
        return pltpu.make_async_remote_copy(
            src_ref=pair_out.at[c],
            dst_ref=pair_in.at[c],
            send_sem=pair_send.at[c],
            recv_sem=pair_recv.at[c],
            device_id={"sp": seq, "tp": partner},
            device_id_type=MESH,
        )

    def cross_copy(c, group, source, slot):
        return pltpu.make_async_remote_copy(
            src_ref=cross_out.at[c, group],
            dst_ref=cross_in.at[c, source],
            send_sem=cross_send.at[c, slot],
            recv_sem=cross_recv.at[c, source],
            device_id={"sp": seq, "tp": 2 * group + parity},
            device_id_type=MESH,
        )

    my_group = lax.div(ten, 2)
    for load in loads[:2]:
        load.wait()
    for c in range(cols):
        part = jnp.dot(
            attn[...], proj_w[:, c * col_len : (c + 1) * col_len], preferred_element_type=F32
        )
        proj_f32[c] = part
        for group in range(half_groups):
            pair_out[c, group] = proj_f32[c, row_ds(group, 1 - parity), :].astype(BF16)
        pair_copy(c).start()
    for c in range(cols):
        pair_copy(c).wait_recv()
        for hop in range(1, half_groups):
            group = lax.rem(my_group + hop, half_groups)
            cross_out[c, group] = (
                proj_f32[c, row_ds(group, parity), :] + pair_in[c, group].astype(F32)
            ).astype(BF16)
            cross_copy(c, group, my_group, hop).start()
    def slot_ds(peer):
        return pl.ds(pl.multiple_of(peer * cap, cap), cap)

    def exchange(source_ref, target_ref, send, recv, peer, sender):
        return pltpu.make_async_remote_copy(
            src_ref=source_ref.at[slot_ds(peer)],
            dst_ref=target_ref.at[slot_ds(sender)],
            send_sem=send.at[peer],
            recv_sem=recv.at[sender],
            device_id={"sp": lax.div(peer, n_tp), "tp": lax.rem(peer, n_tp)},
            device_id_type=MESH,
        )

    def part_copy(c, peer, sender):
        if c < cols:
            source_ref, target_ref = outgoing.at[c], arrived.at[c]
        else:
            source_ref, target_ref = scale_out, scale_in
        return exchange(source_ref, target_ref, disp_send.at[c], disp_recv.at[c], peer, sender)

    def for_members(plane, action):
        def one(j, carry):
            peer = plane * n_tp + lax.rem(ten + j, n_tp)

            @pl.when(peer != me)
            def _():
                action(peer)

            return carry

        lax.fori_loop(0, n_tp, one, 0)

    slots = experts * cap
    block_rows = min(256, slots)

    def place_rows(values, c):
        for b in range(slots // block_rows):
            span = slice(b * block_rows, (b + 1) * block_rows)
            chosen = pick_ref[:rows, span]
            for k in range(1, top_count):
                chosen = chosen + pick_ref[k * rows : (k + 1) * rows, span]
            placed = lax.dot_general(
                chosen, values, (((0,), (0,)), ((), ())), preferred_element_type=F32
            ).astype(BF16)
            if c < cols:
                outgoing[c, span, :] = placed
            else:
                scale_out[span, :] = placed

        def dispatch(i, carry):
            for_members(
                lax.rem(seq + n_sp - i, n_sp), lambda peer: part_copy(c, peer, me).start()
            )
            return carry

        lax.fori_loop(0, n_sp, dispatch, 0)

    squares = jnp.zeros((rows, 1), F32)
    gain = norm_gain[...].astype(F32).reshape(1, width)
    for c in range(cols):
        span = slice(c * col_len, (c + 1) * col_len)
        value = proj_f32[c, row_ds(my_group, parity), :] + pair_in[c, my_group].astype(F32)
        for hop in range(1, half_groups):
            source = lax.rem(my_group + hop, half_groups)
            cross_copy(c, source, source, hop).wait_recv()
            value = value + cross_in[c, source].astype(F32)
        value = value + residual_in[:, span].astype(F32)
        resid_ref[:, span] = value
        squares = squares + jnp.sum(value * value, axis=1, keepdims=True)
        place_rows((value * gain[:, span]).astype(BF16), c)
    scale = lax.rsqrt(squares * (1.0 / width) + 1e-06)
    first = scale.astype(BF16).astype(F32)
    second = (scale - first).astype(BF16).astype(F32)
    third = scale - first - second
    lane = lax.broadcasted_iota(jnp.int32, (rows, 128), 1)
    parts = jnp.where(lane == 0, first, jnp.where(lane == 1, second, jnp.where(lane == 2, third, 0.0)))
    place_rows(parts.astype(BF16), cols)
    for c in range(cols):
        arrived[c, slot_ds(me), :] = outgoing[c, slot_ds(me), :]
    scale_in[slot_ds(me), :] = scale_out[slot_ds(me), :]
    for load in loads[2:]:
        load.wait()

    group_rows = n_tp * cap

    def serve(i, carry):
        plane = lax.rem(seq + i, n_sp)
        span = pl.ds(pl.multiple_of(plane * group_rows, group_rows), group_rows)
        gate_part = jnp.zeros((group_rows, gate_w.shape[1]), F32)
        up_part = jnp.zeros((group_rows, gate_w.shape[1]), F32)
        for c in range(cols):
            for_members(plane, lambda peer: part_copy(c, me, peer).wait_recv())
            came = arrived[c, span, :]
            depth = slice(c * col_len, (c + 1) * col_len)
            gate_part = gate_part + jnp.dot(came, gate_w[depth, :], preferred_element_type=F32)
            up_part = up_part + jnp.dot(came, up_w[depth, :], preferred_element_type=F32)
        for_members(plane, lambda peer: part_copy(cols, me, peer).wait_recv())
        row_scale = jnp.sum(scale_in[span, :].astype(F32), axis=1, keepdims=True)
        gate_part, up_part = gate_part * row_scale, up_part * row_scale
        hidden = (gate_part / (1.0 + jnp.exp(-gate_part)) * up_part).astype(BF16)
        result[span, :] = jnp.dot(hidden, down_w[...], preferred_element_type=F32).astype(BF16)
        for_members(
            plane,
            lambda peer: exchange(result, returned, back_send, back_recv, peer, me).start(),
        )
        return carry

    lax.fori_loop(0, n_sp, serve, 0)
    returned[slot_ds(me), :] = result[slot_ds(me), :]

    def collect(i, carry):
        peer = lax.rem(me + i, experts)
        exchange(result, returned, back_send, back_recv, me, peer).wait_recv()
        return carry

    lax.fori_loop(1, experts, collect, 0)
    for c in range(cols):
        span = slice(c * col_len, (c + 1) * col_len)
        picked = jnp.dot(pick_ref[...], returned[:, span], preferred_element_type=F32)
        value = resid_ref[:, span]
        for k in range(top_count):
            value = value + picked[k * rows : (k + 1) * rows] * column(route_weight, k)
        out[:, span] = value.astype(BF16)

    def sent_kv(target, carry):
        gate_copy(seq, target, target).wait_send()
        kv_copy(seq, target, target).wait_send()
        return carry

    lax.fori_loop(seq + 1, n_sp, sent_kv, 0)

    def sent_fwd(block, carry):
        fwd_copy(block, parity).wait_send()
        return carry

    lax.fori_loop(0, seq, sent_fwd, 0)
    for c in range(cols):
        pair_copy(c).wait_send()
        for hop in range(1, half_groups):
            group = lax.rem(my_group + hop, half_groups)
            cross_copy(c, group, my_group, hop).wait_send()

    def sent_rows(i, carry):
        peer = lax.rem(me + i, experts)
        for c in range(cols + 1):
            part_copy(c, peer, me).wait_send()
        exchange(result, returned, back_send, back_recv, peer, me).wait_send()
        return carry

    lax.fori_loop(1, experts, sent_rows, 0)


def shards(
    residual_in,
    query_small,
    query_large,
    key_small,
    key_large,
    value_small,
    value_large,
    forget_small,
    forget_large,
    project_small,
    project_large,
    norm_gain,
    expert_gate,
    expert_up,
    expert_down,
    routing,
    route_weight,
):
    n_sp, n_tp = lax.axis_size("sp"), lax.axis_size("tp")
    experts = n_sp * n_tp
    rows, width = residual_in.shape
    top_count = routing.shape[1]
    tokens = query_small.shape[0]
    size_small, size_large = key_small.shape[0], key_large.shape[0]
    heads_small, heads_large = forget_small.shape[0], forget_large.shape[0]
    heads = heads_small + heads_large
    gate_rows = -(-heads // 8) * 8
    extra_rows = -(-3 * gate_rows // 16) * 16
    capacity = max(2, 2 * rows * top_count // experts)
    cap = -(-capacity // 16) * 16
    col_len = min(width, 512)
    cols = width // col_len
    hidden = expert_gate.shape[2]
    attn_width = heads_small * size_small + heads_large * size_large
    half_groups = n_tp // 2
    slots = experts * cap
    vmem, dma = pltpu.VMEM, pltpu.SemaphoreType.DMA
    return pl.pallas_call(
        functools.partial(layer_kernel, (n_sp, n_tp, cap, col_len)),
        out_shape=jax.ShapeDtypeStruct((rows, width), BF16),
        in_specs=[pl.BlockSpec(memory_space=pltpu.VMEM)] * 12
        + [pl.BlockSpec(memory_space=pl.ANY)] * 5,
        out_specs=pl.BlockSpec(memory_space=pltpu.VMEM),
        scratch_shapes=[
            vmem((n_sp, 2, size_small + size_large, tokens), BF16),
            vmem((n_sp, gate_rows, tokens), F32),
            vmem((heads_small, size_small + extra_rows, tokens), BF16),
            vmem((heads_large, size_large + extra_rows, tokens), BF16),
            vmem((gate_rows, tokens), F32),
            vmem((gate_rows, tokens), F32),
            vmem((heads_small, size_small, tokens), F32),
            vmem((heads_large, size_large, tokens), F32),
            vmem((attn_width, tokens), BF16),
            vmem((tokens, attn_width), BF16),
            vmem((attn_width, width), BF16),
            vmem((width, hidden), BF16),
            vmem((width, hidden), BF16),
            vmem((hidden, width), BF16),
            vmem((cols, tokens, col_len), F32),
            vmem((cols, half_groups, rows, col_len), BF16),
            vmem((cols, half_groups, rows, col_len), BF16),
            vmem((cols, half_groups, rows, col_len), BF16),
            vmem((cols, half_groups, rows, col_len), BF16),
            vmem((rows, width), F32),
            vmem((top_count * rows, slots), BF16),
            vmem((cols, slots, col_len), BF16),
            vmem((cols, slots, col_len), BF16),
            vmem((slots, 128), BF16),
            vmem((slots, 128), BF16),
            vmem((slots, width), BF16),
            vmem((slots, width), BF16),
            dma((5,)),
            dma((n_sp,)),
            dma((n_sp,)),
            dma((n_sp,)),
            dma((n_sp,)),
            dma((n_sp,)),
            dma((n_sp,)),
            dma((cols,)),
            dma((cols,)),
            dma((cols, half_groups)),
            dma((cols, half_groups)),
            dma((cols + 1, experts)),
            dma((cols + 1, experts)),
            dma((experts,)),
            dma((experts,)),
        ],
        compiler_params=pltpu.CompilerParams(
            collective_id=0, has_side_effects=True, vmem_limit_bytes=60 * 1024 * 1024
        ),
    )(
        residual_in,
        query_small,
        query_large,
        key_small,
        key_large,
        value_small,
        value_large,
        forget_small,
        forget_large,
        norm_gain,
        routing.T,
        route_weight.T,
        project_small,
        project_large,
        expert_gate,
        expert_up,
        expert_down,
    )


def solution(mesh):
    in_specs = (
        P(("grp", "sp", "tp"), None),
        P(("grp", "sp"), "tp"),
        P(("grp", "sp"), "tp"),
        P(None, ("grp", "sp")),
        P(None, ("grp", "sp")),
        P(None, ("grp", "sp")),
        P(None, ("grp", "sp")),
        P("tp", ("grp", "sp")),
        P("tp", ("grp", "sp")),
        P("tp", None),
        P("tp", None),
        P(),
        P(("sp", "tp"), None, None),
        P(("sp", "tp"), None, None),
        P(("sp", "tp"), None, None),
        P(("grp", "sp", "tp"), None),
        P(("grp", "sp", "tp"), None),
    )
    out_specs = P(("grp", "sp", "tp"), None)
    return jax.shard_map(shards, mesh=mesh, in_specs=in_specs, out_specs=out_specs, check_vma=False)
```

```python
import functools
import math

import jax
import jax.numpy as jnp
from jax import lax
from jax.experimental import pallas as pl
from jax.experimental.pallas import tpu as pltpu
from jax.sharding import PartitionSpec as P

MESH = pl.DeviceIdType.MESH
F32 = jnp.float32
BF16 = jnp.bfloat16


def layer_kernel(dims, *refs):
    (
        residual_in,
        query_small,
        query_large,
        key_small,
        key_large,
        value_small,
        value_large,
        forget_small,
        forget_large,
        norm_gain,
        routing,
        route_weight,
        project_small,
        project_large,
        expert_gate,
        expert_up,
        expert_down,
        out,
        kv,
        gates,
        turned_q_small,
        turned_q_large,
        top_ref,
        total_ref,
        acc_small,
        acc_large,
        attn_t,
        attn,
        proj_w,
        gate_w,
        up_w,
        down_w,
        proj_f32,
        pair_out,
        pair_in,
        cross_out,
        cross_in,
        resid_ref,
        weight_sem,
        kv_send,
        kv_recv,
        gate_send,
        gate_recv,
        fwd_send,
        fwd_recv,
        pair_send,
        pair_recv,
        cross_send,
        cross_recv,
        *tail,
    ) = refs
    n_sp, n_tp, cap, col_len, lined = dims
    experts = n_sp * n_tp
    seq = lax.axis_index("sp")
    ten = lax.axis_index("tp")
    me = seq * n_tp + ten
    parity = lax.rem(ten, 2)
    partner = ten + 1 - 2 * parity
    tokens = query_small.shape[0]
    size_small, size_large = key_small.shape[0], key_large.shape[0]
    heads_small, heads_large = forget_small.shape[0], forget_large.shape[0]
    width_small = heads_small * size_small
    rows, width = residual_in.shape
    piece_small, piece_large = size_small // n_tp, size_large // n_tp
    cols = width // col_len
    half_groups = n_tp // 2

    loads = [
        pltpu.make_async_copy(project_small, proj_w.at[pl.ds(0, width_small)], weight_sem.at[0]),
        pltpu.make_async_copy(
            project_large,
            proj_w.at[pl.ds(width_small, heads_large * size_large)],
            weight_sem.at[1],
        ),
        pltpu.make_async_copy(expert_gate.at[0], gate_w, weight_sem.at[2]),
        pltpu.make_async_copy(expert_up.at[0], up_w, weight_sem.at[3]),
        pltpu.make_async_copy(expert_down.at[0], down_w, weight_sem.at[4]),
    ]
    for load in loads:
        load.start()

    barrier = pltpu.get_barrier_semaphore()

    def greet(peer_sp, peer_tp):
        pl.semaphore_signal(
            barrier, inc=1, device_id={"sp": peer_sp, "tp": peer_tp}, device_id_type=MESH
        )

    if lined:
        for i in range(1, n_tp):
            greet(seq, lax.rem(ten + i, n_tp))
        for i in range(1, n_sp):
            greet(lax.rem(seq + i, n_sp), ten)
    else:

        def greet_all(i, carry):
            peer = lax.rem(me + i, experts)
            greet(lax.div(peer, n_tp), lax.rem(peer, n_tp))
            return carry

        lax.fori_loop(1, experts, greet_all, 0)

    for p in range(n_tp):
        base = 0
        for source, piece in (
            (key_small, piece_small),
            (key_large, piece_large),
            (value_small, piece_small),
            (value_large, piece_large),
        ):
            kv[seq, p, base : base + piece, :] = source[p * piece : (p + 1) * piece, :]
            base += piece
    gates[seq, :heads_small, :] = forget_small[...]
    gates[seq, heads_small : heads_small + heads_large, :] = forget_large[...]
    gate_rows = gates.shape[1]
    if gate_rows > heads_small + heads_large:
        gates[seq, heads_small + heads_large :, :] = jnp.zeros(
            (gate_rows - heads_small - heads_large, tokens), F32
        )

    pl.semaphore_wait(barrier, n_tp + n_sp - 2 if lined else experts - 1)

    def kv_copy(source, target, slot):
        return pltpu.make_async_remote_copy(
            src_ref=kv.at[source, ten],
            dst_ref=kv.at[source, ten],
            send_sem=kv_send.at[slot],
            recv_sem=kv_recv.at[source],
            device_id={"sp": target, "tp": ten},
            device_id_type=MESH,
        )

    def gate_copy(source, target, slot):
        return pltpu.make_async_remote_copy(
            src_ref=gates.at[source],
            dst_ref=gates.at[source],
            send_sem=gate_send.at[slot],
            recv_sem=gate_recv.at[source],
            device_id={"sp": target, "tp": ten},
            device_id_type=MESH,
        )

    def fwd_copy(source, piece, peer):
        return pltpu.make_async_remote_copy(
            src_ref=kv.at[source, piece],
            dst_ref=kv.at[source, piece],
            send_sem=fwd_send.at[source, peer],
            recv_sem=fwd_recv.at[source, piece],
            device_id={"sp": seq, "tp": peer},
            device_id_type=MESH,
        )

    def for_mates(action):
        for i in range(1, n_tp):
            action(lax.rem(ten + i, n_tp))

    def send_kv(target, carry):
        gate_copy(seq, target, target).start()
        kv_copy(seq, target, target).start()
        return carry

    lax.fori_loop(seq + 1, n_sp, send_kv, 0)

    lanes = lax.broadcasted_iota(jnp.int32, (rows, experts), 1)
    same = lax.broadcasted_iota(jnp.int32, (rows, rows), 0) == lax.broadcasted_iota(
        jnp.int32, (rows, rows), 1
    )

    def column(ref, k):
        return jnp.sum(
            jnp.where(same, ref[k : k + 1, :].astype(F32), 0.0), axis=1, keepdims=True
        )

    top_count = routing.shape[0]
    routes = [column(routing, k) for k in range(top_count)]
    hot = [(routes[k] == lanes.astype(F32)).astype(F32) for k in range(top_count)]
    named = sum(hot).astype(BF16)
    below = (
        lax.broadcasted_iota(jnp.int32, (rows, rows), 0)
        > lax.broadcasted_iota(jnp.int32, (rows, rows), 1)
    ).astype(F32)
    earlier = jnp.dot(below.astype(BF16), named, preferred_element_type=F32)
    places = [
        routes[k] * cap + jnp.sum(earlier * hot[k], axis=1, keepdims=True)
        for k in range(top_count)
    ]

    if lined:
        (
            pick_out,
            pick_in,
            choose,
            weight_in,
            lane_rows,
            lane_scale,
            outgoing,
            arrived,
            scale_out,
            scale_in,
            result,
            returned,
            line_out,
            line_in,
            pick_send,
            pick_recv,
            share_send,
            share_recv,
            lane_send,
            lane_recv,
            disp_send,
            disp_recv,
            back_send,
            back_recv,
            line_send,
            line_recv,
        ) = tail
        plane_slots = n_tp * cap
        slot_lane = lax.broadcasted_iota(jnp.int32, (rows, plane_slots), 1)
        for p in range(n_sp):
            spots = (slot_lane + p * plane_slots).astype(F32)
            for k in range(top_count):
                pick_out[p, k * rows : (k + 1) * rows, :] = (
                    (spots == places[k]).astype(F32).astype(BF16)
                )
        pick_in[seq] = pick_out[seq]
        wide = lax.broadcasted_iota(jnp.int32, (rows, 128), 1)
        shares = jnp.zeros((rows, 128), F32)
        for k in range(top_count):
            shares = jnp.where(wide == k, column(route_weight, k), shares)
        weight_in[seq] = shares

        def pick_copy(target, sender):
            return pltpu.make_async_remote_copy(
                src_ref=pick_out.at[target],
                dst_ref=pick_in.at[sender],
                send_sem=pick_send.at[target],
                recv_sem=pick_recv.at[sender],
                device_id={"sp": target, "tp": ten},
                device_id_type=MESH,
            )

        def share_copy(target, sender):
            return pltpu.make_async_remote_copy(
                src_ref=weight_in.at[sender],
                dst_ref=weight_in.at[sender],
                send_sem=share_send.at[target],
                recv_sem=share_recv.at[sender],
                device_id={"sp": target, "tp": ten},
                device_id_type=MESH,
            )

        for i in range(1, n_sp):
            target = lax.rem(seq + i, n_sp)
            pick_copy(target, seq).start()
            share_copy(target, seq).start()
    else:
        (
            pick_ref,
            outgoing,
            arrived,
            scale_out,
            scale_in,
            result,
            returned,
            disp_send,
            disp_recv,
            back_send,
            back_recv,
        ) = tail
        spots = lax.broadcasted_iota(jnp.int32, (rows, experts * cap), 1).astype(F32)
        for k in range(top_count):
            pick_ref[k * rows : (k + 1) * rows, :] = (
                (spots == places[k]).astype(F32).astype(BF16)
            )

    extra_rows = turned_q_small.shape[1] - size_small

    def fold(size):
        power = 2.0 ** math.floor(math.log2(size**-0.5))
        return power, size**-0.5 / power

    extra_row = lax.broadcasted_iota(jnp.int32, (extra_rows, tokens), 0)
    for kind in range(2):
        heads, size, offset, source, q_ref = (
            (heads_small, size_small, 0, query_small, turned_q_small),
            (heads_large, size_large, heads_small, query_large, turned_q_large),
        )[kind]
        turned = (source[...] * fold(size)[0]).astype(BF16).T
        for h in range(heads):
            chosen = (lax.rem(extra_row, gate_rows) == offset + h) & (extra_row < 3 * gate_rows)
            q_ref[h, :size, :] = turned[h * size : (h + 1) * size, :]
            q_ref[h, size:, :] = jnp.where(chosen, 1.0, 0.0).astype(BF16)
    key_base = (0, piece_small)
    value_base = (piece_small + piece_large, 2 * piece_small + piece_large)

    def attend(block, diagonal):
        block_gates = gates[block]
        if diagonal:
            k_pos = lax.broadcasted_iota(jnp.int32, (tokens, tokens), 0)
            q_pos = lax.broadcasted_iota(jnp.int32, (tokens, tokens), 1)
            seen = q_pos >= k_pos
        for kind in range(2):
            heads, size, piece, offset, q_ref, acc = (
                (heads_small, size_small, piece_small, 0, turned_q_small, acc_small),
                (heads_large, size_large, piece_large, heads_small, turned_q_large, acc_large),
            )[kind]
            kb, vb = key_base[kind], value_base[kind]
            rest = fold(size)[1]
            shift = block_gates * (-1.0 / rest)
            first = shift.astype(BF16).astype(F32)
            second = (shift - first).astype(BF16).astype(F32)
            pieces = [first, second, shift - first - second]
            if extra_rows > 3 * gate_rows:
                pieces.append(jnp.zeros((extra_rows - 3 * gate_rows, tokens), F32))
            keys = jnp.concatenate(
                [kv[block, p, kb : kb + piece, :] for p in range(n_tp)]
                + [jnp.concatenate(pieces, axis=0).astype(BF16)],
                axis=0,
            ).T
            values = jnp.concatenate(
                [kv[block, p, vb : vb + piece, :] for p in range(n_tp)], axis=0
            )
            for h in range(heads):
                g = slice(offset + h, offset + h + 1)
                scores = jnp.dot(keys, q_ref[h], preferred_element_type=F32)
                if diagonal:
                    scores = jnp.where(seen, scores, -jnp.inf)
                block_top = jnp.max(scores, axis=0, keepdims=True)
                top = block_top if diagonal else jnp.maximum(top_ref[g, :], block_top)
                below_top = scores - top
                weights = jnp.exp(below_top if rest == 1.0 else below_top * rest)
                total = jnp.sum(weights, axis=0, keepdims=True)
                mixed = jnp.dot(values, weights.astype(BF16), preferred_element_type=F32)
                if not diagonal:
                    factor = jnp.exp((top_ref[g, :] - top) * rest)
                    total = total_ref[g, :] * factor + total
                    mixed = acc[h] * factor + mixed
                top_ref[g, :] = top
                total_ref[g, :] = total
                acc[h] = mixed

    def pass_on(block):
        kv_copy(block, seq, block).wait_recv()
        for_mates(lambda peer: fwd_copy(block, ten, peer).start())

    attend(seq, True)

    @pl.when(seq > 0)
    def _():
        pass_on(seq - 1)

    def earlier_block(i, carry):
        block = seq - 1 - i

        @pl.when(block > 0)
        def _():
            pass_on(block - 1)

        for_mates(lambda peer: fwd_copy(block, peer, peer).wait_recv())
        gate_copy(block, seq, block).wait_recv()
        attend(block, False)
        return carry

    lax.fori_loop(0, seq, earlier_block, 0)

    for h in range(heads_small):
        attn_t[h * size_small : (h + 1) * size_small, :] = (
            acc_small[h] * (1.0 / total_ref[h : h + 1, :])
        ).astype(BF16)
    for h in range(heads_large):
        first = width_small + h * size_large
        g = heads_small + h
        attn_t[first : first + size_large, :] = (
            acc_large[h] * (1.0 / total_ref[g : g + 1, :])
        ).astype(BF16)
    attn[...] = attn_t[...].T

    def row_ds(group, par):
        return pl.ds(pl.multiple_of((2 * group + par) * rows, rows), rows)

    def pair_copy(c):
        return pltpu.make_async_remote_copy(
            src_ref=pair_out.at[c],
            dst_ref=pair_in.at[c],
            send_sem=pair_send.at[c],
            recv_sem=pair_recv.at[c],
            device_id={"sp": seq, "tp": partner},
            device_id_type=MESH,
        )

    def cross_copy(c, group, source, slot):
        return pltpu.make_async_remote_copy(
            src_ref=cross_out.at[c, group],
            dst_ref=cross_in.at[c, source],
            send_sem=cross_send.at[c, slot],
            recv_sem=cross_recv.at[c, source],
            device_id={"sp": seq, "tp": 2 * group + parity},
            device_id_type=MESH,
        )

    my_group = lax.div(ten, 2)
    for load in loads[:2]:
        load.wait()
    for c in range(cols):
        part = jnp.dot(
            attn[...], proj_w[:, c * col_len : (c + 1) * col_len], preferred_element_type=F32
        )
        proj_f32[c] = part
        for group in range(half_groups):
            pair_out[c, group] = proj_f32[c, row_ds(group, 1 - parity), :].astype(BF16)
        pair_copy(c).start()
    for c in range(cols):
        pair_copy(c).wait_recv()
        for hop in range(1, half_groups):
            group = lax.rem(my_group + hop, half_groups)
            cross_out[c, group] = (
                proj_f32[c, row_ds(group, parity), :] + pair_in[c, group].astype(F32)
            ).astype(BF16)
            cross_copy(c, group, my_group, hop).start()
    def own_rows(c, span, squares):
        value = proj_f32[c, row_ds(my_group, parity), :] + pair_in[c, my_group].astype(F32)
        for hop in range(1, half_groups):
            source = lax.rem(my_group + hop, half_groups)
            cross_copy(c, source, source, hop).wait_recv()
            value = value + cross_in[c, source].astype(F32)
        value = value + residual_in[:, span].astype(F32)
        resid_ref[:, span] = value
        squares = squares + jnp.sum(value * value, axis=1, keepdims=True)
        return value, squares

    def scale_parts(squares):
        scale = lax.rsqrt(squares * (1.0 / width) + 1e-06)
        first = scale.astype(BF16).astype(F32)
        second = (scale - first).astype(BF16).astype(F32)
        third = scale - first - second
        lane = lax.broadcasted_iota(jnp.int32, (rows, 128), 1)
        parts = jnp.where(lane == 0, first, 0.0)
        parts = jnp.where(lane == 1, second, parts)
        return jnp.where(lane == 2, third, parts).astype(BF16)

    if lined:

        def slot_ds(member):
            return pl.ds(pl.multiple_of(member * cap, cap), cap)

        def lane_copy(z, c, up):
            ref = lane_rows.at[z, c] if c < cols else lane_scale.at[z]
            return pltpu.make_async_remote_copy(
                src_ref=ref,
                dst_ref=ref,
                send_sem=lane_send.at[up, z, c],
                recv_sem=lane_recv.at[z, c],
                device_id={"sp": seq + 2 * up - 1, "tp": ten},
                device_id_type=MESH,
            )

        def disp_copy(z, c, peer, sender):
            source, target = (
                (outgoing.at[z, c], arrived.at[z, c])
                if c < cols
                else (scale_out.at[z], scale_in.at[z])
            )
            return pltpu.make_async_remote_copy(
                src_ref=source.at[slot_ds(peer)],
                dst_ref=target.at[slot_ds(sender)],
                send_sem=disp_send.at[z, c, peer],
                recv_sem=disp_recv.at[z, c, sender],
                device_id={"sp": seq, "tp": peer},
                device_id_type=MESH,
            )

        def back_copy(z, c, peer, sender):
            return pltpu.make_async_remote_copy(
                src_ref=result.at[z, c, slot_ds(peer)],
                dst_ref=returned.at[z, c, slot_ds(sender)],
                send_sem=back_send.at[z, c, peer],
                recv_sem=back_recv.at[z, c, sender],
                device_id={"sp": seq, "tp": peer},
                device_id_type=MESH,
            )

        def line_copy(z, c, up):
            return pltpu.make_async_remote_copy(
                src_ref=line_out.at[z, c],
                dst_ref=line_in.at[z + up, c],
                send_sem=line_send.at[z, c],
                recv_sem=line_recv.at[z + up, c],
                device_id={"sp": seq + 2 * up - 1, "tp": ten},
                device_id_type=MESH,
            )

        def go_on(z, c, up):
            if up:

                @pl.when(seq + 1 < n_sp)
                def _():
                    lane_copy(z, c, 1).start()
            else:

                @pl.when(seq > 0)
                def _():
                    lane_copy(z, c, 0).start()

        def place_rows(z, c):
            values = lane_rows[z, c] if c < cols else lane_scale[z]
            placed = jnp.dot(choose[z], values, preferred_element_type=F32).astype(BF16)
            if c < cols:
                outgoing[z, c] = placed
            else:
                scale_out[z] = placed
            for_mates(lambda peer: disp_copy(z, c, peer, ten).start())
            if c < cols:
                arrived[z, c, slot_ds(ten), :] = outgoing[z, c, slot_ds(ten), :]
            else:
                scale_in[z, slot_ds(ten), :] = scale_out[z, slot_ds(ten), :]

        def at_sides(distance, action):
            for up in range(2):
                z = seq - distance if up else seq + distance

                @pl.when(z >= 0 if up else z < n_sp)
                def _():
                    action(z, up)

        def turn_choice(z):
            both = pick_in[z, :rows, :].astype(F32)
            for k in range(1, top_count):
                both = both + pick_in[z, k * rows : (k + 1) * rows, :].astype(F32)
            choose[z] = both.T.astype(BF16)

        def take(distance, c):
            def one(z, up):
                lane_copy(z, c, up).wait_recv()
                go_on(z, c, up)

            def two(z, up):
                if c == 0:
                    pick_copy(seq, z).wait_recv()
                    turn_choice(z)
                place_rows(z, c)

            at_sides(distance, one)
            at_sides(distance, two)

        def serve(z):
            gate_part = jnp.zeros((plane_slots, gate_w.shape[1]), F32)
            up_part = jnp.zeros((plane_slots, gate_w.shape[1]), F32)
            for c in range(cols):
                for_mates(lambda peer: disp_copy(z, c, ten, peer).wait_recv())
                came = arrived[z, c]
                depth = slice(c * col_len, (c + 1) * col_len)
                gate_part = gate_part + jnp.dot(came, gate_w[depth, :], preferred_element_type=F32)
                up_part = up_part + jnp.dot(came, up_w[depth, :], preferred_element_type=F32)
            for_mates(lambda peer: disp_copy(z, cols, ten, peer).wait_recv())
            row_scale = jnp.sum(scale_in[z].astype(F32), axis=1, keepdims=True)
            gate_part, up_part = gate_part * row_scale, up_part * row_scale
            hidden = (gate_part / (1.0 + jnp.exp(-gate_part)) * up_part).astype(BF16)
            for c in range(cols):
                result[z, c] = jnp.dot(
                    hidden, down_w[:, c * col_len : (c + 1) * col_len], preferred_element_type=F32
                ).astype(BF16)
                for_mates(lambda peer: back_copy(z, c, peer, ten).start())
                returned[z, c, slot_ds(ten), :] = result[z, c, slot_ds(ten), :]

        def mixed(z, c):
            for_mates(lambda peer: back_copy(z, c, ten, peer).wait_recv())
            picked = jnp.dot(pick_in[z], returned[z, c], preferred_element_type=F32)
            shares = weight_in[z]
            value = picked[:rows] * shares[:, 0:1]
            for k in range(1, top_count):
                value = value + picked[k * rows : (k + 1) * rows] * shares[:, k : k + 1]
            return value

        def give_back(z, up):
            share_copy(seq, z).wait_recv()
            slot = z + up
            outer = seq > 0 if up else seq + 1 < n_sp
            for c in range(cols):
                value = mixed(z, c)

                @pl.when(outer)
                def _():
                    line_copy(z, c, up).wait_recv()
                    line_out[z, c] = (value + line_in[slot, c].astype(F32)).astype(BF16)

                @pl.when(jnp.logical_not(outer))
                def _():
                    line_out[z, c] = value.astype(BF16)

                line_copy(z, c, up).start()

        def chain(j):
            @pl.when(n_sp - 1 - j < seq)
            def _():
                give_back(n_sp - 1 - j, 0)

            @pl.when(j > seq)
            def _():
                give_back(j, 1)

        turn_choice(seq)
        squares = jnp.zeros((rows, 1), F32)
        gain = norm_gain[...].astype(F32).reshape(1, width)
        for c in range(cols):
            span = slice(c * col_len, (c + 1) * col_len)
            value, squares = own_rows(c, span, squares)
            lane_rows[seq, c] = (value * gain[:, span]).astype(BF16)
            go_on(seq, c, 0)
            go_on(seq, c, 1)
            place_rows(seq, c)
        lane_scale[seq] = scale_parts(squares)
        go_on(seq, cols, 0)
        go_on(seq, cols, 1)
        place_rows(seq, cols)
        for load in loads[2:]:
            load.wait()

        for step in range(1, n_sp + 2):
            moving = step < n_sp
            if moving:
                take(step, 0)
            if step == 2:
                for c in range(cols):
                    span = slice(c * col_len, (c + 1) * col_len)
                    resid_ref[:, span] = resid_ref[:, span] + mixed(seq, c)
            elif step > 2:
                chain(step - 2)
            if moving:
                take(step, 1)
            if step == 1:
                for c in range(2, cols + 1):
                    take(step, c)
                serve(seq)
            elif step <= n_sp:
                at_sides(step - 1, lambda z, up: serve(z))
                if moving:
                    for c in range(2, cols + 1):
                        take(step, c)

        for c in range(cols):
            span = slice(c * col_len, (c + 1) * col_len)
            for up in range(2):

                @pl.when(seq > 0 if up else seq + 1 < n_sp)
                def _():
                    line_copy(seq, c, up).wait_recv()
                    resid_ref[:, span] = resid_ref[:, span] + line_in[seq + up, c].astype(F32)

            out[:, span] = resid_ref[:, span].astype(BF16)

        for i in range(1, n_sp):
            target = lax.rem(seq + i, n_sp)
            pick_copy(target, seq).wait_send()
            share_copy(target, seq).wait_send()

        def sent_lane(z, c, up):
            @pl.when(seq + 1 < n_sp if up else seq > 0)
            def _():
                lane_copy(z, c, up).wait_send()

        def sent_block(z, carry):
            for c in range(cols + 1):
                for_mates(lambda peer: disp_copy(z, c, peer, ten).wait_send())
                if c < cols:
                    for_mates(lambda peer: back_copy(z, c, peer, ten).wait_send())
                for up in range(2):

                    @pl.when(z <= seq if up else z >= seq)
                    def _():
                        sent_lane(z, c, up)

                if c < cols:

                    @pl.when(z < seq)
                    def _():
                        line_copy(z, c, 0).wait_send()

                    @pl.when(z > seq)
                    def _():
                        line_copy(z, c, 1).wait_send()

            return carry

        lax.fori_loop(0, n_sp, sent_block, 0)
    else:
        def slot_ds(peer):
            return pl.ds(pl.multiple_of(peer * cap, cap), cap)

        def exchange(source_ref, target_ref, send, recv, peer, sender):
            return pltpu.make_async_remote_copy(
                src_ref=source_ref.at[slot_ds(peer)],
                dst_ref=target_ref.at[slot_ds(sender)],
                send_sem=send.at[peer],
                recv_sem=recv.at[sender],
                device_id={"sp": lax.div(peer, n_tp), "tp": lax.rem(peer, n_tp)},
                device_id_type=MESH,
            )

        def part_copy(c, peer, sender):
            if c < cols:
                source_ref, target_ref = outgoing.at[c], arrived.at[c]
            else:
                source_ref, target_ref = scale_out, scale_in
            return exchange(source_ref, target_ref, disp_send.at[c], disp_recv.at[c], peer, sender)

        def for_members(plane, action):
            def one(j, carry):
                peer = plane * n_tp + lax.rem(ten + j, n_tp)

                @pl.when(peer != me)
                def _():
                    action(peer)

                return carry

            lax.fori_loop(0, n_tp, one, 0)

        slots = experts * cap
        block_rows = min(256, slots)

        def place_rows(values, c):
            for b in range(slots // block_rows):
                span = slice(b * block_rows, (b + 1) * block_rows)
                chosen = pick_ref[:rows, span]
                for k in range(1, top_count):
                    chosen = chosen + pick_ref[k * rows : (k + 1) * rows, span]
                placed = lax.dot_general(
                    chosen, values, (((0,), (0,)), ((), ())), preferred_element_type=F32
                ).astype(BF16)
                if c < cols:
                    outgoing[c, span, :] = placed
                else:
                    scale_out[span, :] = placed

            def dispatch(i, carry):
                for_members(
                    lax.rem(seq + n_sp - i, n_sp), lambda peer: part_copy(c, peer, me).start()
                )
                return carry

            lax.fori_loop(0, n_sp, dispatch, 0)

        squares = jnp.zeros((rows, 1), F32)
        gain = norm_gain[...].astype(F32).reshape(1, width)
        for c in range(cols):
            span = slice(c * col_len, (c + 1) * col_len)
            value, squares = own_rows(c, span, squares)
            place_rows((value * gain[:, span]).astype(BF16), c)
        place_rows(scale_parts(squares), cols)
        for c in range(cols):
            arrived[c, slot_ds(me), :] = outgoing[c, slot_ds(me), :]
        scale_in[slot_ds(me), :] = scale_out[slot_ds(me), :]
        for load in loads[2:]:
            load.wait()

        group_rows = n_tp * cap

        def serve(i, carry):
            plane = lax.rem(seq + i, n_sp)
            span = pl.ds(pl.multiple_of(plane * group_rows, group_rows), group_rows)
            gate_part = jnp.zeros((group_rows, gate_w.shape[1]), F32)
            up_part = jnp.zeros((group_rows, gate_w.shape[1]), F32)
            for c in range(cols):
                for_members(plane, lambda peer: part_copy(c, me, peer).wait_recv())
                came = arrived[c, span, :]
                depth = slice(c * col_len, (c + 1) * col_len)
                gate_part = gate_part + jnp.dot(came, gate_w[depth, :], preferred_element_type=F32)
                up_part = up_part + jnp.dot(came, up_w[depth, :], preferred_element_type=F32)
            for_members(plane, lambda peer: part_copy(cols, me, peer).wait_recv())
            row_scale = jnp.sum(scale_in[span, :].astype(F32), axis=1, keepdims=True)
            gate_part, up_part = gate_part * row_scale, up_part * row_scale
            hidden = (gate_part / (1.0 + jnp.exp(-gate_part)) * up_part).astype(BF16)
            result[span, :] = jnp.dot(hidden, down_w[...], preferred_element_type=F32).astype(BF16)
            for_members(
                plane,
                lambda peer: exchange(result, returned, back_send, back_recv, peer, me).start(),
            )
            return carry

        lax.fori_loop(0, n_sp, serve, 0)
        returned[slot_ds(me), :] = result[slot_ds(me), :]

        def collect(i, carry):
            peer = lax.rem(me + i, experts)
            exchange(result, returned, back_send, back_recv, me, peer).wait_recv()
            return carry

        lax.fori_loop(1, experts, collect, 0)
        for c in range(cols):
            span = slice(c * col_len, (c + 1) * col_len)
            picked = jnp.dot(pick_ref[...], returned[:, span], preferred_element_type=F32)
            value = resid_ref[:, span]
            for k in range(top_count):
                value = value + picked[k * rows : (k + 1) * rows] * column(route_weight, k)
            out[:, span] = value.astype(BF16)

        def sent_rows(i, carry):
            peer = lax.rem(me + i, experts)
            for c in range(cols + 1):
                part_copy(c, peer, me).wait_send()
            exchange(result, returned, back_send, back_recv, peer, me).wait_send()
            return carry

        lax.fori_loop(1, experts, sent_rows, 0)

    def sent_kv(target, carry):
        gate_copy(seq, target, target).wait_send()
        kv_copy(seq, target, target).wait_send()
        return carry

    lax.fori_loop(seq + 1, n_sp, sent_kv, 0)

    def sent_fwd(block, carry):
        for_mates(lambda peer: fwd_copy(block, ten, peer).wait_send())
        return carry

    lax.fori_loop(0, seq, sent_fwd, 0)
    for c in range(cols):
        pair_copy(c).wait_send()
        for hop in range(1, half_groups):
            group = lax.rem(my_group + hop, half_groups)
            cross_copy(c, group, my_group, hop).wait_send()


def shards(
    residual_in,
    query_small,
    query_large,
    key_small,
    key_large,
    value_small,
    value_large,
    forget_small,
    forget_large,
    project_small,
    project_large,
    norm_gain,
    expert_gate,
    expert_up,
    expert_down,
    routing,
    route_weight,
):
    n_sp, n_tp = lax.axis_size("sp"), lax.axis_size("tp")
    experts = n_sp * n_tp
    rows, width = residual_in.shape
    top_count = routing.shape[1]
    tokens = query_small.shape[0]
    size_small, size_large = key_small.shape[0], key_large.shape[0]
    heads_small, heads_large = forget_small.shape[0], forget_large.shape[0]
    heads = heads_small + heads_large
    gate_rows = -(-heads // 8) * 8
    extra_rows = -(-3 * gate_rows // 16) * 16
    capacity = max(2, 2 * rows * top_count // experts)
    cap = -(-capacity // 16) * 16
    col_len = min(width, 512)
    cols = width // col_len
    hidden = expert_gate.shape[2]
    attn_width = heads_small * size_small + heads_large * size_large
    half_groups = n_tp // 2
    slots = experts * cap
    group = n_tp * cap
    lined = n_tp * capacity >= rows
    vmem, dma = pltpu.VMEM, pltpu.SemaphoreType.DMA
    if lined:
        tail = [
            vmem((n_sp, top_count * rows, group), BF16),
            vmem((n_sp, top_count * rows, group), BF16),
            vmem((n_sp, group, rows), BF16),
            vmem((n_sp, rows, 128), F32),
            vmem((n_sp, cols, rows, col_len), BF16),
            vmem((n_sp, rows, 128), BF16),
            vmem((n_sp, cols, group, col_len), BF16),
            vmem((n_sp, cols, group, col_len), BF16),
            vmem((n_sp, group, 128), BF16),
            vmem((n_sp, group, 128), BF16),
            vmem((n_sp, cols, group, col_len), BF16),
            vmem((n_sp, cols, group, col_len), BF16),
            vmem((n_sp, cols, rows, col_len), BF16),
            vmem((n_sp + 1, cols, rows, col_len), BF16),
            dma((n_sp,)),
            dma((n_sp,)),
            dma((n_sp,)),
            dma((n_sp,)),
            dma((2, n_sp, cols + 1)),
            dma((n_sp, cols + 1)),
            dma((n_sp, cols + 1, n_tp)),
            dma((n_sp, cols + 1, n_tp)),
            dma((n_sp, cols, n_tp)),
            dma((n_sp, cols, n_tp)),
            dma((n_sp, cols)),
            dma((n_sp + 1, cols)),
        ]
    else:
        tail = [
            vmem((top_count * rows, slots), BF16),
            vmem((cols, slots, col_len), BF16),
            vmem((cols, slots, col_len), BF16),
            vmem((slots, 128), BF16),
            vmem((slots, 128), BF16),
            vmem((slots, width), BF16),
            vmem((slots, width), BF16),
            dma((cols + 1, experts)),
            dma((cols + 1, experts)),
            dma((experts,)),
            dma((experts,)),
        ]
    return pl.pallas_call(
        functools.partial(layer_kernel, (n_sp, n_tp, cap, col_len, lined)),
        out_shape=jax.ShapeDtypeStruct((rows, width), BF16),
        in_specs=[pl.BlockSpec(memory_space=pltpu.VMEM)] * 12
        + [pl.BlockSpec(memory_space=pl.ANY)] * 5,
        out_specs=pl.BlockSpec(memory_space=pltpu.VMEM),
        scratch_shapes=[
            vmem((n_sp, n_tp, 2 * (size_small + size_large) // n_tp, tokens), BF16),
            vmem((n_sp, gate_rows, tokens), F32),
            vmem((heads_small, size_small + extra_rows, tokens), BF16),
            vmem((heads_large, size_large + extra_rows, tokens), BF16),
            vmem((gate_rows, tokens), F32),
            vmem((gate_rows, tokens), F32),
            vmem((heads_small, size_small, tokens), F32),
            vmem((heads_large, size_large, tokens), F32),
            vmem((attn_width, tokens), BF16),
            vmem((tokens, attn_width), BF16),
            vmem((attn_width, width), BF16),
            vmem((width, hidden), BF16),
            vmem((width, hidden), BF16),
            vmem((hidden, width), BF16),
            vmem((cols, tokens, col_len), F32),
            vmem((cols, half_groups, rows, col_len), BF16),
            vmem((cols, half_groups, rows, col_len), BF16),
            vmem((cols, half_groups, rows, col_len), BF16),
            vmem((cols, half_groups, rows, col_len), BF16),
            vmem((rows, width), F32),
            dma((5,)),
            dma((n_sp,)),
            dma((n_sp,)),
            dma((n_sp,)),
            dma((n_sp,)),
            dma((n_sp, n_tp)),
            dma((n_sp, n_tp)),
            dma((cols,)),
            dma((cols,)),
            dma((cols, half_groups)),
            dma((cols, half_groups)),
        ]
        + tail,
        compiler_params=pltpu.CompilerParams(
            collective_id=0, has_side_effects=True, vmem_limit_bytes=60 * 1024 * 1024
        ),
    )(
        residual_in,
        query_small,
        query_large,
        key_small,
        key_large,
        value_small,
        value_large,
        forget_small,
        forget_large,
        norm_gain,
        routing.T,
        route_weight.T,
        project_small,
        project_large,
        expert_gate,
        expert_up,
        expert_down,
    )


def solution(mesh):
    in_specs = (
        P(("grp", "sp", "tp"), None),
        P(("grp", "sp"), "tp"),
        P(("grp", "sp"), "tp"),
        P(None, ("grp", "sp")),
        P(None, ("grp", "sp")),
        P(None, ("grp", "sp")),
        P(None, ("grp", "sp")),
        P("tp", ("grp", "sp")),
        P("tp", ("grp", "sp")),
        P("tp", None),
        P("tp", None),
        P(),
        P(("sp", "tp"), None, None),
        P(("sp", "tp"), None, None),
        P(("sp", "tp"), None, None),
        P(("grp", "sp", "tp"), None),
        P(("grp", "sp", "tp"), None),
    )
    out_specs = P(("grp", "sp", "tp"), None)
    return jax.shard_map(shards, mesh=mesh, in_specs=in_specs, out_specs=out_specs, check_vma=False)
```

```python
import functools
import math

import jax
import jax.numpy as jnp
from jax import lax
from jax.experimental import pallas as pl
from jax.experimental.pallas import tpu as pltpu
from jax.sharding import PartitionSpec as P

MESH = pl.DeviceIdType.MESH
F32 = jnp.float32
BF16 = jnp.bfloat16


def layer_kernel(dims, *refs):
    (
        residual_in,
        query_small,
        query_large,
        key_small,
        key_large,
        value_small,
        value_large,
        forget_small,
        forget_large,
        norm_gain,
        routing,
        route_weight,
        project_small,
        project_large,
        expert_gate,
        expert_up,
        expert_down,
        out,
        kv,
        gates,
        turned_q_small,
        turned_q_large,
        top_ref,
        total_ref,
        acc_small,
        acc_large,
        attn_t,
        attn,
        proj_w,
        gate_w,
        up_w,
        down_w,
        proj_f32,
        pair_out,
        pair_in,
        cross_out,
        cross_in,
        resid_ref,
        weight_sem,
        kv_send,
        kv_recv,
        gate_send,
        gate_recv,
        share_send,
        side_recv,
        pass_recv,
        pair_send,
        pair_recv,
        cross_send,
        cross_recv,
        *tail,
    ) = refs
    n_sp, n_tp, cap, col_len, lined = dims
    experts = n_sp * n_tp
    seq = lax.axis_index("sp")
    ten = lax.axis_index("tp")
    me = seq * n_tp + ten
    parity = lax.rem(ten, 2)
    partner = ten + 1 - 2 * parity
    tokens = query_small.shape[0]
    size_small, size_large = key_small.shape[0], key_large.shape[0]
    heads_small, heads_large = forget_small.shape[0], forget_large.shape[0]
    width_small = heads_small * size_small
    rows, width = residual_in.shape
    piece_small, piece_large = size_small // n_tp, size_large // n_tp
    cols = width // col_len
    half_groups = n_tp // 2
    my_group = lax.div(ten, 2)

    loads = [
        pltpu.make_async_copy(project_small, proj_w.at[pl.ds(0, width_small)], weight_sem.at[0]),
        pltpu.make_async_copy(
            project_large,
            proj_w.at[pl.ds(width_small, heads_large * size_large)],
            weight_sem.at[1],
        ),
        pltpu.make_async_copy(expert_gate.at[0], gate_w, weight_sem.at[2]),
        pltpu.make_async_copy(expert_up.at[0], up_w, weight_sem.at[3]),
        pltpu.make_async_copy(expert_down.at[0], down_w, weight_sem.at[4]),
    ]
    barrier = pltpu.get_barrier_semaphore()

    def greet(peer_sp, peer_tp):
        pl.semaphore_signal(
            barrier, inc=1, device_id={"sp": peer_sp, "tp": peer_tp}, device_id_type=MESH
        )

    def greet_all(i, carry):
        peer = lax.rem(me + i, experts)
        greet(lax.div(peer, n_tp), lax.rem(peer, n_tp))
        return carry

    lax.fori_loop(1, experts, greet_all, 0)

    for p in range(n_tp):
        base = 0
        for source, piece in (
            (key_small, piece_small),
            (key_large, piece_large),
            (value_small, piece_small),
            (value_large, piece_large),
        ):
            kv[seq, p, base : base + piece, :] = source[p * piece : (p + 1) * piece, :]
            base += piece
    top_count = routing.shape[0]
    gate_rows = gates.shape[1]
    gates[seq] = jnp.zeros(gates.shape[1:], F32)
    gates[seq, :heads_small, :tokens] = forget_small[...]
    gates[seq, heads_small : heads_small + heads_large, :tokens] = forget_large[...]
    gates[seq, :top_count, tokens : tokens + rows] = routing[...].astype(F32)

    pl.semaphore_wait(barrier, experts - 1)

    def kv_copy(source, target, slot):
        return pltpu.make_async_remote_copy(
            src_ref=kv.at[source, ten],
            dst_ref=kv.at[source, ten],
            send_sem=kv_send.at[slot],
            recv_sem=kv_recv.at[source],
            device_id={"sp": target, "tp": ten},
            device_id_type=MESH,
        )

    def gate_copy(source, target, slot):
        return pltpu.make_async_remote_copy(
            src_ref=gates.at[source],
            dst_ref=gates.at[source],
            send_sem=gate_send.at[slot],
            recv_sem=gate_recv.at[source],
            device_id={"sp": target, "tp": ten},
            device_id_type=MESH,
        )

    def other_group(hop):
        return lax.rem(my_group + hop, half_groups)

    def side_copy(source, group_from, group_to):
        piece = kv.at[source, 2 * group_from + parity]
        return pltpu.make_async_remote_copy(
            src_ref=piece,
            dst_ref=piece,
            send_sem=share_send.at[source],
            recv_sem=side_recv.at[source, group_from],
            device_id={"sp": seq, "tp": 2 * group_to + parity},
            device_id_type=MESH,
        )

    def pass_copy(source, piece):
        return pltpu.make_async_remote_copy(
            src_ref=kv.at[source, piece],
            dst_ref=kv.at[source, piece],
            send_sem=share_send.at[source],
            recv_sem=pass_recv.at[source],
            device_id={"sp": seq, "tp": partner},
            device_id_type=MESH,
        )

    def for_mates(action):
        for i in range(1, n_tp):
            action(lax.rem(ten + i, n_tp))

    def send_kv(target, carry):
        gate_copy(seq, target, target).start()
        kv_copy(seq, target, target).start()
        return carry

    def send_gates(target, carry):
        gate_copy(seq, target, target).start()
        return carry

    lax.fori_loop(seq + 1, n_sp, send_kv, 0)
    if lined:
        lax.fori_loop(0, seq, send_gates, 0)
    for load in loads:
        load.start()

    lanes = lax.broadcasted_iota(jnp.int32, (rows, experts), 1)
    same = lax.broadcasted_iota(jnp.int32, (rows, rows), 0) == lax.broadcasted_iota(
        jnp.int32, (rows, rows), 1
    )

    def column(ref, k):
        return jnp.sum(
            jnp.where(same, ref[k : k + 1, :].astype(F32), 0.0), axis=1, keepdims=True
        )

    def route_places(routes):
        hot = [(route == lanes.astype(F32)).astype(F32) for route in routes]
        named = sum(hot).astype(BF16)
        below = (
            lax.broadcasted_iota(jnp.int32, (rows, rows), 0)
            > lax.broadcasted_iota(jnp.int32, (rows, rows), 1)
        ).astype(F32)
        earlier = jnp.dot(below.astype(BF16), named, preferred_element_type=F32)
        return [
            route * cap + jnp.sum(earlier * one, axis=1, keepdims=True)
            for route, one in zip(routes, hot)
        ]

    if lined:
        (
            pick_ref,
            choose,
            lane_rows,
            lane_scale,
            outgoing,
            arrived,
            scale_out,
            scale_in,
            result,
            returned,
            lane_send,
            lane_recv,
            disp_send,
            disp_recv,
            back_send,
            back_recv,
        ) = tail
        plane_slots = n_tp * cap
        slot_lane = lax.broadcasted_iota(jnp.int32, (rows, plane_slots), 1)

        def prepare(z):
            known = gates[z][:, tokens : tokens + rows]
            spots = (slot_lane + seq * plane_slots).astype(F32)
            both = jnp.zeros((rows, plane_slots), F32)
            for place in route_places([column(known, k) for k in range(top_count)]):
                both = both + (spots == place).astype(F32)
            choose[z] = both.T.astype(BF16)

        prepare(seq)
    else:
        (
            pick_ref,
            outgoing,
            arrived,
            scale_out,
            scale_in,
            result,
            returned,
            disp_send,
            disp_recv,
            back_send,
            back_recv,
        ) = tail

    spots = lax.broadcasted_iota(jnp.int32, (rows, experts * cap), 1).astype(F32)
    places = route_places([column(routing, k) for k in range(top_count)])
    for k in range(top_count):
        pick_ref[k * rows : (k + 1) * rows, :] = (spots == places[k]).astype(F32).astype(BF16)

    extra_rows = turned_q_small.shape[1] - size_small

    def fold(size):
        power = 2.0 ** math.floor(math.log2(size**-0.5))
        return power, size**-0.5 / power

    extra_row = lax.broadcasted_iota(jnp.int32, (extra_rows, tokens), 0)
    for kind in range(2):
        heads, size, offset, source, q_ref = (
            (heads_small, size_small, 0, query_small, turned_q_small),
            (heads_large, size_large, heads_small, query_large, turned_q_large),
        )[kind]
        turned = (source[...] * fold(size)[0]).astype(BF16).T
        for h in range(heads):
            chosen = (lax.rem(extra_row, gate_rows) == offset + h) & (extra_row < 3 * gate_rows)
            q_ref[h, :size, :] = turned[h * size : (h + 1) * size, :]
            q_ref[h, size:, :] = jnp.where(chosen, 1.0, 0.0).astype(BF16)
    key_base = (0, piece_small)
    value_base = (piece_small + piece_large, 2 * piece_small + piece_large)

    def attend(block, diagonal):
        block_gates = gates[block][:, :tokens]
        if diagonal:
            k_pos = lax.broadcasted_iota(jnp.int32, (tokens, tokens), 0)
            q_pos = lax.broadcasted_iota(jnp.int32, (tokens, tokens), 1)
            seen = q_pos >= k_pos
        for kind in range(2):
            heads, size, piece, offset, q_ref, acc = (
                (heads_small, size_small, piece_small, 0, turned_q_small, acc_small),
                (heads_large, size_large, piece_large, heads_small, turned_q_large, acc_large),
            )[kind]
            kb, vb = key_base[kind], value_base[kind]
            rest = fold(size)[1]
            shift = block_gates * (-1.0 / rest)
            first = shift.astype(BF16).astype(F32)
            second = (shift - first).astype(BF16).astype(F32)
            pieces = [first, second, shift - first - second]
            if extra_rows > 3 * gate_rows:
                pieces.append(jnp.zeros((extra_rows - 3 * gate_rows, tokens), F32))
            keys = jnp.concatenate(
                [kv[block, p, kb : kb + piece, :] for p in range(n_tp)]
                + [jnp.concatenate(pieces, axis=0).astype(BF16)],
                axis=0,
            ).T
            values = jnp.concatenate(
                [kv[block, p, vb : vb + piece, :] for p in range(n_tp)], axis=0
            )
            for h in range(heads):
                g = slice(offset + h, offset + h + 1)
                scores = jnp.dot(keys, q_ref[h], preferred_element_type=F32)
                if diagonal:
                    scores = jnp.where(seen, scores, -jnp.inf)
                block_top = jnp.max(scores, axis=0, keepdims=True)
                top = block_top if diagonal else jnp.maximum(top_ref[g, :], block_top)
                below_top = scores - top
                weights = jnp.exp(below_top if rest == 1.0 else below_top * rest)
                total = jnp.sum(weights, axis=0, keepdims=True)
                mixed = jnp.dot(values, weights.astype(BF16), preferred_element_type=F32)
                if not diagonal:
                    factor = jnp.exp((top_ref[g, :] - top) * rest)
                    total = total_ref[g, :] * factor + total
                    mixed = acc[h] * factor + mixed
                top_ref[g, :] = top
                total_ref[g, :] = total
                acc[h] = mixed

    def share_out(block):
        kv_copy(block, seq, block).wait_recv()
        for hop in range(1, half_groups):
            side_copy(block, my_group, other_group(hop)).start()
        pass_copy(block, ten).start()

    def hand_on(block):
        for hop in range(1, half_groups):
            group = other_group(hop)
            side_copy(block, group, group).wait_recv()
            pass_copy(block, 2 * group + parity).start()

    attend(seq, True)

    @pl.when(seq > 0)
    def _():
        share_out(seq - 1)

    if lined:
        for i in range(1, n_sp):
            z = lax.rem(seq + i, n_sp)
            gate_copy(z, seq, z).wait_recv()
            prepare(z)

    def earlier_block(i, carry):
        @pl.when(i < seq)
        def _():
            share_out(seq - 1 - i)

        @pl.when(i <= seq)
        def _():
            hand_on(seq - i)

        @pl.when(i > 1)
        def _():
            block = seq + 1 - i
            pass_copy(block, pl.ds(0, half_groups)).wait_recv()
            if not lined:
                gate_copy(block, seq, block).wait_recv()
            attend(block, False)

        return carry

    lax.fori_loop(1, jnp.where(seq > 0, seq + 2, 1), earlier_block, 0)

    for h in range(heads_small):
        attn_t[h * size_small : (h + 1) * size_small, :] = (
            acc_small[h] * (1.0 / total_ref[h : h + 1, :])
        ).astype(BF16)
    for h in range(heads_large):
        first = width_small + h * size_large
        g = heads_small + h
        attn_t[first : first + size_large, :] = (
            acc_large[h] * (1.0 / total_ref[g : g + 1, :])
        ).astype(BF16)
    attn[...] = attn_t[...].T

    def row_ds(group, par):
        return pl.ds(pl.multiple_of((2 * group + par) * rows, rows), rows)

    def pair_copy(c):
        return pltpu.make_async_remote_copy(
            src_ref=pair_out.at[c],
            dst_ref=pair_in.at[c],
            send_sem=pair_send.at[0],
            recv_sem=pair_recv.at[c],
            device_id={"sp": seq, "tp": partner},
            device_id_type=MESH,
        )

    def cross_copy(c, group, source, slot, part=None):
        return pltpu.make_async_remote_copy(
            src_ref=cross_out.at[c, group],
            dst_ref=cross_in.at[c, source],
            send_sem=cross_send.at[slot],
            recv_sem=cross_recv.at[c if part is None else part, source],
            device_id={"sp": seq, "tp": 2 * group + parity},
            device_id_type=MESH,
        )

    for load in loads[:2]:
        load.wait()
    for c in range(cols):
        part = jnp.dot(
            attn[...], proj_w[:, c * col_len : (c + 1) * col_len], preferred_element_type=F32
        )
        proj_f32[c] = part
        for group in range(half_groups):
            pair_out[c, group] = proj_f32[c, row_ds(group, 1 - parity), :].astype(BF16)
        pair_copy(c).start()
    for c in range(cols):
        pair_copy(c).wait_recv()
        for hop in range(1, half_groups):
            group = lax.rem(my_group + hop, half_groups)
            cross_out[c, group] = (
                proj_f32[c, row_ds(group, parity), :] + pair_in[c, group].astype(F32)
            ).astype(BF16)
            cross_copy(c, group, my_group, hop).start()
    def own_rows(c, span, squares):
        value = proj_f32[c, row_ds(my_group, parity), :] + pair_in[c, my_group].astype(F32)
        for hop in range(1, half_groups):
            source = lax.rem(my_group + hop, half_groups)
            cross_copy(c, source, source, hop).wait_recv()
            value = value + cross_in[c, source].astype(F32)
        value = value + residual_in[:, span].astype(F32)
        resid_ref[:, span] = value
        squares = squares + jnp.sum(value * value, axis=1, keepdims=True)
        return value, squares

    def finish():
        for c in range(cols):
            span = slice(c * col_len, (c + 1) * col_len)
            picked = jnp.dot(pick_ref[...], returned[:, span], preferred_element_type=F32)
            value = resid_ref[:, span]
            for k in range(top_count):
                value = value + picked[k * rows : (k + 1) * rows] * column(route_weight, k)
            out[:, span] = value.astype(BF16)

    def scale_parts(squares):
        scale = lax.rsqrt(squares * (1.0 / width) + 1e-06)
        first = scale.astype(BF16).astype(F32)
        second = (scale - first).astype(BF16).astype(F32)
        third = scale - first - second
        lane = lax.broadcasted_iota(jnp.int32, (rows, 128), 1)
        parts = jnp.where(lane == 0, first, 0.0)
        parts = jnp.where(lane == 1, second, parts)
        return jnp.where(lane == 2, third, parts).astype(BF16)

    if lined:

        def slot_ds(member):
            return pl.ds(pl.multiple_of(member * cap, cap), cap)

        def lane_copy(z, c, up):
            ref = lane_rows.at[z, c] if c < cols else lane_scale.at[z]
            return pltpu.make_async_remote_copy(
                src_ref=ref,
                dst_ref=ref,
                send_sem=lane_send.at[up, z, 1 if c == cols else 0],
                recv_sem=lane_recv.at[z, c],
                device_id={"sp": seq + 2 * up - 1, "tp": ten},
                device_id_type=MESH,
            )

        def disp_copy(z, c, peer, sender):
            source, target = (
                (outgoing.at[z, c], arrived.at[z, c])
                if c < cols
                else (scale_out.at[z], scale_in.at[z])
            )
            return pltpu.make_async_remote_copy(
                src_ref=source.at[slot_ds(peer)],
                dst_ref=target.at[slot_ds(sender)],
                send_sem=disp_send.at[z, 1 if c == cols else 0],
                recv_sem=disp_recv.at[z, c],
                device_id={"sp": seq, "tp": peer},
                device_id_type=MESH,
            )

        def back_copy(z, peer):
            return pltpu.make_async_remote_copy(
                src_ref=result.at[z, slot_ds(peer)],
                dst_ref=returned.at[slot_ds(me)],
                send_sem=back_send.at[0],
                recv_sem=back_recv.at[0],
                device_id={"sp": z, "tp": peer},
                device_id_type=MESH,
            )

        mates_rows = pl.ds(0, (n_tp - 1) * cap)
        next_mate = lax.rem(ten + 1, n_tp)

        def bulk(source, target, send_sem, recv_sem):
            return pltpu.make_async_remote_copy(
                src_ref=source,
                dst_ref=target,
                send_sem=send_sem,
                recv_sem=recv_sem,
                device_id={"sp": seq, "tp": next_mate},
                device_id_type=MESH,
            )

        def disp_came(z, c):
            ref = arrived.at[z, c, mates_rows] if c < cols else scale_in.at[z, mates_rows]
            bulk(ref, ref, disp_send.at[z, 0], disp_recv.at[z, c]).wait_recv()

        def sent_plane(z):
            ref = outgoing.at[z, :, mates_rows]
            bulk(ref, ref, disp_send.at[z, 0], disp_recv.at[z, 0]).wait_send()
            ref = scale_out.at[z, mates_rows]
            bulk(ref, ref, disp_send.at[z, 1], disp_recv.at[z, 0]).wait_send()

        def sent_lane(z, up):
            @pl.when(seq + 1 < n_sp if up else seq > 0)
            def _():
                bulk(
                    lane_rows.at[z], lane_rows.at[z], lane_send.at[up, z, 0], lane_recv.at[z, 0]
                ).wait_send()
                bulk(
                    lane_scale.at[z], lane_scale.at[z], lane_send.at[up, z, 1], lane_recv.at[z, 0]
                ).wait_send()

        def go_on(z, c, up):
            if up:

                @pl.when(seq + 1 < n_sp)
                def _():
                    lane_copy(z, c, 1).start()
            else:

                @pl.when(seq > 0)
                def _():
                    lane_copy(z, c, 0).start()

        def place_rows(z, c):
            values = lane_rows[z, c] if c < cols else lane_scale[z]
            placed = jnp.dot(choose[z], values, preferred_element_type=F32).astype(BF16)
            if c < cols:
                outgoing[z, c] = placed
            else:
                scale_out[z] = placed
            for_mates(lambda peer: disp_copy(z, c, peer, ten).start())
            if c < cols:
                arrived[z, c, slot_ds(ten), :] = outgoing[z, c, slot_ds(ten), :]
            else:
                scale_in[z, slot_ds(ten), :] = scale_out[z, slot_ds(ten), :]

        def at_pair(k, action, own):
            low, high = seq - k - 1, seq + k

            @pl.when(low >= 0)
            def _():
                action(low, 1)

            if k > 0:

                @pl.when(high < n_sp)
                def _():
                    action(high, 0)
            elif own is not None:
                own()

        def take(k, c):
            def one(z, up):
                lane_copy(z, c, up).wait_recv()
                go_on(z, c, up)
                place_rows(z, c)

            at_pair(k, one, None)

        def serve(*blocks):
            count = len(blocks) * plane_slots
            gate_part = jnp.zeros((count, gate_w.shape[1]), F32)
            up_part = jnp.zeros((count, gate_w.shape[1]), F32)
            for c in range(cols):
                for z in blocks:
                    disp_came(z, c)
                came = jnp.concatenate([arrived[z, c] for z in blocks], axis=0)
                depth = slice(c * col_len, (c + 1) * col_len)
                gate_part = gate_part + jnp.dot(came, gate_w[depth, :], preferred_element_type=F32)
                up_part = up_part + jnp.dot(came, up_w[depth, :], preferred_element_type=F32)
            for z in blocks:
                disp_came(z, cols)
            row_scale = jnp.concatenate(
                [jnp.sum(scale_in[z].astype(F32), axis=1, keepdims=True) for z in blocks], axis=0
            )
            gate_part, up_part = gate_part * row_scale, up_part * row_scale
            hidden = (gate_part / (1.0 + jnp.exp(-gate_part)) * up_part).astype(BF16)
            for c in range(cols):
                span = slice(c * col_len, (c + 1) * col_len)
                made = jnp.dot(hidden, down_w[:, span], preferred_element_type=F32).astype(BF16)
                for i, z in enumerate(blocks):
                    result[z, :, span] = made[i * plane_slots : (i + 1) * plane_slots]
            for z in blocks:
                for_mates(lambda peer: back_copy(z, peer).start())

                @pl.when(z != seq)
                def _():
                    back_copy(z, ten).start()

                @pl.when(z == seq)
                def _():
                    returned[slot_ds(me), :] = result[z, slot_ds(ten), :]

        def serve_pair(k):
            low, high = seq - k - 1, seq + k
            both = jnp.logical_and(low >= 0, high < n_sp)

            if 2 * k + 1 < n_sp:

                @pl.when(both)
                def _():
                    serve(low, high)

            @pl.when(jnp.logical_not(both))
            def _():
                @pl.when(jnp.logical_or(low >= 0, high < n_sp))
                def _():
                    serve(jnp.where(low >= 0, low, high))

        squares = jnp.zeros((rows, 1), F32)
        gain = norm_gain[...].astype(F32).reshape(1, width)
        for c in range(cols):
            span = slice(c * col_len, (c + 1) * col_len)
            value, squares = own_rows(c, span, squares)
            lane_rows[seq, c] = (value * gain[:, span]).astype(BF16)
            go_on(seq, c, 0)
            go_on(seq, c, 1)
            place_rows(seq, c)
            take(0, c)
        lane_scale[seq] = scale_parts(squares)
        go_on(seq, cols, 0)
        go_on(seq, cols, 1)
        place_rows(seq, cols)
        take(0, cols)
        for load in loads[2:]:
            load.wait()

        def sent_own():
            sent_plane(seq)
            sent_lane(seq, 0)
            sent_lane(seq, 1)

        def sent_block(z, up):
            sent_plane(z)
            sent_lane(z, up)

        for step in range(1, n_sp + 2):
            moving = step < n_sp
            if moving:
                take(step, 0)
            if moving:
                take(step, 1)
            if step <= n_sp:
                serve_pair(step - 1)
            if moving:
                for c in range(2, cols + 1):
                    take(step, c)
            if step > 1:
                at_pair(step - 2, sent_block, sent_own)

        others = pl.ds(0, (experts - 1) * cap)
        bulk(
            returned.at[others], returned.at[others], back_send.at[0], back_recv.at[0]
        ).wait_recv()
        finish()
        bulk(
            returned.at[others], returned.at[others], back_send.at[0], back_recv.at[0]
        ).wait_send()
    else:
        def slot_ds(peer):
            return pl.ds(pl.multiple_of(peer * cap, cap), cap)

        def exchange(source_ref, target_ref, send, recv, peer, sender):
            return pltpu.make_async_remote_copy(
                src_ref=source_ref.at[slot_ds(peer)],
                dst_ref=target_ref.at[slot_ds(sender)],
                send_sem=send.at[peer],
                recv_sem=recv.at[sender],
                device_id={"sp": lax.div(peer, n_tp), "tp": lax.rem(peer, n_tp)},
                device_id_type=MESH,
            )

        def part_copy(c, peer, sender):
            if c < cols:
                source_ref, target_ref = outgoing.at[c], arrived.at[c]
            else:
                source_ref, target_ref = scale_out, scale_in
            return exchange(source_ref, target_ref, disp_send.at[c], disp_recv.at[c], peer, sender)

        def for_members(plane, action):
            def one(j, carry):
                peer = plane * n_tp + lax.rem(ten + j, n_tp)

                @pl.when(peer != me)
                def _():
                    action(peer)

                return carry

            lax.fori_loop(0, n_tp, one, 0)

        slots = experts * cap
        block_rows = min(256, slots)

        def place_rows(values, c):
            for b in range(slots // block_rows):
                span = slice(b * block_rows, (b + 1) * block_rows)
                chosen = pick_ref[:rows, span]
                for k in range(1, top_count):
                    chosen = chosen + pick_ref[k * rows : (k + 1) * rows, span]
                placed = lax.dot_general(
                    chosen, values, (((0,), (0,)), ((), ())), preferred_element_type=F32
                ).astype(BF16)
                if c < cols:
                    outgoing[c, span, :] = placed
                else:
                    scale_out[span, :] = placed

            def dispatch(i, carry):
                for_members(
                    lax.rem(seq + n_sp - i, n_sp), lambda peer: part_copy(c, peer, me).start()
                )
                return carry

            lax.fori_loop(0, n_sp, dispatch, 0)

        squares = jnp.zeros((rows, 1), F32)
        gain = norm_gain[...].astype(F32).reshape(1, width)
        for c in range(cols):
            span = slice(c * col_len, (c + 1) * col_len)
            value, squares = own_rows(c, span, squares)
            place_rows((value * gain[:, span]).astype(BF16), c)
        place_rows(scale_parts(squares), cols)
        for c in range(cols):
            arrived[c, slot_ds(me), :] = outgoing[c, slot_ds(me), :]
        scale_in[slot_ds(me), :] = scale_out[slot_ds(me), :]
        for load in loads[2:]:
            load.wait()

        group_rows = n_tp * cap

        def serve(i, carry):
            plane = lax.rem(seq + i, n_sp)
            span = pl.ds(pl.multiple_of(plane * group_rows, group_rows), group_rows)
            gate_part = jnp.zeros((group_rows, gate_w.shape[1]), F32)
            up_part = jnp.zeros((group_rows, gate_w.shape[1]), F32)
            for c in range(cols):
                for_members(plane, lambda peer: part_copy(c, me, peer).wait_recv())
                came = arrived[c, span, :]
                depth = slice(c * col_len, (c + 1) * col_len)
                gate_part = gate_part + jnp.dot(came, gate_w[depth, :], preferred_element_type=F32)
                up_part = up_part + jnp.dot(came, up_w[depth, :], preferred_element_type=F32)
            for_members(plane, lambda peer: part_copy(cols, me, peer).wait_recv())
            row_scale = jnp.sum(scale_in[span, :].astype(F32), axis=1, keepdims=True)
            gate_part, up_part = gate_part * row_scale, up_part * row_scale
            hidden = (gate_part / (1.0 + jnp.exp(-gate_part)) * up_part).astype(BF16)
            result[span, :] = jnp.dot(hidden, down_w[...], preferred_element_type=F32).astype(BF16)
            for_members(
                plane,
                lambda peer: exchange(result, returned, back_send, back_recv, peer, me).start(),
            )
            return carry

        lax.fori_loop(0, n_sp, serve, 0)
        returned[slot_ds(me), :] = result[slot_ds(me), :]

        def collect(i, carry):
            peer = lax.rem(me + i, experts)
            exchange(result, returned, back_send, back_recv, me, peer).wait_recv()
            return carry

        lax.fori_loop(1, experts, collect, 0)
        finish()

        def sent_rows(i, carry):
            peer = lax.rem(me + i, experts)
            for c in range(cols + 1):
                part_copy(c, peer, me).wait_send()
            exchange(result, returned, back_send, back_recv, peer, me).wait_send()
            return carry

        lax.fori_loop(1, experts, sent_rows, 0)

    def sent_kv(target, carry):
        gate_copy(seq, target, target).wait_send()
        kv_copy(seq, target, target).wait_send()
        return carry

    lax.fori_loop(seq + 1, n_sp, sent_kv, 0)
    if lined:

        def sent_gates(target, carry):
            gate_copy(seq, target, target).wait_send()
            return carry

        lax.fori_loop(0, seq, sent_gates, 0)

    def sent_fwd(block, carry):
        pass_copy(block, pl.ds(0, n_tp - 1)).wait_send()
        return carry

    lax.fori_loop(0, seq, sent_fwd, 0)
    pltpu.make_async_remote_copy(
        src_ref=pair_out,
        dst_ref=pair_in,
        send_sem=pair_send.at[0],
        recv_sem=pair_recv.at[0],
        device_id={"sp": seq, "tp": partner},
        device_id_type=MESH,
    ).wait_send()
    for hop in range(1, half_groups):
        cross_copy(pl.ds(0, cols), lax.rem(my_group + hop, half_groups), my_group, hop, 0).wait_send()


def shards(
    residual_in,
    query_small,
    query_large,
    key_small,
    key_large,
    value_small,
    value_large,
    forget_small,
    forget_large,
    project_small,
    project_large,
    norm_gain,
    expert_gate,
    expert_up,
    expert_down,
    routing,
    route_weight,
):
    n_sp, n_tp = lax.axis_size("sp"), lax.axis_size("tp")
    experts = n_sp * n_tp
    rows, width = residual_in.shape
    top_count = routing.shape[1]
    tokens = query_small.shape[0]
    size_small, size_large = key_small.shape[0], key_large.shape[0]
    heads_small, heads_large = forget_small.shape[0], forget_large.shape[0]
    heads = heads_small + heads_large
    gate_rows = -(-max(heads, 2 * top_count) // 8) * 8
    extra_rows = -(-3 * gate_rows // 16) * 16
    capacity = max(2, 2 * rows * top_count // experts)
    cap = -(-capacity // 16) * 16
    col_len = min(width, 512)
    cols = width // col_len
    hidden = expert_gate.shape[2]
    attn_width = heads_small * size_small + heads_large * size_large
    half_groups = n_tp // 2
    slots = experts * cap
    group = n_tp * cap
    lined = n_tp * capacity >= rows
    vmem, dma = pltpu.VMEM, pltpu.SemaphoreType.DMA
    if lined:
        tail = [
            vmem((top_count * rows, slots), BF16),
            vmem((n_sp, group, rows), BF16),
            vmem((n_sp, cols, rows, col_len), BF16),
            vmem((n_sp, rows, 128), BF16),
            vmem((n_sp, cols, group, col_len), BF16),
            vmem((n_sp, cols, group, col_len), BF16),
            vmem((n_sp, group, 128), BF16),
            vmem((n_sp, group, 128), BF16),
            vmem((n_sp, group, width), BF16),
            vmem((slots, width), BF16),
            dma((2, n_sp, 2)),
            dma((n_sp, cols + 1)),
            dma((n_sp, 2)),
            dma((n_sp, cols + 1)),
            dma((1,)),
            dma((1,)),
        ]
    else:
        tail = [
            vmem((top_count * rows, slots), BF16),
            vmem((cols, slots, col_len), BF16),
            vmem((cols, slots, col_len), BF16),
            vmem((slots, 128), BF16),
            vmem((slots, 128), BF16),
            vmem((slots, width), BF16),
            vmem((slots, width), BF16),
            dma((cols + 1, experts)),
            dma((cols + 1, experts)),
            dma((experts,)),
            dma((experts,)),
        ]
    return pl.pallas_call(
        functools.partial(layer_kernel, (n_sp, n_tp, cap, col_len, lined)),
        out_shape=jax.ShapeDtypeStruct((rows, width), BF16),
        in_specs=[pl.BlockSpec(memory_space=pltpu.VMEM)] * 12
        + [pl.BlockSpec(memory_space=pl.ANY)] * 5,
        out_specs=pl.BlockSpec(memory_space=pltpu.VMEM),
        scratch_shapes=[
            vmem((n_sp, n_tp, 2 * (size_small + size_large) // n_tp, tokens), BF16),
            vmem((n_sp, gate_rows, tokens + -(-rows // 128) * 128), F32),
            vmem((heads_small, size_small + extra_rows, tokens), BF16),
            vmem((heads_large, size_large + extra_rows, tokens), BF16),
            vmem((gate_rows, tokens), F32),
            vmem((gate_rows, tokens), F32),
            vmem((heads_small, size_small, tokens), F32),
            vmem((heads_large, size_large, tokens), F32),
            vmem((attn_width, tokens), BF16),
            vmem((tokens, attn_width), BF16),
            vmem((attn_width, width), BF16),
            vmem((width, hidden), BF16),
            vmem((width, hidden), BF16),
            vmem((hidden, width), BF16),
            vmem((cols, tokens, col_len), F32),
            vmem((cols, half_groups, rows, col_len), BF16),
            vmem((cols, half_groups, rows, col_len), BF16),
            vmem((cols, half_groups, rows, col_len), BF16),
            vmem((cols, half_groups, rows, col_len), BF16),
            vmem((rows, width), F32),
            dma((5,)),
            dma((n_sp,)),
            dma((n_sp,)),
            dma((n_sp,)),
            dma((n_sp,)),
            dma((n_sp,)),
            dma((n_sp, half_groups)),
            dma((n_sp,)),
            dma((1,)),
            dma((cols,)),
            dma((half_groups,)),
            dma((cols, half_groups)),
        ]
        + tail,
        compiler_params=pltpu.CompilerParams(
            collective_id=0, has_side_effects=True, vmem_limit_bytes=60 * 1024 * 1024
        ),
    )(
        residual_in,
        query_small,
        query_large,
        key_small,
        key_large,
        value_small,
        value_large,
        forget_small,
        forget_large,
        norm_gain,
        routing.T,
        route_weight.T,
        project_small,
        project_large,
        expert_gate,
        expert_up,
        expert_down,
    )


def solution(mesh):
    in_specs = (
        P(("grp", "sp", "tp"), None),
        P(("grp", "sp"), "tp"),
        P(("grp", "sp"), "tp"),
        P(None, ("grp", "sp")),
        P(None, ("grp", "sp")),
        P(None, ("grp", "sp")),
        P(None, ("grp", "sp")),
        P("tp", ("grp", "sp")),
        P("tp", ("grp", "sp")),
        P("tp", None),
        P("tp", None),
        P(),
        P(("sp", "tp"), None, None),
        P(("sp", "tp"), None, None),
        P(("sp", "tp"), None, None),
        P(("grp", "sp", "tp"), None),
        P(("grp", "sp", "tp"), None),
    )
    out_specs = P(("grp", "sp", "tp"), None)
    return jax.shard_map(shards, mesh=mesh, in_specs=in_specs, out_specs=out_specs, check_vma=False)
```

```python
import functools
import math

import jax
import jax.numpy as jnp
from jax import lax
from jax.experimental import pallas as pl
from jax.experimental.pallas import tpu as pltpu
from jax.sharding import PartitionSpec as P

MESH = pl.DeviceIdType.MESH
F32 = jnp.float32
BF16 = jnp.bfloat16


def layer_kernel(dims, *refs):
    given, refs = refs[:12], refs[12:]
    (
        project_small,
        project_large,
        expert_gate,
        expert_up,
        expert_down,
        out,
        residual_in,
        query_small,
        query_large,
        key_small,
        key_large,
        value_small,
        value_large,
        forget_small,
        forget_large,
        norm_gain,
        routing,
        route_weight,
        kv,
        gates,
        turned_q_small,
        turned_q_large,
        top_ref,
        total_ref,
        acc_small,
        acc_large,
        attn_t,
        attn,
        proj_w,
        gate_w,
        up_w,
        down_w,
        proj_f32,
        pair_out,
        pair_in,
        cross_out,
        cross_in,
        resid_ref,
        weight_sem,
        given_sem,
        kv_send,
        kv_recv,
        gate_send,
        gate_recv,
        share_send,
        side_recv,
        pass_recv,
        pair_send,
        pair_recv,
        cross_send,
        cross_recv,
        *tail,
    ) = refs
    n_sp, n_tp, cap, col_len, lined = dims
    held = (
        residual_in,
        query_small,
        query_large,
        key_small,
        key_large,
        value_small,
        value_large,
        forget_small,
        forget_large,
        norm_gain,
        routing,
        route_weight,
    )
    fetches = [
        pltpu.make_async_copy(source, target, given_sem.at[i])
        for i, (source, target) in enumerate(zip(given, held))
    ]
    early, queries, late = (3, 4, 5, 6, 7, 8, 10, 11), (1, 2), (0, 9)
    for i in early + queries + late:
        fetches[i].start()
    experts = n_sp * n_tp
    seq = lax.axis_index("sp")
    ten = lax.axis_index("tp")
    me = seq * n_tp + ten
    parity = lax.rem(ten, 2)
    partner = ten + 1 - 2 * parity
    tokens = query_small.shape[0]
    size_small, size_large = key_small.shape[0], key_large.shape[0]
    heads_small, heads_large = forget_small.shape[0], forget_large.shape[0]
    width_small = heads_small * size_small
    rows, width = residual_in.shape
    piece_small, piece_large = size_small // n_tp, size_large // n_tp
    cols = width // col_len
    half_groups = n_tp // 2
    my_group = lax.div(ten, 2)

    loads = [
        pltpu.make_async_copy(project_small, proj_w.at[pl.ds(0, width_small)], weight_sem.at[0]),
        pltpu.make_async_copy(
            project_large,
            proj_w.at[pl.ds(width_small, heads_large * size_large)],
            weight_sem.at[1],
        ),
        pltpu.make_async_copy(expert_gate.at[0], gate_w, weight_sem.at[2]),
        pltpu.make_async_copy(expert_up.at[0], up_w, weight_sem.at[3]),
        pltpu.make_async_copy(expert_down.at[0], down_w, weight_sem.at[4]),
    ]
    barrier = pltpu.get_barrier_semaphore()

    def greet(peer_sp, peer_tp):
        pl.semaphore_signal(
            barrier, inc=1, device_id={"sp": peer_sp, "tp": peer_tp}, device_id_type=MESH
        )

    def greet_all(i, carry):
        peer = lax.rem(me + i, experts)
        greet(lax.div(peer, n_tp), lax.rem(peer, n_tp))
        return carry

    lax.fori_loop(1, experts, greet_all, 0)
    for i in early:
        fetches[i].wait()

    for p in range(n_tp):
        base = 0
        for source, piece in (
            (key_small, piece_small),
            (key_large, piece_large),
            (value_small, piece_small),
            (value_large, piece_large),
        ):
            kv[seq, p, base : base + piece, :] = source[p * piece : (p + 1) * piece, :]
            base += piece
    top_count = routing.shape[0]
    gate_rows = gates.shape[1]
    gates[seq] = jnp.zeros(gates.shape[1:], F32)
    gates[seq, :heads_small, :tokens] = forget_small[...]
    gates[seq, heads_small : heads_small + heads_large, :tokens] = forget_large[...]
    gates[seq, :top_count, tokens : tokens + rows] = routing[...].astype(F32)

    pl.semaphore_wait(barrier, experts - 1)

    def kv_copy(source, target, slot):
        return pltpu.make_async_remote_copy(
            src_ref=kv.at[source, ten],
            dst_ref=kv.at[source, ten],
            send_sem=kv_send.at[slot],
            recv_sem=kv_recv.at[source],
            device_id={"sp": target, "tp": ten},
            device_id_type=MESH,
        )

    def gate_copy(source, target, slot):
        return pltpu.make_async_remote_copy(
            src_ref=gates.at[source],
            dst_ref=gates.at[source],
            send_sem=gate_send.at[slot],
            recv_sem=gate_recv.at[source],
            device_id={"sp": target, "tp": ten},
            device_id_type=MESH,
        )

    def other_group(hop):
        return lax.rem(my_group + hop, half_groups)

    def side_copy(source, group_from, group_to):
        piece = kv.at[source, 2 * group_from + parity]
        return pltpu.make_async_remote_copy(
            src_ref=piece,
            dst_ref=piece,
            send_sem=share_send.at[source],
            recv_sem=side_recv.at[source, group_from],
            device_id={"sp": seq, "tp": 2 * group_to + parity},
            device_id_type=MESH,
        )

    def pass_copy(source, piece):
        return pltpu.make_async_remote_copy(
            src_ref=kv.at[source, piece],
            dst_ref=kv.at[source, piece],
            send_sem=share_send.at[source],
            recv_sem=pass_recv.at[source],
            device_id={"sp": seq, "tp": partner},
            device_id_type=MESH,
        )

    def for_mates(action):
        for i in range(1, n_tp):
            action(lax.rem(ten + i, n_tp))

    def send_kv(target, carry):
        kv_copy(seq, target, target).start()
        return carry

    def send_gates(target, carry):
        gate_copy(seq, target, target).start()
        return carry

    lax.fori_loop(seq + 1, n_sp, send_gates, 0)
    lax.fori_loop(seq + 1, jnp.minimum(seq + 2, n_sp), send_kv, 0)
    if lined:
        lax.fori_loop(0, seq, send_gates, 0)
    for load in loads:
        load.start()

    lanes = lax.broadcasted_iota(jnp.int32, (rows, experts), 1)
    same = lax.broadcasted_iota(jnp.int32, (rows, rows), 0) == lax.broadcasted_iota(
        jnp.int32, (rows, rows), 1
    )

    def column(ref, k):
        return jnp.sum(
            jnp.where(same, ref[k : k + 1, :].astype(F32), 0.0), axis=1, keepdims=True
        )

    def route_places(routes):
        hot = [(route == lanes.astype(F32)).astype(F32) for route in routes]
        named = sum(hot).astype(BF16)
        below = (
            lax.broadcasted_iota(jnp.int32, (rows, rows), 0)
            > lax.broadcasted_iota(jnp.int32, (rows, rows), 1)
        ).astype(F32)
        earlier = jnp.dot(below.astype(BF16), named, preferred_element_type=F32)
        return [
            route * cap + jnp.sum(earlier * one, axis=1, keepdims=True)
            for route, one in zip(routes, hot)
        ]

    if lined:
        (
            pick_ref,
            choose,
            lane_rows,
            lane_scale,
            outgoing,
            arrived,
            scale_out,
            scale_in,
            result,
            returned,
            lane_send,
            lane_recv,
            disp_send,
            disp_recv,
            back_send,
            back_recv,
        ) = tail
        plane_slots = n_tp * cap
        slot_lane = lax.broadcasted_iota(jnp.int32, (rows, plane_slots), 1)

        def prepare(z):
            known = gates[z][:, tokens : tokens + rows]
            spots = (slot_lane + seq * plane_slots).astype(F32)
            both = jnp.zeros((rows, plane_slots), F32)
            for place in route_places([column(known, k) for k in range(top_count)]):
                both = both + (spots == place).astype(F32)
            choose[z] = both.T.astype(BF16)

        prepare(seq)
    else:
        (
            pick_ref,
            outgoing,
            arrived,
            scale_out,
            scale_in,
            result,
            returned,
            disp_send,
            disp_recv,
            back_send,
            back_recv,
        ) = tail

    spots = lax.broadcasted_iota(jnp.int32, (rows, experts * cap), 1).astype(F32)
    places = route_places([column(routing, k) for k in range(top_count)])
    for k in range(top_count):
        pick_ref[k * rows : (k + 1) * rows, :] = (spots == places[k]).astype(F32).astype(BF16)

    extra_rows = turned_q_small.shape[0] - size_small

    def fold(size):
        power = 2.0 ** math.floor(math.log2(size**-0.5))
        return power, size**-0.5 / power

    for i in queries:
        fetches[i].wait()
    extra_row = lax.broadcasted_iota(jnp.int32, (extra_rows, tokens), 0)
    for kind in range(2):
        heads, size, offset, source, q_ref = (
            (heads_small, size_small, 0, query_small, turned_q_small),
            (heads_large, size_large, heads_small, query_large, turned_q_large),
        )[kind]
        turned = (source[...] * fold(size)[0]).astype(BF16).T
        for h in range(heads):
            chosen = (lax.rem(extra_row, gate_rows) == offset + h) & (extra_row < 3 * gate_rows)
            span = slice(h * tokens, (h + 1) * tokens)
            q_ref[:size, span] = turned[h * size : (h + 1) * size, :]
            q_ref[size:, span] = jnp.where(chosen, 1.0, 0.0).astype(BF16)
    key_base = (0, piece_small)
    value_base = (piece_small + piece_large, 2 * piece_small + piece_large)

    def attend(block, diagonal):
        block_gates = gates[block][:, :tokens]

        def seen(heads):
            shape = (tokens, heads * tokens)
            k_pos = lax.broadcasted_iota(jnp.int32, shape, 0)
            q_pos = lax.rem(lax.broadcasted_iota(jnp.int32, shape, 1), tokens)
            return q_pos >= k_pos

        for kind in range(2):
            heads, size, piece, offset, q_ref, acc = (
                (heads_small, size_small, piece_small, 0, turned_q_small, acc_small),
                (heads_large, size_large, piece_large, heads_small, turned_q_large, acc_large),
            )[kind]
            kb, vb = key_base[kind], value_base[kind]
            rest = fold(size)[1]
            shift = block_gates * (-1.0 / rest)
            first = shift.astype(BF16).astype(F32)
            second = (shift - first).astype(BF16).astype(F32)
            pieces = [first, second, shift - first - second]
            if extra_rows > 3 * gate_rows:
                pieces.append(jnp.zeros((extra_rows - 3 * gate_rows, tokens), F32))
            keys = jnp.concatenate(
                [kv[block, p, kb : kb + piece, :] for p in range(n_tp)]
                + [jnp.concatenate(pieces, axis=0).astype(BF16)],
                axis=0,
            ).T
            values = jnp.concatenate(
                [kv[block, p, vb : vb + piece, :] for p in range(n_tp)], axis=0
            )
            side = slice(offset * tokens, (offset + heads) * tokens)
            scores = jnp.dot(keys, q_ref[...], preferred_element_type=F32)
            if diagonal:
                scores = jnp.where(seen(heads), scores, -jnp.inf)
            block_top = jnp.max(scores, axis=0, keepdims=True)
            top = block_top if diagonal else jnp.maximum(top_ref[:, side], block_top)
            below_top = scores - top
            weights = jnp.exp(below_top if rest == 1.0 else below_top * rest)
            total = jnp.sum(weights, axis=0, keepdims=True)
            mixed = jnp.dot(values, weights.astype(BF16), preferred_element_type=F32)
            if not diagonal:
                factor = jnp.exp((top_ref[:, side] - top) * rest)
                total = total_ref[:, side] * factor + total
                mixed = acc[...] * factor + mixed
            top_ref[:, side] = top
            total_ref[:, side] = total
            acc[...] = mixed

    def share_out(block):
        kv_copy(block, seq, block).wait_recv()
        for hop in range(1, half_groups):
            side_copy(block, my_group, other_group(hop)).start()
        pass_copy(block, ten).start()

    def hand_on(block):
        for hop in range(1, half_groups):
            group = other_group(hop)
            side_copy(block, group, group).wait_recv()
            pass_copy(block, 2 * group + parity).start()

    attend(seq, True)
    lax.fori_loop(seq + 2, n_sp, send_kv, 0)

    def learn(distances):
        if lined:
            for i in distances:
                z = lax.rem(seq + n_sp - i, n_sp)
                gate_copy(z, seq, z).wait_recv()
                prepare(z)

    learn(range(1, n_sp))

    @pl.when(seq > 0)
    def _():
        share_out(seq - 1)

    def earlier_block(i, carry):
        @pl.when(i < seq)
        def _():
            share_out(seq - 1 - i)

        @pl.when(i <= seq)
        def _():
            hand_on(seq - i)

        @pl.when(i > 1)
        def _():
            block = seq + 1 - i
            pass_copy(block, pl.ds(0, half_groups)).wait_recv()
            if not lined:
                gate_copy(block, seq, block).wait_recv()
            attend(block, False)

        return carry

    lax.fori_loop(1, jnp.where(seq > 0, seq + 2, 1), earlier_block, 0)

    for h in range(heads_small):
        span = slice(h * tokens, (h + 1) * tokens)
        attn_t[h * size_small : (h + 1) * size_small, :] = (
            acc_small[:, span] * (1.0 / total_ref[:, span])
        ).astype(BF16)
    for h in range(heads_large):
        first = width_small + h * size_large
        span = slice(h * tokens, (h + 1) * tokens)
        side = slice((heads_small + h) * tokens, (heads_small + h + 1) * tokens)
        attn_t[first : first + size_large, :] = (
            acc_large[:, span] * (1.0 / total_ref[:, side])
        ).astype(BF16)
    attn[...] = attn_t[...].T

    def row_ds(group, par):
        return pl.ds(pl.multiple_of((2 * group + par) * rows, rows), rows)

    def pair_copy(c):
        return pltpu.make_async_remote_copy(
            src_ref=pair_out.at[c],
            dst_ref=pair_in.at[c],
            send_sem=pair_send.at[0],
            recv_sem=pair_recv.at[c],
            device_id={"sp": seq, "tp": partner},
            device_id_type=MESH,
        )

    def cross_copy(c, group, source, slot, part=None):
        return pltpu.make_async_remote_copy(
            src_ref=cross_out.at[c, group],
            dst_ref=cross_in.at[c, source],
            send_sem=cross_send.at[slot],
            recv_sem=cross_recv.at[c if part is None else part, source],
            device_id={"sp": seq, "tp": 2 * group + parity},
            device_id_type=MESH,
        )

    for load in loads[:2]:
        load.wait()
    for i in late:
        fetches[i].wait()
    for c in range(cols):
        part = jnp.dot(
            attn[...], proj_w[:, c * col_len : (c + 1) * col_len], preferred_element_type=F32
        )
        proj_f32[c] = part
        for group in range(half_groups):
            pair_out[c, group] = proj_f32[c, row_ds(group, 1 - parity), :].astype(BF16)
        pair_copy(c).start()
    for c in range(cols):
        pair_copy(c).wait_recv()
        for hop in range(1, half_groups):
            group = lax.rem(my_group + hop, half_groups)
            cross_out[c, group] = (
                proj_f32[c, row_ds(group, parity), :] + pair_in[c, group].astype(F32)
            ).astype(BF16)
            cross_copy(c, group, my_group, hop).start()
    def own_rows(c, span, squares):
        value = proj_f32[c, row_ds(my_group, parity), :] + pair_in[c, my_group].astype(F32)
        for hop in range(1, half_groups):
            source = lax.rem(my_group + hop, half_groups)
            cross_copy(c, source, source, hop).wait_recv()
            value = value + cross_in[c, source].astype(F32)
        value = value + residual_in[:, span].astype(F32)
        resid_ref[:, span] = value
        squares = squares + jnp.sum(value * value, axis=1, keepdims=True)
        return value, squares

    def finish():
        for c in range(cols):
            span = slice(c * col_len, (c + 1) * col_len)
            picked = jnp.dot(pick_ref[...], returned[:, span], preferred_element_type=F32)
            value = resid_ref[:, span]
            for k in range(top_count):
                value = value + picked[k * rows : (k + 1) * rows] * column(route_weight, k)
            out[:, span] = value.astype(BF16)

    def scale_parts(squares):
        scale = lax.rsqrt(squares * (1.0 / width) + 1e-06)
        first = scale.astype(BF16).astype(F32)
        second = (scale - first).astype(BF16).astype(F32)
        third = scale - first - second
        lane = lax.broadcasted_iota(jnp.int32, (rows, 128), 1)
        parts = jnp.where(lane == 0, first, 0.0)
        parts = jnp.where(lane == 1, second, parts)
        return jnp.where(lane == 2, third, parts).astype(BF16)

    if lined:

        def slot_ds(member):
            return pl.ds(pl.multiple_of(member * cap, cap), cap)

        def lane_copy(z, c, up):
            ref = lane_rows.at[z, c] if c < cols else lane_scale.at[z]
            return pltpu.make_async_remote_copy(
                src_ref=ref,
                dst_ref=ref,
                send_sem=lane_send.at[up, z, 1 if c == cols else 0],
                recv_sem=lane_recv.at[z, c],
                device_id={"sp": seq + 2 * up - 1, "tp": ten},
                device_id_type=MESH,
            )

        def disp_copy(z, c, peer, sender):
            source, target = (
                (outgoing.at[z, c], arrived.at[z, c])
                if c < cols
                else (scale_out.at[z], scale_in.at[z])
            )
            return pltpu.make_async_remote_copy(
                src_ref=source.at[slot_ds(peer)],
                dst_ref=target.at[slot_ds(sender)],
                send_sem=disp_send.at[z, 1 if c == cols else 0],
                recv_sem=disp_recv.at[z, 1 if c == cols else 0],
                device_id={"sp": seq, "tp": peer},
                device_id_type=MESH,
            )

        def back_copy(z, peer):
            return pltpu.make_async_remote_copy(
                src_ref=result.at[z, slot_ds(peer)],
                dst_ref=returned.at[slot_ds(me)],
                send_sem=back_send.at[0],
                recv_sem=back_recv.at[0],
                device_id={"sp": z, "tp": peer},
                device_id_type=MESH,
            )

        mates_rows = pl.ds(0, (n_tp - 1) * cap)
        next_mate = lax.rem(ten + 1, n_tp)

        def bulk(source, target, send_sem, recv_sem):
            return pltpu.make_async_remote_copy(
                src_ref=source,
                dst_ref=target,
                send_sem=send_sem,
                recv_sem=recv_sem,
                device_id={"sp": seq, "tp": next_mate},
                device_id_type=MESH,
            )

        def disp_came(z):
            ref = arrived.at[z, :, mates_rows]
            bulk(ref, ref, disp_send.at[z, 0], disp_recv.at[z, 0]).wait_recv()
            ref = scale_in.at[z, mates_rows]
            bulk(ref, ref, disp_send.at[z, 1], disp_recv.at[z, 1]).wait_recv()

        def sent_plane(z):
            ref = outgoing.at[z, :, mates_rows]
            bulk(ref, ref, disp_send.at[z, 0], disp_recv.at[z, 0]).wait_send()
            ref = scale_out.at[z, mates_rows]
            bulk(ref, ref, disp_send.at[z, 1], disp_recv.at[z, 0]).wait_send()

        def sent_lane(z, up):
            @pl.when(seq + 1 < n_sp if up else seq > 0)
            def _():
                bulk(
                    lane_rows.at[z], lane_rows.at[z], lane_send.at[up, z, 0], lane_recv.at[z, 0]
                ).wait_send()
                bulk(
                    lane_scale.at[z], lane_scale.at[z], lane_send.at[up, z, 1], lane_recv.at[z, 0]
                ).wait_send()

        def go_on(z, c, up):
            if up:

                @pl.when(seq + 1 < n_sp)
                def _():
                    lane_copy(z, c, 1).start()
            else:

                @pl.when(seq > 0)
                def _():
                    lane_copy(z, c, 0).start()

        def place_rows(z, c):
            values = lane_rows[z, c] if c < cols else lane_scale[z]
            placed = jnp.dot(choose[z], values, preferred_element_type=F32).astype(BF16)
            if c < cols:
                outgoing[z, c] = placed
            else:
                scale_out[z] = placed
            for_mates(lambda peer: disp_copy(z, c, peer, ten).start())
            if c < cols:
                arrived[z, c, slot_ds(ten), :] = outgoing[z, c, slot_ds(ten), :]
            else:
                scale_in[z, slot_ds(ten), :] = scale_out[z, slot_ds(ten), :]

        def at_pair(k, action, own):
            low, high = seq - k - 1, seq + k
            if k > 0:

                @pl.when(high < n_sp)
                def _():
                    action(high, 0)
            elif own is not None:
                own()

            @pl.when(low >= 0)
            def _():
                action(low, 1)

        def take(k, c):
            def one(z, up):
                lane_copy(z, c, up).wait_recv()
                go_on(z, c, up)
                place_rows(z, c)

            at_pair(k, one, None)

        def serve(*blocks):
            for z in blocks:
                disp_came(z)
            came = jnp.concatenate(
                [
                    jnp.concatenate([arrived[z, c] for c in range(cols)], axis=1)
                    for z in blocks
                ],
                axis=0,
            )
            gate_part = jnp.dot(came, gate_w[...], preferred_element_type=F32)
            up_part = jnp.dot(came, up_w[...], preferred_element_type=F32)
            row_scale = jnp.concatenate(
                [jnp.sum(scale_in[z].astype(F32), axis=1, keepdims=True) for z in blocks], axis=0
            )
            gate_part, up_part = gate_part * row_scale, up_part * row_scale
            hidden = (gate_part / (1.0 + jnp.exp(-gate_part)) * up_part).astype(BF16)
            for c in range(cols):
                span = slice(c * col_len, (c + 1) * col_len)
                made = jnp.dot(hidden, down_w[:, span], preferred_element_type=F32).astype(BF16)
                for i, z in enumerate(blocks):
                    result[z, :, span] = made[i * plane_slots : (i + 1) * plane_slots]

        def give(z, up):
            for_mates(lambda peer: back_copy(z, peer).start())
            back_copy(z, ten).start()

        def give_own():
            for_mates(lambda peer: back_copy(seq, peer).start())
            returned[slot_ds(me), :] = result[seq, slot_ds(ten), :]

        def serve_pair(k):
            low, high = seq - k - 1, seq + k
            both = jnp.logical_and(low >= 0, high < n_sp)

            if 2 * k + 1 < n_sp:

                @pl.when(both)
                def _():
                    serve(high, low)

            @pl.when(jnp.logical_not(both))
            def _():
                @pl.when(jnp.logical_or(low >= 0, high < n_sp))
                def _():
                    serve(jnp.where(low >= 0, low, high))

        squares = jnp.zeros((rows, 1), F32)
        gain = norm_gain[...].astype(F32).reshape(1, width)
        for c in range(cols):
            span = slice(c * col_len, (c + 1) * col_len)
            value, squares = own_rows(c, span, squares)
            lane_rows[seq, c] = (value * gain[:, span]).astype(BF16)
            go_on(seq, c, 0)
            go_on(seq, c, 1)
            place_rows(seq, c)
        lane_scale[seq] = scale_parts(squares)
        go_on(seq, cols, 0)
        go_on(seq, cols, 1)
        place_rows(seq, cols)
        for c in range(cols + 1):
            take(0, c)
        for load in loads[2:]:
            load.wait()

        def sent_own():
            sent_plane(seq)
            sent_lane(seq, 0)
            sent_lane(seq, 1)

        def sent_block(z, up):
            sent_plane(z)
            sent_lane(z, up)

        for step in range(1, n_sp + 2):
            moving = step < n_sp
            if moving:
                for c in range(cols + 1):
                    take(step, c)
            if step <= n_sp:
                serve_pair(step - 1)
                if step == 1:
                    give_own()
                else:

                    @pl.when(seq + step - 1 < n_sp)
                    def _():
                        give(seq + step - 1, 0)

            for earlier in range(1, min(step, n_sp) + 1):
                due = jnp.maximum(earlier, n_sp - 1 - seq) == step

                @pl.when(jnp.logical_and(due, seq >= earlier))
                def _():
                    give(seq - earlier, 1)

            if step > 1:
                at_pair(step - 2, sent_block, sent_own)

        others = pl.ds(0, (experts - 1) * cap)
        bulk(
            returned.at[others], returned.at[others], back_send.at[0], back_recv.at[0]
        ).wait_recv()
        finish()
        bulk(
            returned.at[others], returned.at[others], back_send.at[0], back_recv.at[0]
        ).wait_send()
    else:
        def slot_ds(peer):
            return pl.ds(pl.multiple_of(peer * cap, cap), cap)

        def exchange(source_ref, target_ref, send, recv, peer, sender):
            return pltpu.make_async_remote_copy(
                src_ref=source_ref.at[slot_ds(peer)],
                dst_ref=target_ref.at[slot_ds(sender)],
                send_sem=send.at[peer],
                recv_sem=recv.at[sender],
                device_id={"sp": lax.div(peer, n_tp), "tp": lax.rem(peer, n_tp)},
                device_id_type=MESH,
            )

        def part_copy(c, peer, sender):
            if c < cols:
                source_ref, target_ref = outgoing.at[c], arrived.at[c]
            else:
                source_ref, target_ref = scale_out, scale_in
            return exchange(source_ref, target_ref, disp_send.at[c], disp_recv.at[c], peer, sender)

        def for_members(plane, action):
            def one(j, carry):
                peer = plane * n_tp + lax.rem(ten + j, n_tp)

                @pl.when(peer != me)
                def _():
                    action(peer)

                return carry

            lax.fori_loop(0, n_tp, one, 0)

        slots = experts * cap
        block_rows = min(256, slots)

        def place_rows(values, c):
            for b in range(slots // block_rows):
                span = slice(b * block_rows, (b + 1) * block_rows)
                chosen = pick_ref[:rows, span]
                for k in range(1, top_count):
                    chosen = chosen + pick_ref[k * rows : (k + 1) * rows, span]
                placed = lax.dot_general(
                    chosen, values, (((0,), (0,)), ((), ())), preferred_element_type=F32
                ).astype(BF16)
                if c < cols:
                    outgoing[c, span, :] = placed
                else:
                    scale_out[span, :] = placed

            def dispatch(i, carry):
                for_members(
                    lax.rem(seq + n_sp - i, n_sp), lambda peer: part_copy(c, peer, me).start()
                )
                return carry

            lax.fori_loop(0, n_sp, dispatch, 0)

        squares = jnp.zeros((rows, 1), F32)
        gain = norm_gain[...].astype(F32).reshape(1, width)
        for c in range(cols):
            span = slice(c * col_len, (c + 1) * col_len)
            value, squares = own_rows(c, span, squares)
            place_rows((value * gain[:, span]).astype(BF16), c)
        place_rows(scale_parts(squares), cols)
        for c in range(cols):
            arrived[c, slot_ds(me), :] = outgoing[c, slot_ds(me), :]
        scale_in[slot_ds(me), :] = scale_out[slot_ds(me), :]
        for load in loads[2:]:
            load.wait()

        group_rows = n_tp * cap

        def serve(i, carry):
            plane = lax.rem(seq + i, n_sp)
            span = pl.ds(pl.multiple_of(plane * group_rows, group_rows), group_rows)
            gate_part = jnp.zeros((group_rows, gate_w.shape[1]), F32)
            up_part = jnp.zeros((group_rows, gate_w.shape[1]), F32)
            for c in range(cols):
                for_members(plane, lambda peer: part_copy(c, me, peer).wait_recv())
                came = arrived[c, span, :]
                depth = slice(c * col_len, (c + 1) * col_len)
                gate_part = gate_part + jnp.dot(came, gate_w[depth, :], preferred_element_type=F32)
                up_part = up_part + jnp.dot(came, up_w[depth, :], preferred_element_type=F32)
            for_members(plane, lambda peer: part_copy(cols, me, peer).wait_recv())
            row_scale = jnp.sum(scale_in[span, :].astype(F32), axis=1, keepdims=True)
            gate_part, up_part = gate_part * row_scale, up_part * row_scale
            hidden = (gate_part / (1.0 + jnp.exp(-gate_part)) * up_part).astype(BF16)
            result[span, :] = jnp.dot(hidden, down_w[...], preferred_element_type=F32).astype(BF16)
            for_members(
                plane,
                lambda peer: exchange(result, returned, back_send, back_recv, peer, me).start(),
            )
            return carry

        lax.fori_loop(0, n_sp, serve, 0)
        returned[slot_ds(me), :] = result[slot_ds(me), :]

        def collect(i, carry):
            peer = lax.rem(me + i, experts)
            exchange(result, returned, back_send, back_recv, me, peer).wait_recv()
            return carry

        lax.fori_loop(1, experts, collect, 0)
        finish()

        def sent_rows(i, carry):
            peer = lax.rem(me + i, experts)
            for c in range(cols + 1):
                part_copy(c, peer, me).wait_send()
            exchange(result, returned, back_send, back_recv, peer, me).wait_send()
            return carry

        lax.fori_loop(1, experts, sent_rows, 0)

    def sent_kv(target, carry):
        gate_copy(seq, target, target).wait_send()
        kv_copy(seq, target, target).wait_send()
        return carry

    lax.fori_loop(seq + 1, n_sp, sent_kv, 0)
    if lined:

        def sent_gates(target, carry):
            gate_copy(seq, target, target).wait_send()
            return carry

        lax.fori_loop(0, seq, sent_gates, 0)

    def sent_fwd(block, carry):
        pass_copy(block, pl.ds(0, n_tp - 1)).wait_send()
        return carry

    lax.fori_loop(0, seq, sent_fwd, 0)
    pltpu.make_async_remote_copy(
        src_ref=pair_out,
        dst_ref=pair_in,
        send_sem=pair_send.at[0],
        recv_sem=pair_recv.at[0],
        device_id={"sp": seq, "tp": partner},
        device_id_type=MESH,
    ).wait_send()
    for hop in range(1, half_groups):
        cross_copy(pl.ds(0, cols), lax.rem(my_group + hop, half_groups), my_group, hop, 0).wait_send()


def shards(
    residual_in,
    query_small,
    query_large,
    key_small,
    key_large,
    value_small,
    value_large,
    forget_small,
    forget_large,
    project_small,
    project_large,
    norm_gain,
    expert_gate,
    expert_up,
    expert_down,
    routing,
    route_weight,
):
    n_sp, n_tp = lax.axis_size("sp"), lax.axis_size("tp")
    experts = n_sp * n_tp
    rows, width = residual_in.shape
    top_count = routing.shape[1]
    tokens = query_small.shape[0]
    size_small, size_large = key_small.shape[0], key_large.shape[0]
    heads_small, heads_large = forget_small.shape[0], forget_large.shape[0]
    heads = heads_small + heads_large
    gate_rows = -(-max(heads, 2 * top_count) // 8) * 8
    extra_rows = -(-3 * gate_rows // 16) * 16
    capacity = max(2, 2 * rows * top_count // experts)
    cap = -(-capacity // 16) * 16
    col_len = min(width, 512)
    cols = width // col_len
    hidden = expert_gate.shape[2]
    attn_width = heads_small * size_small + heads_large * size_large
    half_groups = n_tp // 2
    slots = experts * cap
    group = n_tp * cap
    lined = n_tp * capacity >= rows
    vmem, dma = pltpu.VMEM, pltpu.SemaphoreType.DMA
    inputs = (
        residual_in,
        query_small,
        query_large,
        key_small,
        key_large,
        value_small,
        value_large,
        forget_small,
        forget_large,
        norm_gain,
        routing.T,
        route_weight.T,
    )
    if lined:
        tail = [
            vmem((top_count * rows, slots), BF16),
            vmem((n_sp, group, rows), BF16),
            vmem((n_sp, cols, rows, col_len), BF16),
            vmem((n_sp, rows, 128), BF16),
            vmem((n_sp, cols, group, col_len), BF16),
            vmem((n_sp, cols, group, col_len), BF16),
            vmem((n_sp, group, 128), BF16),
            vmem((n_sp, group, 128), BF16),
            vmem((n_sp, group, width), BF16),
            vmem((slots, width), BF16),
            dma((2, n_sp, 2)),
            dma((n_sp, cols + 1)),
            dma((n_sp, 2)),
            dma((n_sp, 2)),
            dma((1,)),
            dma((1,)),
        ]
    else:
        tail = [
            vmem((top_count * rows, slots), BF16),
            vmem((cols, slots, col_len), BF16),
            vmem((cols, slots, col_len), BF16),
            vmem((slots, 128), BF16),
            vmem((slots, 128), BF16),
            vmem((slots, width), BF16),
            vmem((slots, width), BF16),
            dma((cols + 1, experts)),
            dma((cols + 1, experts)),
            dma((experts,)),
            dma((experts,)),
        ]
    return pl.pallas_call(
        functools.partial(layer_kernel, (n_sp, n_tp, cap, col_len, lined)),
        out_shape=jax.ShapeDtypeStruct((rows, width), BF16),
        in_specs=[pl.BlockSpec(memory_space=pl.ANY)] * 17,
        out_specs=pl.BlockSpec(memory_space=pltpu.VMEM),
        scratch_shapes=[vmem(given.shape, given.dtype) for given in inputs]
        + [
            vmem((n_sp, n_tp, 2 * (size_small + size_large) // n_tp, tokens), BF16),
            vmem((n_sp, gate_rows, tokens + -(-rows // 128) * 128), F32),
            vmem((size_small + extra_rows, heads_small * tokens), BF16),
            vmem((size_large + extra_rows, heads_large * tokens), BF16),
            vmem((1, heads * tokens), F32),
            vmem((1, heads * tokens), F32),
            vmem((size_small, heads_small * tokens), F32),
            vmem((size_large, heads_large * tokens), F32),
            vmem((attn_width, tokens), BF16),
            vmem((tokens, attn_width), BF16),
            vmem((attn_width, width), BF16),
            vmem((width, hidden), BF16),
            vmem((width, hidden), BF16),
            vmem((hidden, width), BF16),
            vmem((cols, tokens, col_len), F32),
            vmem((cols, half_groups, rows, col_len), BF16),
            vmem((cols, half_groups, rows, col_len), BF16),
            vmem((cols, half_groups, rows, col_len), BF16),
            vmem((cols, half_groups, rows, col_len), BF16),
            vmem((rows, width), F32),
            dma((5,)),
            dma((12,)),
            dma((n_sp,)),
            dma((n_sp,)),
            dma((n_sp,)),
            dma((n_sp,)),
            dma((n_sp,)),
            dma((n_sp, half_groups)),
            dma((n_sp,)),
            dma((1,)),
            dma((cols,)),
            dma((half_groups,)),
            dma((cols, half_groups)),
        ]
        + tail,
        compiler_params=pltpu.CompilerParams(
            collective_id=0, has_side_effects=True, vmem_limit_bytes=60 * 1024 * 1024
        ),
    )(
        *inputs,
        project_small,
        project_large,
        expert_gate,
        expert_up,
        expert_down,
    )


def solution(mesh):
    in_specs = (
        P(("grp", "sp", "tp"), None),
        P(("grp", "sp"), "tp"),
        P(("grp", "sp"), "tp"),
        P(None, ("grp", "sp")),
        P(None, ("grp", "sp")),
        P(None, ("grp", "sp")),
        P(None, ("grp", "sp")),
        P("tp", ("grp", "sp")),
        P("tp", ("grp", "sp")),
        P("tp", None),
        P("tp", None),
        P(),
        P(("sp", "tp"), None, None),
        P(("sp", "tp"), None, None),
        P(("sp", "tp"), None, None),
        P(("grp", "sp", "tp"), None),
        P(("grp", "sp", "tp"), None),
    )
    out_specs = P(("grp", "sp", "tp"), None)
    return jax.shard_map(shards, mesh=mesh, in_specs=in_specs, out_specs=out_specs, check_vma=False)
```

```python
import functools
import math

import jax
import jax.numpy as jnp
from jax import lax
from jax.experimental import pallas as pl
from jax.experimental.pallas import tpu as pltpu
from jax.sharding import PartitionSpec as P

MESH = pl.DeviceIdType.MESH
F32 = jnp.float32
BF16 = jnp.bfloat16


def layer_kernel(dims, *refs):
    given, refs = refs[:12], refs[12:]
    (
        project_small,
        project_large,
        expert_gate,
        expert_up,
        expert_down,
        out,
        residual_in,
        query_small,
        query_large,
        key_small,
        key_large,
        value_small,
        value_large,
        forget_small,
        forget_large,
        norm_gain,
        routing,
        route_weight,
        kv,
        gates,
        turned_q_small,
        turned_q_large,
        top_ref,
        total_ref,
        acc_small,
        acc_large,
        attn_t,
        attn,
        proj_w,
        gate_w,
        up_w,
        down_w,
        proj_f32,
        pair_out,
        pair_in,
        cross_out,
        cross_in,
        resid_ref,
        weight_sem,
        given_sem,
        kv_send,
        kv_recv,
        gate_send,
        gate_recv,
        share_send,
        pass_recv,
        pair_send,
        pair_recv,
        cross_send,
        cross_recv,
        *tail,
    ) = refs
    n_sp, n_tp, cap, col_len, lined = dims
    held = (
        residual_in,
        query_small,
        query_large,
        key_small,
        key_large,
        value_small,
        value_large,
        forget_small,
        forget_large,
        norm_gain,
        routing,
        route_weight,
    )
    fetches = [
        pltpu.make_async_copy(source, target, given_sem.at[i])
        for i, (source, target) in enumerate(zip(given, held))
    ]
    early, queries, late = (3, 4, 5, 6, 7, 8, 10, 11), (1, 2), (0, 9)
    for i in early + queries + late:
        fetches[i].start()
    experts = n_sp * n_tp
    seq = lax.axis_index("sp")
    ten = lax.axis_index("tp")
    me = seq * n_tp + ten
    parity = lax.rem(ten, 2)
    partner = ten + 1 - 2 * parity
    tokens = query_small.shape[0]
    size_small, size_large = key_small.shape[0], key_large.shape[0]
    heads_small, heads_large = forget_small.shape[0], forget_large.shape[0]
    width_small = heads_small * size_small
    rows, width = residual_in.shape
    piece_count = kv.shape[1]
    piece_small, piece_large = size_small // piece_count, size_large // piece_count
    cols = width // col_len
    half_groups = n_tp // 2
    my_group = lax.div(ten, 2)

    loads = [
        pltpu.make_async_copy(project_small, proj_w.at[pl.ds(0, width_small)], weight_sem.at[0]),
        pltpu.make_async_copy(
            project_large,
            proj_w.at[pl.ds(width_small, heads_large * size_large)],
            weight_sem.at[1],
        ),
        pltpu.make_async_copy(expert_gate.at[0], gate_w, weight_sem.at[2]),
        pltpu.make_async_copy(expert_up.at[0], up_w, weight_sem.at[3]),
        pltpu.make_async_copy(expert_down.at[0], down_w, weight_sem.at[4]),
    ]
    barrier = pltpu.get_barrier_semaphore()

    def greet(peer_sp, peer_tp):
        pl.semaphore_signal(
            barrier, inc=1, device_id={"sp": peer_sp, "tp": peer_tp}, device_id_type=MESH
        )

    def greet_all(i, carry):
        peer = lax.rem(me + i, experts)
        greet(lax.div(peer, n_tp), lax.rem(peer, n_tp))
        return carry

    lax.fori_loop(1, experts, greet_all, 0)
    for i in early:
        fetches[i].wait()

    for p in range(piece_count):
        base = 0
        for source, piece in (
            (key_small, piece_small),
            (key_large, piece_large),
            (value_small, piece_small),
            (value_large, piece_large),
        ):
            kv[seq, p, base : base + piece, :] = source[p * piece : (p + 1) * piece, :]
            base += piece
    top_count = routing.shape[0]
    gate_rows = gates.shape[1]
    gates[seq] = jnp.zeros(gates.shape[1:], F32)
    gates[seq, :heads_small, :tokens] = forget_small[...]
    gates[seq, heads_small : heads_small + heads_large, :tokens] = forget_large[...]
    gates[seq, :top_count, tokens : tokens + rows] = routing[...].astype(F32)

    pl.semaphore_wait(barrier, experts - 1)

    def kv_copy(source, target, slot):
        return pltpu.make_async_remote_copy(
            src_ref=kv.at[source, parity],
            dst_ref=kv.at[source, parity],
            send_sem=kv_send.at[slot],
            recv_sem=kv_recv.at[source],
            device_id={"sp": target, "tp": ten},
            device_id_type=MESH,
        )

    def gate_copy(source, target, slot):
        return pltpu.make_async_remote_copy(
            src_ref=gates.at[source],
            dst_ref=gates.at[source],
            send_sem=gate_send.at[slot],
            recv_sem=gate_recv.at[source],
            device_id={"sp": target, "tp": ten},
            device_id_type=MESH,
        )

    def pass_copy(source, piece):
        return pltpu.make_async_remote_copy(
            src_ref=kv.at[source, piece],
            dst_ref=kv.at[source, piece],
            send_sem=share_send.at[source],
            recv_sem=pass_recv.at[source],
            device_id={"sp": seq, "tp": partner},
            device_id_type=MESH,
        )

    def for_mates(action):
        for i in range(1, n_tp):
            action(lax.rem(ten + i, n_tp))

    def send_kv(target, carry):
        kv_copy(seq, target, target).start()
        return carry

    def send_gates(target, carry):
        gate_copy(seq, target, target).start()
        return carry

    lax.fori_loop(seq + 1, n_sp, send_gates, 0)
    lax.fori_loop(seq + 1, jnp.minimum(seq + 2, n_sp), send_kv, 0)
    if lined:
        lax.fori_loop(0, seq, send_gates, 0)
    for load in loads:
        load.start()

    lanes = lax.broadcasted_iota(jnp.int32, (rows, experts), 1)
    same = lax.broadcasted_iota(jnp.int32, (rows, rows), 0) == lax.broadcasted_iota(
        jnp.int32, (rows, rows), 1
    )

    def column(ref, k):
        return jnp.sum(
            jnp.where(same, ref[k : k + 1, :].astype(F32), 0.0), axis=1, keepdims=True
        )

    def route_places(routes):
        hot = [(route == lanes.astype(F32)).astype(F32) for route in routes]
        named = sum(hot).astype(BF16)
        below = (
            lax.broadcasted_iota(jnp.int32, (rows, rows), 0)
            > lax.broadcasted_iota(jnp.int32, (rows, rows), 1)
        ).astype(F32)
        earlier = jnp.dot(below.astype(BF16), named, preferred_element_type=F32)
        return [
            route * cap + jnp.sum(earlier * one, axis=1, keepdims=True)
            for route, one in zip(routes, hot)
        ]

    if lined:
        (
            pick_ref,
            choose,
            lane_rows,
            lane_scale,
            outgoing,
            arrived,
            scale_out,
            scale_in,
            result,
            returned,
            lane_send,
            lane_recv,
            disp_send,
            disp_recv,
            back_send,
            back_recv,
        ) = tail
        plane_slots = n_tp * cap
        slot_lane = lax.broadcasted_iota(jnp.int32, (rows, plane_slots), 1)

        def prepare(z):
            known = gates[z][:, tokens : tokens + rows]
            spots = (slot_lane + seq * plane_slots).astype(F32)
            both = jnp.zeros((rows, plane_slots), F32)
            for place in route_places([column(known, k) for k in range(top_count)]):
                both = both + (spots == place).astype(F32)
            choose[z] = both.T.astype(BF16)

        prepare(seq)
    else:
        (
            pick_ref,
            outgoing,
            arrived,
            scale_out,
            scale_in,
            result,
            returned,
            disp_send,
            disp_recv,
            back_send,
            back_recv,
        ) = tail

    spots = lax.broadcasted_iota(jnp.int32, (rows, experts * cap), 1).astype(F32)
    places = route_places([column(routing, k) for k in range(top_count)])
    for k in range(top_count):
        pick_ref[k * rows : (k + 1) * rows, :] = (spots == places[k]).astype(F32).astype(BF16)

    extra_rows = turned_q_small.shape[0] - size_small

    def fold(size):
        power = 2.0 ** math.floor(math.log2(size**-0.5))
        return power, size**-0.5 / power

    for i in queries:
        fetches[i].wait()
    extra_row = lax.broadcasted_iota(jnp.int32, (extra_rows, tokens), 0)
    for kind in range(2):
        heads, size, offset, source, q_ref = (
            (heads_small, size_small, 0, query_small, turned_q_small),
            (heads_large, size_large, heads_small, query_large, turned_q_large),
        )[kind]
        turned = (source[...] * fold(size)[0]).astype(BF16).T
        for h in range(heads):
            chosen = (lax.rem(extra_row, gate_rows) == offset + h) & (extra_row < 3 * gate_rows)
            span = slice(h * tokens, (h + 1) * tokens)
            q_ref[:size, span] = turned[h * size : (h + 1) * size, :]
            q_ref[size:, span] = jnp.where(chosen, 1.0, 0.0).astype(BF16)
    key_base = (0, piece_small)
    value_base = (piece_small + piece_large, 2 * piece_small + piece_large)

    def attend(block, diagonal):
        block_gates = gates[block][:, :tokens]

        def seen(heads):
            shape = (tokens, heads * tokens)
            k_pos = lax.broadcasted_iota(jnp.int32, shape, 0)
            q_pos = lax.rem(lax.broadcasted_iota(jnp.int32, shape, 1), tokens)
            return q_pos >= k_pos

        for kind in range(2):
            heads, size, piece, offset, q_ref, acc = (
                (heads_small, size_small, piece_small, 0, turned_q_small, acc_small),
                (heads_large, size_large, piece_large, heads_small, turned_q_large, acc_large),
            )[kind]
            kb, vb = key_base[kind], value_base[kind]
            rest = fold(size)[1]
            shift = block_gates * (-1.0 / rest)
            first = shift.astype(BF16).astype(F32)
            second = (shift - first).astype(BF16).astype(F32)
            pieces = [first, second, shift - first - second]
            if extra_rows > 3 * gate_rows:
                pieces.append(jnp.zeros((extra_rows - 3 * gate_rows, tokens), F32))
            keys = jnp.concatenate(
                [kv[block, p, kb : kb + piece, :] for p in range(piece_count)]
                + [jnp.concatenate(pieces, axis=0).astype(BF16)],
                axis=0,
            ).T
            values = jnp.concatenate(
                [kv[block, p, vb : vb + piece, :] for p in range(piece_count)], axis=0
            )
            side = slice(offset * tokens, (offset + heads) * tokens)
            scores = jnp.dot(keys, q_ref[...], preferred_element_type=F32)
            if diagonal:
                scores = jnp.where(seen(heads), scores, -jnp.inf)
            block_top = jnp.max(scores, axis=0, keepdims=True)
            top = block_top if diagonal else jnp.maximum(top_ref[:, side], block_top)
            below_top = scores - top
            weights = jnp.exp(below_top if rest == 1.0 else below_top * rest)
            total = jnp.sum(weights, axis=0, keepdims=True)
            mixed = jnp.dot(values, weights.astype(BF16), preferred_element_type=F32)
            if not diagonal:
                factor = jnp.exp((top_ref[:, side] - top) * rest)
                total = total_ref[:, side] * factor + total
                mixed = acc[...] * factor + mixed
            top_ref[:, side] = top
            total_ref[:, side] = total
            acc[...] = mixed

    def share_out(block):
        kv_copy(block, seq, block).wait_recv()
        pass_copy(block, parity).start()

    attend(seq, True)
    lax.fori_loop(seq + 2, n_sp, send_kv, 0)

    def learn(distances):
        if lined:
            for i in distances:
                z = lax.rem(seq + n_sp - i, n_sp)
                gate_copy(z, seq, z).wait_recv()
                prepare(z)

    learn(range(1, n_sp))

    def at_earlier(block):
        @pl.when(block >= 0)
        def _():
            share_out(block)

    at_earlier(seq - 1)

    def earlier_block(i, carry):
        block = seq - i
        pass_copy(block, 1 - parity).wait_recv()
        if not lined:
            gate_copy(block, seq, block).wait_recv()
        attend(block, False)

        @pl.when(jnp.logical_and(i == 1, seq > 1))
        def _():
            share_out(seq - 2)

        at_earlier(block - 2)
        return carry

    lax.fori_loop(1, seq + 1, earlier_block, 0)

    for h in range(heads_small):
        span = slice(h * tokens, (h + 1) * tokens)
        attn_t[h * size_small : (h + 1) * size_small, :] = (
            acc_small[:, span] * (1.0 / total_ref[:, span])
        ).astype(BF16)
    for h in range(heads_large):
        first = width_small + h * size_large
        span = slice(h * tokens, (h + 1) * tokens)
        side = slice((heads_small + h) * tokens, (heads_small + h + 1) * tokens)
        attn_t[first : first + size_large, :] = (
            acc_large[:, span] * (1.0 / total_ref[:, side])
        ).astype(BF16)
    attn[...] = attn_t[...].T

    def row_ds(group, par):
        return pl.ds(pl.multiple_of((2 * group + par) * rows, rows), rows)

    def pair_copy(c):
        return pltpu.make_async_remote_copy(
            src_ref=pair_out.at[c],
            dst_ref=pair_in.at[c],
            send_sem=pair_send.at[0],
            recv_sem=pair_recv.at[c],
            device_id={"sp": seq, "tp": partner},
            device_id_type=MESH,
        )

    def cross_copy(c, group, source, slot, part=None):
        return pltpu.make_async_remote_copy(
            src_ref=cross_out.at[c, group],
            dst_ref=cross_in.at[c, source],
            send_sem=cross_send.at[slot],
            recv_sem=cross_recv.at[c if part is None else part, source],
            device_id={"sp": seq, "tp": 2 * group + parity},
            device_id_type=MESH,
        )

    for load in loads[:2]:
        load.wait()
    for i in late:
        fetches[i].wait()
    for c in range(cols):
        part = jnp.dot(
            attn[...], proj_w[:, c * col_len : (c + 1) * col_len], preferred_element_type=F32
        )
        proj_f32[c] = part
        for group in range(half_groups):
            pair_out[c, group] = proj_f32[c, row_ds(group, 1 - parity), :].astype(BF16)
        pair_copy(c).start()
    for c in range(cols):
        pair_copy(c).wait_recv()
        for hop in range(1, half_groups):
            group = lax.rem(my_group + hop, half_groups)
            cross_out[c, group] = (
                proj_f32[c, row_ds(group, parity), :] + pair_in[c, group].astype(F32)
            ).astype(BF16)
            cross_copy(c, group, my_group, hop).start()
    def own_rows(c, span, squares):
        value = proj_f32[c, row_ds(my_group, parity), :] + pair_in[c, my_group].astype(F32)
        for hop in range(1, half_groups):
            source = lax.rem(my_group + hop, half_groups)
            cross_copy(c, source, source, hop).wait_recv()
            value = value + cross_in[c, source].astype(F32)
        value = value + residual_in[:, span].astype(F32)
        resid_ref[:, span] = value
        squares = squares + jnp.sum(value * value, axis=1, keepdims=True)
        return value, squares

    def finish():
        for c in range(cols):
            span = slice(c * col_len, (c + 1) * col_len)
            picked = jnp.dot(pick_ref[...], returned[:, span], preferred_element_type=F32)
            value = resid_ref[:, span]
            for k in range(top_count):
                value = value + picked[k * rows : (k + 1) * rows] * column(route_weight, k)
            out[:, span] = value.astype(BF16)

    def scale_parts(squares):
        scale = lax.rsqrt(squares * (1.0 / width) + 1e-06)
        first = scale.astype(BF16).astype(F32)
        second = (scale - first).astype(BF16).astype(F32)
        third = scale - first - second
        lane = lax.broadcasted_iota(jnp.int32, (rows, 128), 1)
        parts = jnp.where(lane == 0, first, 0.0)
        parts = jnp.where(lane == 1, second, parts)
        return jnp.where(lane == 2, third, parts).astype(BF16)

    if lined:

        def slot_ds(member):
            return pl.ds(pl.multiple_of(member * cap, cap), cap)

        def lane_copy(z, c, up):
            ref = lane_rows.at[z, c] if c < cols else lane_scale.at[z]
            return pltpu.make_async_remote_copy(
                src_ref=ref,
                dst_ref=ref,
                send_sem=lane_send.at[up, z, 1 if c == cols else 0],
                recv_sem=lane_recv.at[z, c],
                device_id={"sp": seq + 2 * up - 1, "tp": ten},
                device_id_type=MESH,
            )

        scale_out[...] = jnp.zeros(scale_out.shape, BF16)

        def disp_copy(z, c, peer, sender):
            source, target = (
                (outgoing.at[z, c], arrived.at[z, c])
                if c < cols
                else (scale_out.at[z], scale_in.at[z])
            )
            return pltpu.make_async_remote_copy(
                src_ref=source.at[slot_ds(peer)],
                dst_ref=target.at[slot_ds(sender)],
                send_sem=disp_send.at[z, 1 if c == cols else 0],
                recv_sem=disp_recv.at[z, 1 if c == cols else 0],
                device_id={"sp": seq, "tp": peer},
                device_id_type=MESH,
            )

        def back_copy(z, peer):
            return pltpu.make_async_remote_copy(
                src_ref=result.at[z, slot_ds(peer)],
                dst_ref=returned.at[slot_ds(me)],
                send_sem=back_send.at[0],
                recv_sem=back_recv.at[0],
                device_id={"sp": z, "tp": peer},
                device_id_type=MESH,
            )

        mates_rows = pl.ds(0, (n_tp - 1) * cap)
        next_mate = lax.rem(ten + 1, n_tp)

        def bulk(source, target, send_sem, recv_sem):
            return pltpu.make_async_remote_copy(
                src_ref=source,
                dst_ref=target,
                send_sem=send_sem,
                recv_sem=recv_sem,
                device_id={"sp": seq, "tp": next_mate},
                device_id_type=MESH,
            )

        def disp_came(z):
            ref = arrived.at[z, :, mates_rows]
            bulk(ref, ref, disp_send.at[z, 0], disp_recv.at[z, 0]).wait_recv()
            ref = scale_in.at[z, mates_rows]
            bulk(ref, ref, disp_send.at[z, 1], disp_recv.at[z, 1]).wait_recv()

        def sent_plane(z):
            ref = outgoing.at[z, :, mates_rows]
            bulk(ref, ref, disp_send.at[z, 0], disp_recv.at[z, 0]).wait_send()
            ref = scale_out.at[z, mates_rows]
            bulk(ref, ref, disp_send.at[z, 1], disp_recv.at[z, 0]).wait_send()

        def sent_lane(z, up):
            @pl.when(seq + 1 < n_sp if up else seq > 0)
            def _():
                bulk(
                    lane_rows.at[z], lane_rows.at[z], lane_send.at[up, z, 0], lane_recv.at[z, 0]
                ).wait_send()
                bulk(
                    lane_scale.at[z], lane_scale.at[z], lane_send.at[up, z, 1], lane_recv.at[z, 0]
                ).wait_send()

        def go_on(z, c, up):
            if up:

                @pl.when(seq + 1 < n_sp)
                def _():
                    lane_copy(z, c, 1).start()
            else:

                @pl.when(seq > 0)
                def _():
                    lane_copy(z, c, 0).start()

        def place_rows(z, c):
            if c < cols:
                outgoing[z, c] = jnp.dot(
                    choose[z], lane_rows[z, c], preferred_element_type=F32
                ).astype(BF16)
            else:
                parts = lane_scale[z, :, :rows].astype(F32).T.astype(BF16)
                scale_out[z, :, : parts.shape[1]] = jnp.dot(
                    choose[z], parts, preferred_element_type=F32
                ).astype(BF16)
            for_mates(lambda peer: disp_copy(z, c, peer, ten).start())
            if c < cols:
                arrived[z, c, slot_ds(ten), :] = outgoing[z, c, slot_ds(ten), :]
            else:
                scale_in[z, slot_ds(ten), :] = scale_out[z, slot_ds(ten), :]

        def at_pair(k, action, own):
            low, high = seq - k - 1, seq + k
            if k > 0:

                @pl.when(high < n_sp)
                def _():
                    action(high, 0)
            elif own is not None:
                own()

            @pl.when(low >= 0)
            def _():
                action(low, 1)

        def take(k, c):
            def one(z, up):
                lane_copy(z, c, up).wait_recv()
                go_on(z, c, up)
                place_rows(z, c)

            low, high = seq - k - 1, seq + k

            @pl.when(low >= 0)
            def _():
                one(low, 1)

            if k > 0:

                @pl.when(high < n_sp)
                def _():
                    one(high, 0)

        def serve(*blocks):
            for z in blocks:
                disp_came(z)
            came = jnp.concatenate(
                [
                    jnp.concatenate([arrived[z, c] for c in range(cols)], axis=1)
                    for z in blocks
                ],
                axis=0,
            )
            gate_part = jnp.dot(came, gate_w[...], preferred_element_type=F32)
            up_part = jnp.dot(came, up_w[...], preferred_element_type=F32)
            row_scale = jnp.concatenate(
                [
                    jnp.sum(
                        scale_in[z, :, : lane_scale.shape[1]].astype(F32), axis=1, keepdims=True
                    )
                    for z in blocks
                ],
                axis=0,
            )
            gate_part, up_part = gate_part * row_scale, up_part * row_scale
            hidden = (gate_part / (1.0 + jnp.exp(-gate_part)) * up_part).astype(BF16)
            for c in range(cols):
                span = slice(c * col_len, (c + 1) * col_len)
                made = jnp.dot(hidden, down_w[:, span], preferred_element_type=F32).astype(BF16)
                for i, z in enumerate(blocks):
                    result[z, :, span] = made[i * plane_slots : (i + 1) * plane_slots]

        def give(z, up):
            for_mates(lambda peer: back_copy(z, peer).start())
            back_copy(z, ten).start()

        def give_own():
            for_mates(lambda peer: back_copy(seq, peer).start())
            returned[slot_ds(me), :] = result[seq, slot_ds(ten), :]

        def serve_pair(k):
            low, high = seq - k - 1, seq + k
            both = jnp.logical_and(low >= 0, high < n_sp)

            if 2 * k + 1 < n_sp:

                @pl.when(both)
                def _():
                    serve(high, low)

            @pl.when(jnp.logical_not(both))
            def _():
                @pl.when(jnp.logical_or(low >= 0, high < n_sp))
                def _():
                    serve(jnp.where(low >= 0, low, high))

        squares = jnp.zeros((rows, 1), F32)
        gain = norm_gain[...].astype(F32).reshape(1, width)
        for c in range(cols):
            span = slice(c * col_len, (c + 1) * col_len)
            value, squares = own_rows(c, span, squares)
            lane_rows[seq, c] = (value * gain[:, span]).astype(BF16)
            go_on(seq, c, 0)
            go_on(seq, c, 1)
            place_rows(seq, c)
        lane_scale[seq] = jnp.zeros(lane_scale.shape[1:], BF16)
        turned_scale = scale_parts(squares).astype(F32).T
        lane_scale[seq, :, :rows] = turned_scale[: lane_scale.shape[1]].astype(BF16)
        go_on(seq, cols, 0)
        go_on(seq, cols, 1)
        place_rows(seq, cols)
        for c in range(cols + 1):
            take(0, c)
        for load in loads[2:]:
            load.wait()

        def sent_own():
            sent_plane(seq)
            sent_lane(seq, 0)
            sent_lane(seq, 1)

        def sent_block(z, up):
            sent_plane(z)
            sent_lane(z, up)

        for step in range(1, n_sp + 2):
            moving = step < n_sp
            if moving:
                for c in range(cols + 1):
                    take(step, c)
            if step <= n_sp:
                serve_pair(step - 1)
                if step == n_sp:
                    give_own()
                if step > 1:

                    @pl.when(seq + step - 1 < n_sp)
                    def _():
                        give(seq + step - 1, 0)

            for earlier in range(1, min(step, n_sp) + 1):
                due = jnp.maximum(earlier, n_sp - 1 - seq) == step

                @pl.when(jnp.logical_and(due, seq >= earlier))
                def _():
                    give(seq - earlier, 1)

            if step > 1:
                at_pair(step - 2, sent_block, sent_own)

        others = pl.ds(0, (experts - 1) * cap)
        bulk(
            returned.at[others], returned.at[others], back_send.at[0], back_recv.at[0]
        ).wait_recv()
        finish()
        bulk(
            returned.at[others], returned.at[others], back_send.at[0], back_recv.at[0]
        ).wait_send()
    else:
        def slot_ds(peer):
            return pl.ds(pl.multiple_of(peer * cap, cap), cap)

        def exchange(source_ref, target_ref, send, recv, peer, sender):
            return pltpu.make_async_remote_copy(
                src_ref=source_ref.at[slot_ds(peer)],
                dst_ref=target_ref.at[slot_ds(sender)],
                send_sem=send.at[peer],
                recv_sem=recv.at[sender],
                device_id={"sp": lax.div(peer, n_tp), "tp": lax.rem(peer, n_tp)},
                device_id_type=MESH,
            )

        def part_copy(c, peer, sender):
            if c < cols:
                source_ref, target_ref = outgoing.at[c], arrived.at[c]
            else:
                source_ref, target_ref = scale_out, scale_in
            return exchange(source_ref, target_ref, disp_send.at[c], disp_recv.at[c], peer, sender)

        def for_members(plane, action):
            def one(j, carry):
                peer = plane * n_tp + lax.rem(ten + j, n_tp)

                @pl.when(peer != me)
                def _():
                    action(peer)

                return carry

            lax.fori_loop(0, n_tp, one, 0)

        slots = experts * cap
        block_rows = min(256, slots)

        def place_rows(values, c):
            for b in range(slots // block_rows):
                span = slice(b * block_rows, (b + 1) * block_rows)
                chosen = pick_ref[:rows, span]
                for k in range(1, top_count):
                    chosen = chosen + pick_ref[k * rows : (k + 1) * rows, span]
                placed = lax.dot_general(
                    chosen, values, (((0,), (0,)), ((), ())), preferred_element_type=F32
                ).astype(BF16)
                if c < cols:
                    outgoing[c, span, :] = placed
                else:
                    scale_out[span, :] = placed

            def dispatch(i, carry):
                for_members(
                    lax.rem(seq + n_sp - i, n_sp), lambda peer: part_copy(c, peer, me).start()
                )
                return carry

            lax.fori_loop(0, n_sp, dispatch, 0)

        squares = jnp.zeros((rows, 1), F32)
        gain = norm_gain[...].astype(F32).reshape(1, width)
        for c in range(cols):
            span = slice(c * col_len, (c + 1) * col_len)
            value, squares = own_rows(c, span, squares)
            place_rows((value * gain[:, span]).astype(BF16), c)
        place_rows(scale_parts(squares), cols)
        for c in range(cols):
            arrived[c, slot_ds(me), :] = outgoing[c, slot_ds(me), :]
        scale_in[slot_ds(me), :] = scale_out[slot_ds(me), :]
        for load in loads[2:]:
            load.wait()

        group_rows = n_tp * cap

        def serve(i, carry):
            plane = lax.rem(seq + i, n_sp)
            span = pl.ds(pl.multiple_of(plane * group_rows, group_rows), group_rows)
            gate_part = jnp.zeros((group_rows, gate_w.shape[1]), F32)
            up_part = jnp.zeros((group_rows, gate_w.shape[1]), F32)
            for c in range(cols):
                for_members(plane, lambda peer: part_copy(c, me, peer).wait_recv())
                came = arrived[c, span, :]
                depth = slice(c * col_len, (c + 1) * col_len)
                gate_part = gate_part + jnp.dot(came, gate_w[depth, :], preferred_element_type=F32)
                up_part = up_part + jnp.dot(came, up_w[depth, :], preferred_element_type=F32)
            for_members(plane, lambda peer: part_copy(cols, me, peer).wait_recv())
            row_scale = jnp.sum(scale_in[span, :].astype(F32), axis=1, keepdims=True)
            gate_part, up_part = gate_part * row_scale, up_part * row_scale
            hidden = (gate_part / (1.0 + jnp.exp(-gate_part)) * up_part).astype(BF16)
            result[span, :] = jnp.dot(hidden, down_w[...], preferred_element_type=F32).astype(BF16)
            for_members(
                plane,
                lambda peer: exchange(result, returned, back_send, back_recv, peer, me).start(),
            )
            return carry

        lax.fori_loop(0, n_sp, serve, 0)
        returned[slot_ds(me), :] = result[slot_ds(me), :]

        def collect(i, carry):
            peer = lax.rem(me + i, experts)
            exchange(result, returned, back_send, back_recv, me, peer).wait_recv()
            return carry

        lax.fori_loop(1, experts, collect, 0)
        finish()

        def sent_rows(i, carry):
            peer = lax.rem(me + i, experts)
            for c in range(cols + 1):
                part_copy(c, peer, me).wait_send()
            exchange(result, returned, back_send, back_recv, peer, me).wait_send()
            return carry

        lax.fori_loop(1, experts, sent_rows, 0)

    def sent_kv(target, carry):
        gate_copy(seq, target, target).wait_send()
        kv_copy(seq, target, target).wait_send()
        return carry

    lax.fori_loop(seq + 1, n_sp, sent_kv, 0)
    if lined:

        def sent_gates(target, carry):
            gate_copy(seq, target, target).wait_send()
            return carry

        lax.fori_loop(0, seq, sent_gates, 0)

    def sent_fwd(block, carry):
        pass_copy(block, parity).wait_send()
        return carry

    lax.fori_loop(0, seq, sent_fwd, 0)
    pltpu.make_async_remote_copy(
        src_ref=pair_out,
        dst_ref=pair_in,
        send_sem=pair_send.at[0],
        recv_sem=pair_recv.at[0],
        device_id={"sp": seq, "tp": partner},
        device_id_type=MESH,
    ).wait_send()
    for hop in range(1, half_groups):
        cross_copy(pl.ds(0, cols), lax.rem(my_group + hop, half_groups), my_group, hop, 0).wait_send()


def shards(
    residual_in,
    query_small,
    query_large,
    key_small,
    key_large,
    value_small,
    value_large,
    forget_small,
    forget_large,
    project_small,
    project_large,
    norm_gain,
    expert_gate,
    expert_up,
    expert_down,
    routing,
    route_weight,
):
    n_sp, n_tp = lax.axis_size("sp"), lax.axis_size("tp")
    experts = n_sp * n_tp
    rows, width = residual_in.shape
    top_count = routing.shape[1]
    tokens = query_small.shape[0]
    size_small, size_large = key_small.shape[0], key_large.shape[0]
    heads_small, heads_large = forget_small.shape[0], forget_large.shape[0]
    heads = heads_small + heads_large
    gate_rows = -(-max(heads, 2 * top_count) // 8) * 8
    extra_rows = -(-3 * gate_rows // 16) * 16
    capacity = max(2, 2 * rows * top_count // experts)
    cap = -(-capacity // 16) * 16
    col_len = min(width, 512)
    cols = width // col_len
    hidden = expert_gate.shape[2]
    attn_width = heads_small * size_small + heads_large * size_large
    half_groups = n_tp // 2
    slots = experts * cap
    group = n_tp * cap
    lined = n_tp * capacity >= rows
    vmem, dma = pltpu.VMEM, pltpu.SemaphoreType.DMA
    inputs = (
        residual_in,
        query_small,
        query_large,
        key_small,
        key_large,
        value_small,
        value_large,
        forget_small,
        forget_large,
        norm_gain,
        routing.T,
        route_weight.T,
    )
    if lined:
        tail = [
            vmem((top_count * rows, slots), BF16),
            vmem((n_sp, group, rows), BF16),
            vmem((n_sp, cols, rows, col_len), BF16),
            vmem((n_sp, 16, -(-rows // 128) * 128), BF16),
            vmem((n_sp, cols, group, col_len), BF16),
            vmem((n_sp, cols, group, col_len), BF16),
            vmem((n_sp, group, 128), BF16),
            vmem((n_sp, group, 128), BF16),
            vmem((n_sp, group, width), BF16),
            vmem((slots, width), BF16),
            dma((2, n_sp, 2)),
            dma((n_sp, cols + 1)),
            dma((n_sp, 2)),
            dma((n_sp, 2)),
            dma((1,)),
            dma((1,)),
        ]
    else:
        tail = [
            vmem((top_count * rows, slots), BF16),
            vmem((cols, slots, col_len), BF16),
            vmem((cols, slots, col_len), BF16),
            vmem((slots, 128), BF16),
            vmem((slots, 128), BF16),
            vmem((slots, width), BF16),
            vmem((slots, width), BF16),
            dma((cols + 1, experts)),
            dma((cols + 1, experts)),
            dma((experts,)),
            dma((experts,)),
        ]
    return pl.pallas_call(
        functools.partial(layer_kernel, (n_sp, n_tp, cap, col_len, lined)),
        out_shape=jax.ShapeDtypeStruct((rows, width), BF16),
        in_specs=[pl.BlockSpec(memory_space=pl.ANY)] * 17,
        out_specs=pl.BlockSpec(memory_space=pltpu.VMEM),
        scratch_shapes=[vmem(given.shape, given.dtype) for given in inputs]
        + [
            vmem((n_sp, 2, size_small + size_large, tokens), BF16),
            vmem((n_sp, gate_rows, tokens + -(-rows // 128) * 128), F32),
            vmem((size_small + extra_rows, heads_small * tokens), BF16),
            vmem((size_large + extra_rows, heads_large * tokens), BF16),
            vmem((1, heads * tokens), F32),
            vmem((1, heads * tokens), F32),
            vmem((size_small, heads_small * tokens), F32),
            vmem((size_large, heads_large * tokens), F32),
            vmem((attn_width, tokens), BF16),
            vmem((tokens, attn_width), BF16),
            vmem((attn_width, width), BF16),
            vmem((width, hidden), BF16),
            vmem((width, hidden), BF16),
            vmem((hidden, width), BF16),
            vmem((cols, tokens, col_len), F32),
            vmem((cols, half_groups, rows, col_len), BF16),
            vmem((cols, half_groups, rows, col_len), BF16),
            vmem((cols, half_groups, rows, col_len), BF16),
            vmem((cols, half_groups, rows, col_len), BF16),
            vmem((rows, width), F32),
            dma((5,)),
            dma((12,)),
            dma((n_sp,)),
            dma((n_sp,)),
            dma((n_sp,)),
            dma((n_sp,)),
            dma((n_sp,)),
            dma((n_sp,)),
            dma((1,)),
            dma((cols,)),
            dma((half_groups,)),
            dma((cols, half_groups)),
        ]
        + tail,
        compiler_params=pltpu.CompilerParams(
            collective_id=0, has_side_effects=True, vmem_limit_bytes=60 * 1024 * 1024
        ),
    )(
        *inputs,
        project_small,
        project_large,
        expert_gate,
        expert_up,
        expert_down,
    )


def solution(mesh):
    in_specs = (
        P(("grp", "sp", "tp"), None),
        P(("grp", "sp"), "tp"),
        P(("grp", "sp"), "tp"),
        P(None, ("grp", "sp")),
        P(None, ("grp", "sp")),
        P(None, ("grp", "sp")),
        P(None, ("grp", "sp")),
        P("tp", ("grp", "sp")),
        P("tp", ("grp", "sp")),
        P("tp", None),
        P("tp", None),
        P(),
        P(("sp", "tp"), None, None),
        P(("sp", "tp"), None, None),
        P(("sp", "tp"), None, None),
        P(("grp", "sp", "tp"), None),
        P(("grp", "sp", "tp"), None),
    )
    out_specs = P(("grp", "sp", "tp"), None)
    return jax.shard_map(shards, mesh=mesh, in_specs=in_specs, out_specs=out_specs, check_vma=False)
```

```python
import functools
import math

import jax
import jax.numpy as jnp
from jax import lax
from jax.experimental import pallas as pl
from jax.experimental.pallas import tpu as pltpu
from jax.sharding import PartitionSpec as P

MESH = pl.DeviceIdType.MESH
F32 = jnp.float32
BF16 = jnp.bfloat16


def layer_kernel(dims, *refs):
    given, refs = refs[:12], refs[12:]
    (
        project_small,
        project_large,
        expert_gate,
        expert_up,
        expert_down,
        out,
        residual_in,
        query_small,
        query_large,
        key_small,
        key_large,
        value_small,
        value_large,
        forget_small,
        forget_large,
        norm_gain,
        routing,
        route_weight,
        kv,
        gates,
        turned_q_small,
        turned_q_large,
        top_ref,
        total_ref,
        acc_small,
        acc_large,
        attn_t,
        attn,
        proj_w,
        gate_w,
        up_w,
        down_w,
        proj_f32,
        pair_out,
        pair_in,
        cross_out,
        cross_in,
        resid_ref,
        weight_sem,
        given_sem,
        kv_send,
        kv_recv,
        gate_send,
        gate_recv,
        share_send,
        pass_recv,
        pair_send,
        pair_recv,
        cross_send,
        cross_recv,
        *tail,
    ) = refs
    n_sp, n_tp, cap, col_len, lined = dims
    held = (
        residual_in,
        query_small,
        query_large,
        key_small,
        key_large,
        value_small,
        value_large,
        forget_small,
        forget_large,
        norm_gain,
        routing,
        route_weight,
    )
    fetches = [
        pltpu.make_async_copy(source, target, given_sem.at[i])
        for i, (source, target) in enumerate(zip(given, held))
    ]
    early, queries, late = (3, 4, 5, 6, 7, 8, 10, 11), (1, 2), (0, 9)
    for i in early + queries + late:
        fetches[i].start()
    experts = n_sp * n_tp
    seq = lax.axis_index("sp")
    ten = lax.axis_index("tp")
    me = seq * n_tp + ten
    parity = lax.rem(ten, 2)
    partner = ten + 1 - 2 * parity
    tokens = query_small.shape[0]
    size_small, size_large = key_small.shape[0], key_large.shape[0]
    heads_small, heads_large = forget_small.shape[0], forget_large.shape[0]
    width_small = heads_small * size_small
    rows, width = residual_in.shape
    piece_count = kv.shape[1]
    piece_small, piece_large = size_small // piece_count, size_large // piece_count
    cols = width // col_len
    half_groups = n_tp // 2
    my_group = lax.div(ten, 2)

    loads = [
        pltpu.make_async_copy(project_small, proj_w.at[pl.ds(0, width_small)], weight_sem.at[0]),
        pltpu.make_async_copy(
            project_large,
            proj_w.at[pl.ds(width_small, heads_large * size_large)],
            weight_sem.at[1],
        ),
        pltpu.make_async_copy(expert_gate.at[0], gate_w, weight_sem.at[2]),
        pltpu.make_async_copy(expert_up.at[0], up_w, weight_sem.at[3]),
        pltpu.make_async_copy(expert_down.at[0], down_w, weight_sem.at[4]),
    ]
    barrier = pltpu.get_barrier_semaphore()

    def greet(peer_sp, peer_tp):
        pl.semaphore_signal(
            barrier, inc=1, device_id={"sp": peer_sp, "tp": peer_tp}, device_id_type=MESH
        )

    def greet_all(i, carry):
        peer = lax.rem(me + i, experts)
        greet(lax.div(peer, n_tp), lax.rem(peer, n_tp))
        return carry

    lax.fori_loop(1, experts, greet_all, 0)
    for i in early:
        fetches[i].wait()

    for p in range(piece_count):
        base = 0
        for source, piece in (
            (key_small, piece_small),
            (key_large, piece_large),
            (value_small, piece_small),
            (value_large, piece_large),
        ):
            kv[seq, p, base : base + piece, :] = source[p * piece : (p + 1) * piece, :]
            base += piece
    top_count = routing.shape[0]
    gate_rows = gates.shape[1]
    gates[seq] = jnp.zeros(gates.shape[1:], F32)
    gates[seq, :heads_small, :tokens] = forget_small[...]
    gates[seq, heads_small : heads_small + heads_large, :tokens] = forget_large[...]
    gates[seq, :top_count, tokens : tokens + rows] = routing[...].astype(F32)

    pl.semaphore_wait(barrier, experts - 1)

    def kv_copy(source, target, slot):
        return pltpu.make_async_remote_copy(
            src_ref=kv.at[source, parity],
            dst_ref=kv.at[source, parity],
            send_sem=kv_send.at[slot],
            recv_sem=kv_recv.at[source],
            device_id={"sp": target, "tp": ten},
            device_id_type=MESH,
        )

    def gate_copy(source, target, slot):
        return pltpu.make_async_remote_copy(
            src_ref=gates.at[source],
            dst_ref=gates.at[source],
            send_sem=gate_send.at[slot],
            recv_sem=gate_recv.at[source],
            device_id={"sp": target, "tp": ten},
            device_id_type=MESH,
        )

    def pass_copy(source, piece):
        return pltpu.make_async_remote_copy(
            src_ref=kv.at[source, piece],
            dst_ref=kv.at[source, piece],
            send_sem=share_send.at[source],
            recv_sem=pass_recv.at[source],
            device_id={"sp": seq, "tp": partner},
            device_id_type=MESH,
        )

    def for_mates(action):
        for i in range(1, n_tp):
            action(lax.rem(ten + i, n_tp))

    def send_kv(target, carry):
        kv_copy(seq, target, target).start()
        return carry

    def send_gates(target, carry):
        gate_copy(seq, target, target).start()
        return carry

    lax.fori_loop(seq + 1, n_sp, send_gates, 0)
    lax.fori_loop(seq + 1, jnp.minimum(seq + 2, n_sp), send_kv, 0)
    if lined:
        lax.fori_loop(0, seq, send_gates, 0)
    for load in loads:
        load.start()

    lanes = lax.broadcasted_iota(jnp.int32, (rows, experts), 1)
    same = lax.broadcasted_iota(jnp.int32, (rows, rows), 0) == lax.broadcasted_iota(
        jnp.int32, (rows, rows), 1
    )

    def column(ref, k):
        return jnp.sum(
            jnp.where(same, ref[k : k + 1, :].astype(F32), 0.0), axis=1, keepdims=True
        )

    def route_places(routes):
        hot = [(route == lanes.astype(F32)).astype(F32) for route in routes]
        named = sum(hot).astype(BF16)
        below = (
            lax.broadcasted_iota(jnp.int32, (rows, rows), 0)
            > lax.broadcasted_iota(jnp.int32, (rows, rows), 1)
        ).astype(F32)
        earlier = jnp.dot(below.astype(BF16), named, preferred_element_type=F32)
        return [
            route * cap + jnp.sum(earlier * one, axis=1, keepdims=True)
            for route, one in zip(routes, hot)
        ]

    if lined:
        (
            pick_ref,
            choose,
            lane_rows,
            lane_scale,
            outgoing,
            arrived,
            scale_out,
            scale_in,
            result,
            returned,
            lane_send,
            lane_recv,
            disp_send,
            disp_recv,
            back_send,
            back_recv,
        ) = tail
        plane_slots = n_tp * cap
        slot_lane = lax.broadcasted_iota(jnp.int32, (rows, plane_slots), 1)

        def prepare(z):
            known = gates[z][:, tokens : tokens + rows]
            spots = (slot_lane + seq * plane_slots).astype(F32)
            both = jnp.zeros((rows, plane_slots), F32)
            for place in route_places([column(known, k) for k in range(top_count)]):
                both = both + (spots == place).astype(F32)
            choose[z] = both.T.astype(BF16)

        prepare(seq)
    else:
        (
            pick_ref,
            outgoing,
            arrived,
            scale_out,
            scale_in,
            result,
            returned,
            disp_send,
            disp_recv,
            back_send,
            back_recv,
        ) = tail

    spots = lax.broadcasted_iota(jnp.int32, (rows, experts * cap), 1).astype(F32)
    places = route_places([column(routing, k) for k in range(top_count)])
    for k in range(top_count):
        pick_ref[k * rows : (k + 1) * rows, :] = (spots == places[k]).astype(F32).astype(BF16)

    extra_rows = turned_q_small.shape[0] - size_small

    def fold(size):
        power = 2.0 ** math.floor(math.log2(size**-0.5))
        return power, size**-0.5 / power

    for i in queries:
        fetches[i].wait()
    extra_row = lax.broadcasted_iota(jnp.int32, (extra_rows, tokens), 0)
    for kind in range(2):
        heads, size, offset, source, q_ref = (
            (heads_small, size_small, 0, query_small, turned_q_small),
            (heads_large, size_large, heads_small, query_large, turned_q_large),
        )[kind]
        turned = (source[...] * fold(size)[0]).astype(BF16).T
        for h in range(heads):
            chosen = (lax.rem(extra_row, gate_rows) == offset + h) & (extra_row < 3 * gate_rows)
            span = slice(h * tokens, (h + 1) * tokens)
            q_ref[:size, span] = turned[h * size : (h + 1) * size, :]
            q_ref[size:, span] = jnp.where(chosen, 1.0, 0.0).astype(BF16)
    key_base = (0, piece_small)
    value_base = (piece_small + piece_large, 2 * piece_small + piece_large)

    def attend(block, diagonal):
        block_gates = gates[block][:, :tokens]

        def seen(heads):
            shape = (tokens, heads * tokens)
            k_pos = lax.broadcasted_iota(jnp.int32, shape, 0)
            q_pos = lax.rem(lax.broadcasted_iota(jnp.int32, shape, 1), tokens)
            return q_pos >= k_pos

        for kind in range(2):
            heads, size, piece, offset, q_ref, acc = (
                (heads_small, size_small, piece_small, 0, turned_q_small, acc_small),
                (heads_large, size_large, piece_large, heads_small, turned_q_large, acc_large),
            )[kind]
            kb, vb = key_base[kind], value_base[kind]
            rest = fold(size)[1]
            shift = block_gates * (-1.0 / rest)
            first = shift.astype(BF16).astype(F32)
            second = (shift - first).astype(BF16).astype(F32)
            pieces = [first, second, shift - first - second]
            if extra_rows > 3 * gate_rows:
                pieces.append(jnp.zeros((extra_rows - 3 * gate_rows, tokens), F32))
            keys = jnp.concatenate(
                [kv[block, p, kb : kb + piece, :] for p in range(piece_count)]
                + [jnp.concatenate(pieces, axis=0).astype(BF16)],
                axis=0,
            ).T
            values = jnp.concatenate(
                [kv[block, p, vb : vb + piece, :] for p in range(piece_count)], axis=0
            )
            side = slice(offset * tokens, (offset + heads) * tokens)
            scores = jnp.dot(keys, q_ref[...], preferred_element_type=F32)
            if diagonal:
                scores = jnp.where(seen(heads), scores, -jnp.inf)
            block_top = jnp.max(scores, axis=0, keepdims=True)
            top = block_top if diagonal else jnp.maximum(top_ref[:, side], block_top)
            below_top = scores - top
            weights = jnp.exp(below_top if rest == 1.0 else below_top * rest)
            total = jnp.sum(weights, axis=0, keepdims=True)
            mixed = jnp.dot(values, weights.astype(BF16), preferred_element_type=F32)
            if not diagonal:
                factor = jnp.exp((top_ref[:, side] - top) * rest)
                total = total_ref[:, side] * factor + total
                mixed = acc[...] * factor + mixed
            top_ref[:, side] = top
            total_ref[:, side] = total
            acc[...] = mixed

    def share_out(block):
        kv_copy(block, seq, block).wait_recv()
        pass_copy(block, parity).start()

    attend(seq, True)
    lax.fori_loop(seq + 2, n_sp, send_kv, 0)

    def learn(distances):
        if lined:
            for i in distances:
                z = lax.rem(seq + n_sp - i, n_sp)
                gate_copy(z, seq, z).wait_recv()
                prepare(z)

    learn(range(1, n_sp))

    def at_earlier(block):
        @pl.when(block >= 0)
        def _():
            share_out(block)

    at_earlier(seq - 1)

    def earlier_block(i, carry):
        block = seq - i
        pass_copy(block, 1 - parity).wait_recv()
        if not lined:
            gate_copy(block, seq, block).wait_recv()
        attend(block, False)

        @pl.when(jnp.logical_and(i == 1, seq > 1))
        def _():
            share_out(seq - 2)

        at_earlier(block - 2)
        return carry

    lax.fori_loop(1, seq + 1, earlier_block, 0)

    for h in range(heads_small):
        span = slice(h * tokens, (h + 1) * tokens)
        attn_t[h * size_small : (h + 1) * size_small, :] = (
            acc_small[:, span] * (1.0 / total_ref[:, span])
        ).astype(BF16)
    for h in range(heads_large):
        first = width_small + h * size_large
        span = slice(h * tokens, (h + 1) * tokens)
        side = slice((heads_small + h) * tokens, (heads_small + h + 1) * tokens)
        attn_t[first : first + size_large, :] = (
            acc_large[:, span] * (1.0 / total_ref[:, side])
        ).astype(BF16)
    attn[...] = attn_t[...].T

    def row_ds(group, par):
        return pl.ds(pl.multiple_of((2 * group + par) * rows, rows), rows)

    def pair_copy(c):
        return pltpu.make_async_remote_copy(
            src_ref=pair_out.at[c],
            dst_ref=pair_in.at[c],
            send_sem=pair_send.at[0],
            recv_sem=pair_recv.at[c],
            device_id={"sp": seq, "tp": partner},
            device_id_type=MESH,
        )

    def cross_copy(c, group, source, slot, part=None):
        return pltpu.make_async_remote_copy(
            src_ref=cross_out.at[c, group],
            dst_ref=cross_in.at[c, source],
            send_sem=cross_send.at[slot],
            recv_sem=cross_recv.at[c if part is None else part, source],
            device_id={"sp": seq, "tp": 2 * group + parity},
            device_id_type=MESH,
        )

    for load in loads[:2]:
        load.wait()
    for i in late:
        fetches[i].wait()
    for c in range(cols):
        part = jnp.dot(
            attn[...], proj_w[:, c * col_len : (c + 1) * col_len], preferred_element_type=F32
        )
        proj_f32[c] = part
        for group in range(half_groups):
            pair_out[c, group] = proj_f32[c, row_ds(group, 1 - parity), :].astype(BF16)
        pair_copy(c).start()
    for c in range(cols):
        pair_copy(c).wait_recv()
        for hop in range(1, half_groups):
            group = lax.rem(my_group + hop, half_groups)
            cross_out[c, group] = (
                proj_f32[c, row_ds(group, parity), :] + pair_in[c, group].astype(F32)
            ).astype(BF16)
            cross_copy(c, group, my_group, hop).start()
    def own_rows(c, span, squares):
        value = proj_f32[c, row_ds(my_group, parity), :] + pair_in[c, my_group].astype(F32)
        for hop in range(1, half_groups):
            source = lax.rem(my_group + hop, half_groups)
            cross_copy(c, source, source, hop).wait_recv()
            value = value + cross_in[c, source].astype(F32)
        value = value + residual_in[:, span].astype(F32)
        resid_ref[:, span] = value
        squares = squares + jnp.sum(value * value, axis=1, keepdims=True)
        return value, squares

    def finish():
        for c in range(cols):
            span = slice(c * col_len, (c + 1) * col_len)
            picked = jnp.dot(pick_ref[...], returned[:, span], preferred_element_type=F32)
            value = resid_ref[:, span]
            for k in range(top_count):
                value = value + picked[k * rows : (k + 1) * rows] * column(route_weight, k)
            out[:, span] = value.astype(BF16)

    def scale_parts(squares):
        scale = lax.rsqrt(squares * (1.0 / width) + 1e-06)
        first = scale.astype(BF16).astype(F32)
        second = (scale - first).astype(BF16).astype(F32)
        third = scale - first - second
        lane = lax.broadcasted_iota(jnp.int32, (rows, 128), 1)
        parts = jnp.where(lane == 0, first, 0.0)
        parts = jnp.where(lane == 1, second, parts)
        return jnp.where(lane == 2, third, parts).astype(BF16)

    if lined:

        def slot_ds(member):
            return pl.ds(pl.multiple_of(member * cap, cap), cap)

        def lane_copy(z, c, up):
            ref = lane_rows.at[z, c] if c < cols else lane_scale.at[z]
            return pltpu.make_async_remote_copy(
                src_ref=ref,
                dst_ref=ref,
                send_sem=lane_send.at[up, z, 1 if c == cols else 0],
                recv_sem=lane_recv.at[z, c],
                device_id={"sp": seq + 2 * up - 1, "tp": ten},
                device_id_type=MESH,
            )

        scale_out[...] = jnp.zeros(scale_out.shape, BF16)

        def disp_copy(z, c, peer, sender):
            source, target = (
                (outgoing.at[z, c], arrived.at[z, c])
                if c < cols
                else (scale_out.at[z], scale_in.at[z])
            )
            return pltpu.make_async_remote_copy(
                src_ref=source.at[slot_ds(peer)],
                dst_ref=target.at[slot_ds(sender)],
                send_sem=disp_send.at[z, 1 if c == cols else 0],
                recv_sem=disp_recv.at[z, 1 if c == cols else 0],
                device_id={"sp": seq, "tp": peer},
                device_id_type=MESH,
            )

        def back_copy(z, peer):
            return pltpu.make_async_remote_copy(
                src_ref=result.at[z, slot_ds(peer)],
                dst_ref=returned.at[slot_ds(me)],
                send_sem=back_send.at[0],
                recv_sem=back_recv.at[0],
                device_id={"sp": z, "tp": peer},
                device_id_type=MESH,
            )

        mates_rows = pl.ds(0, (n_tp - 1) * cap)
        next_mate = lax.rem(ten + 1, n_tp)

        def bulk(source, target, send_sem, recv_sem):
            return pltpu.make_async_remote_copy(
                src_ref=source,
                dst_ref=target,
                send_sem=send_sem,
                recv_sem=recv_sem,
                device_id={"sp": seq, "tp": next_mate},
                device_id_type=MESH,
            )

        def disp_came(z):
            ref = arrived.at[z, :, mates_rows]
            bulk(ref, ref, disp_send.at[z, 0], disp_recv.at[z, 0]).wait_recv()
            ref = scale_in.at[z, mates_rows]
            bulk(ref, ref, disp_send.at[z, 1], disp_recv.at[z, 1]).wait_recv()

        def sent_plane(z):
            ref = outgoing.at[z, :, mates_rows]
            bulk(ref, ref, disp_send.at[z, 0], disp_recv.at[z, 0]).wait_send()
            ref = scale_out.at[z, mates_rows]
            bulk(ref, ref, disp_send.at[z, 1], disp_recv.at[z, 0]).wait_send()

        def sent_lane(z, up):
            @pl.when(seq + 1 < n_sp if up else seq > 0)
            def _():
                bulk(
                    lane_rows.at[z], lane_rows.at[z], lane_send.at[up, z, 0], lane_recv.at[z, 0]
                ).wait_send()
                bulk(
                    lane_scale.at[z], lane_scale.at[z], lane_send.at[up, z, 1], lane_recv.at[z, 0]
                ).wait_send()

        def go_on(z, c, up):
            if up:

                @pl.when(seq + 1 < n_sp)
                def _():
                    lane_copy(z, c, 1).start()
            else:

                @pl.when(seq > 0)
                def _():
                    lane_copy(z, c, 0).start()

        def place_rows(z, c):
            if c < cols:
                outgoing[z, c] = jnp.dot(
                    choose[z], lane_rows[z, c], preferred_element_type=F32
                ).astype(BF16)
            else:
                parts = lane_scale[z, :, :rows].astype(F32).T.astype(BF16)
                scale_out[z, :, : parts.shape[1]] = jnp.dot(
                    choose[z], parts, preferred_element_type=F32
                ).astype(BF16)
            for_mates(lambda peer: disp_copy(z, c, peer, ten).start())
            if c < cols:
                arrived[z, c, slot_ds(ten), :] = outgoing[z, c, slot_ds(ten), :]
            else:
                scale_in[z, slot_ds(ten), :] = scale_out[z, slot_ds(ten), :]

        def at_pair(k, action, own):
            low, high = seq - k - 1, seq + k
            if k > 0:

                @pl.when(high < n_sp)
                def _():
                    action(high, 0)
            elif own is not None:
                own()

            @pl.when(low >= 0)
            def _():
                action(low, 1)

        def take(k, c):
            def one(z, up):
                lane_copy(z, c, up).wait_recv()
                go_on(z, c, up)
                place_rows(z, c)

            low, high = seq - k - 1, seq + k

            @pl.when(low >= 0)
            def _():
                one(low, 1)

            if k > 0:

                @pl.when(high < n_sp)
                def _():
                    one(high, 0)

        def serve(*blocks):
            for z in blocks:
                disp_came(z)
            came = jnp.concatenate(
                [
                    jnp.concatenate([arrived[z, c] for c in range(cols)], axis=1)
                    for z in blocks
                ],
                axis=0,
            )
            gate_part = jnp.dot(came, gate_w[...], preferred_element_type=F32)
            up_part = jnp.dot(came, up_w[...], preferred_element_type=F32)
            row_scale = jnp.concatenate(
                [
                    jnp.sum(
                        scale_in[z, :, : lane_scale.shape[1]].astype(F32), axis=1, keepdims=True
                    )
                    for z in blocks
                ],
                axis=0,
            )
            gate_part, up_part = gate_part * row_scale, up_part * row_scale
            hidden = (gate_part / (1.0 + jnp.exp(-gate_part)) * up_part).astype(BF16)
            for c in range(cols):
                span = slice(c * col_len, (c + 1) * col_len)
                made = jnp.dot(hidden, down_w[:, span], preferred_element_type=F32).astype(BF16)
                for i, z in enumerate(blocks):
                    result[z, :, span] = made[i * plane_slots : (i + 1) * plane_slots]

        def give(z, up):
            for_mates(lambda peer: back_copy(z, peer).start())
            back_copy(z, ten).start()

        def give_own():
            for_mates(lambda peer: back_copy(seq, peer).start())
            returned[slot_ds(me), :] = result[seq, slot_ds(ten), :]

        def serve_pair(k):
            low, high = seq - k - 1, seq + k
            both = jnp.logical_and(low >= 0, high < n_sp)

            if 2 * k + 1 < n_sp:

                @pl.when(both)
                def _():
                    serve(high, low)

            @pl.when(jnp.logical_not(both))
            def _():
                @pl.when(jnp.logical_or(low >= 0, high < n_sp))
                def _():
                    serve(jnp.where(low >= 0, low, high))

        squares = jnp.zeros((rows, 1), F32)
        gain = norm_gain[...].astype(F32).reshape(1, width)
        for c in range(cols):
            span = slice(c * col_len, (c + 1) * col_len)
            value, squares = own_rows(c, span, squares)
            lane_rows[seq, c] = (value * gain[:, span]).astype(BF16)
            go_on(seq, c, 0)
            go_on(seq, c, 1)
            place_rows(seq, c)
        lane_scale[seq] = jnp.zeros(lane_scale.shape[1:], BF16)
        turned_scale = scale_parts(squares).astype(F32).T
        lane_scale[seq, :, :rows] = turned_scale[: lane_scale.shape[1]].astype(BF16)
        go_on(seq, cols, 0)
        go_on(seq, cols, 1)
        place_rows(seq, cols)
        for c in range(cols + 1):
            take(0, c)
        for load in loads[2:]:
            load.wait()

        def sent_own():
            sent_plane(seq)
            sent_lane(seq, 0)
            sent_lane(seq, 1)

        def sent_block(z, up):
            sent_plane(z)
            sent_lane(z, up)

        for step in range(1, n_sp + 2):
            moving = step < n_sp
            if moving:
                for c in range(cols + 1):
                    take(step, c)
            if step <= n_sp:
                serve_pair(step - 1)
                if step == n_sp:
                    give_own()
                if step > 1:

                    @pl.when(seq + step - 1 < n_sp)
                    def _():
                        give(seq + step - 1, 0)

            for earlier in range(1, min(step, n_sp) + 1):
                due = jnp.maximum(earlier, n_sp - 1 - seq) == step

                @pl.when(jnp.logical_and(due, seq >= earlier))
                def _():
                    give(seq - earlier, 1)

            if step > 1:
                at_pair(step - 2, sent_block, sent_own)

        others = pl.ds(0, (experts - 1) * cap)
        bulk(
            returned.at[others], returned.at[others], back_send.at[0], back_recv.at[0]
        ).wait_recv()
        finish()
        bulk(
            returned.at[others], returned.at[others], back_send.at[0], back_recv.at[0]
        ).wait_send()
    else:
        def slot_ds(peer):
            return pl.ds(pl.multiple_of(peer * cap, cap), cap)

        def exchange(source_ref, target_ref, send, recv, peer, sender):
            return pltpu.make_async_remote_copy(
                src_ref=source_ref.at[slot_ds(peer)],
                dst_ref=target_ref.at[slot_ds(sender)],
                send_sem=send.at[peer],
                recv_sem=recv.at[sender],
                device_id={"sp": lax.div(peer, n_tp), "tp": lax.rem(peer, n_tp)},
                device_id_type=MESH,
            )

        def part_copy(c, peer, sender):
            if c < cols:
                source_ref, target_ref = outgoing.at[c], arrived.at[c]
            else:
                source_ref, target_ref = scale_out, scale_in
            return exchange(source_ref, target_ref, disp_send.at[c], disp_recv.at[c], peer, sender)

        def for_members(plane, action):
            def one(j, carry):
                peer = plane * n_tp + lax.rem(ten + j, n_tp)

                @pl.when(peer != me)
                def _():
                    action(peer)

                return carry

            lax.fori_loop(0, n_tp, one, 0)

        slots = experts * cap
        block_rows = min(256, slots)

        def place_rows(values, c):
            for b in range(slots // block_rows):
                span = slice(b * block_rows, (b + 1) * block_rows)
                chosen = pick_ref[:rows, span]
                for k in range(1, top_count):
                    chosen = chosen + pick_ref[k * rows : (k + 1) * rows, span]
                placed = lax.dot_general(
                    chosen, values, (((0,), (0,)), ((), ())), preferred_element_type=F32
                ).astype(BF16)
                if c < cols:
                    outgoing[c, span, :] = placed
                else:
                    scale_out[span, :] = placed

            def dispatch(i, carry):
                for_members(
                    lax.rem(seq + n_sp - i, n_sp), lambda peer: part_copy(c, peer, me).start()
                )
                return carry

            lax.fori_loop(0, n_sp, dispatch, 0)

        squares = jnp.zeros((rows, 1), F32)
        gain = norm_gain[...].astype(F32).reshape(1, width)
        for c in range(cols):
            span = slice(c * col_len, (c + 1) * col_len)
            value, squares = own_rows(c, span, squares)
            place_rows((value * gain[:, span]).astype(BF16), c)
        place_rows(scale_parts(squares), cols)
        for c in range(cols):
            arrived[c, slot_ds(me), :] = outgoing[c, slot_ds(me), :]
        scale_in[slot_ds(me), :] = scale_out[slot_ds(me), :]
        for load in loads[2:]:
            load.wait()

        group_rows = n_tp * cap

        def serve(i, carry):
            plane = lax.rem(seq + i, n_sp)
            span = pl.ds(pl.multiple_of(plane * group_rows, group_rows), group_rows)
            gate_part = jnp.zeros((group_rows, gate_w.shape[1]), F32)
            up_part = jnp.zeros((group_rows, gate_w.shape[1]), F32)
            for c in range(cols):
                for_members(plane, lambda peer: part_copy(c, me, peer).wait_recv())
                came = arrived[c, span, :]
                depth = slice(c * col_len, (c + 1) * col_len)
                gate_part = gate_part + jnp.dot(came, gate_w[depth, :], preferred_element_type=F32)
                up_part = up_part + jnp.dot(came, up_w[depth, :], preferred_element_type=F32)
            for_members(plane, lambda peer: part_copy(cols, me, peer).wait_recv())
            row_scale = jnp.sum(scale_in[span, :].astype(F32), axis=1, keepdims=True)
            gate_part, up_part = gate_part * row_scale, up_part * row_scale
            hidden = (gate_part / (1.0 + jnp.exp(-gate_part)) * up_part).astype(BF16)
            result[span, :] = jnp.dot(hidden, down_w[...], preferred_element_type=F32).astype(BF16)
            for_members(
                plane,
                lambda peer: exchange(result, returned, back_send, back_recv, peer, me).start(),
            )
            return carry

        lax.fori_loop(0, n_sp, serve, 0)
        returned[slot_ds(me), :] = result[slot_ds(me), :]

        def collect(i, carry):
            peer = lax.rem(me + i, experts)
            exchange(result, returned, back_send, back_recv, me, peer).wait_recv()
            return carry

        lax.fori_loop(1, experts, collect, 0)
        finish()

        def sent_rows(i, carry):
            peer = lax.rem(me + i, experts)
            for c in range(cols + 1):
                part_copy(c, peer, me).wait_send()
            exchange(result, returned, back_send, back_recv, peer, me).wait_send()
            return carry

        lax.fori_loop(1, experts, sent_rows, 0)

    def sent_kv(target, carry):
        gate_copy(seq, target, target).wait_send()
        kv_copy(seq, target, target).wait_send()
        return carry

    lax.fori_loop(seq + 1, n_sp, sent_kv, 0)
    if lined:

        def sent_gates(target, carry):
            gate_copy(seq, target, target).wait_send()
            return carry

        lax.fori_loop(0, seq, sent_gates, 0)

    def sent_fwd(block, carry):
        pass_copy(block, parity).wait_send()
        return carry

    lax.fori_loop(0, seq, sent_fwd, 0)
    pltpu.make_async_remote_copy(
        src_ref=pair_out,
        dst_ref=pair_in,
        send_sem=pair_send.at[0],
        recv_sem=pair_recv.at[0],
        device_id={"sp": seq, "tp": partner},
        device_id_type=MESH,
    ).wait_send()
    for hop in range(1, half_groups):
        cross_copy(pl.ds(0, cols), lax.rem(my_group + hop, half_groups), my_group, hop, 0).wait_send()


def shards(
    residual_in,
    query_small,
    query_large,
    key_small,
    key_large,
    value_small,
    value_large,
    forget_small,
    forget_large,
    project_small,
    project_large,
    norm_gain,
    expert_gate,
    expert_up,
    expert_down,
    routing,
    route_weight,
):
    n_sp, n_tp = lax.axis_size("sp"), lax.axis_size("tp")
    experts = n_sp * n_tp
    rows, width = residual_in.shape
    top_count = routing.shape[1]
    tokens = query_small.shape[0]
    size_small, size_large = key_small.shape[0], key_large.shape[0]
    heads_small, heads_large = forget_small.shape[0], forget_large.shape[0]
    heads = heads_small + heads_large
    gate_rows = -(-max(heads, 2 * top_count) // 8) * 8
    extra_rows = -(-3 * gate_rows // 16) * 16
    capacity = max(2, 2 * rows * top_count // experts)
    cap = -(-capacity // 16) * 16
    col_len = min(width, 512)
    cols = width // col_len
    hidden = expert_gate.shape[2]
    attn_width = heads_small * size_small + heads_large * size_large
    half_groups = n_tp // 2
    slots = experts * cap
    group = n_tp * cap
    lined = n_tp * capacity >= rows
    vmem, dma = pltpu.VMEM, pltpu.SemaphoreType.DMA
    inputs = (
        residual_in,
        query_small,
        query_large,
        key_small,
        key_large,
        value_small,
        value_large,
        forget_small,
        forget_large,
        norm_gain,
        routing.T,
        route_weight.T,
    )
    if lined:
        tail = [
            vmem((top_count * rows, slots), BF16),
            vmem((n_sp, group, rows), BF16),
            vmem((n_sp, cols, rows, col_len), BF16),
            vmem((n_sp, 16, -(-rows // 128) * 128), BF16),
            vmem((n_sp, cols, group, col_len), BF16),
            vmem((n_sp, cols, group, col_len), BF16),
            vmem((n_sp, group, 128), BF16),
            vmem((n_sp, group, 128), BF16),
            vmem((n_sp, group, width), BF16),
            vmem((slots, width), BF16),
            dma((2, n_sp, 2)),
            dma((n_sp, cols + 1)),
            dma((n_sp, 2)),
            dma((n_sp, 2)),
            dma((1,)),
            dma((1,)),
        ]
    else:
        tail = [
            vmem((top_count * rows, slots), BF16),
            vmem((cols, slots, col_len), BF16),
            vmem((cols, slots, col_len), BF16),
            vmem((slots, 128), BF16),
            vmem((slots, 128), BF16),
            vmem((slots, width), BF16),
            vmem((slots, width), BF16),
            dma((cols + 1, experts)),
            dma((cols + 1, experts)),
            dma((experts,)),
            dma((experts,)),
        ]
    return pl.pallas_call(
        functools.partial(layer_kernel, (n_sp, n_tp, cap, col_len, lined)),
        out_shape=pltpu.VMEM((rows, width), BF16),
        in_specs=[pl.BlockSpec(memory_space=pl.ANY)] * 17,
        out_specs=pl.BlockSpec(memory_space=pltpu.VMEM),
        scratch_shapes=[vmem(given.shape, given.dtype) for given in inputs]
        + [
            vmem((n_sp, 2, size_small + size_large, tokens), BF16),
            vmem((n_sp, gate_rows, tokens + -(-rows // 128) * 128), F32),
            vmem((size_small + extra_rows, heads_small * tokens), BF16),
            vmem((size_large + extra_rows, heads_large * tokens), BF16),
            vmem((1, heads * tokens), F32),
            vmem((1, heads * tokens), F32),
            vmem((size_small, heads_small * tokens), F32),
            vmem((size_large, heads_large * tokens), F32),
            vmem((attn_width, tokens), BF16),
            vmem((tokens, attn_width), BF16),
            vmem((attn_width, width), BF16),
            vmem((width, hidden), BF16),
            vmem((width, hidden), BF16),
            vmem((hidden, width), BF16),
            vmem((cols, tokens, col_len), F32),
            vmem((cols, half_groups, rows, col_len), BF16),
            vmem((cols, half_groups, rows, col_len), BF16),
            vmem((cols, half_groups, rows, col_len), BF16),
            vmem((cols, half_groups, rows, col_len), BF16),
            vmem((rows, width), F32),
            dma((5,)),
            dma((12,)),
            dma((n_sp,)),
            dma((n_sp,)),
            dma((n_sp,)),
            dma((n_sp,)),
            dma((n_sp,)),
            dma((n_sp,)),
            dma((1,)),
            dma((cols,)),
            dma((half_groups,)),
            dma((cols, half_groups)),
        ]
        + tail,
        compiler_params=pltpu.CompilerParams(
            collective_id=0, has_side_effects=True, vmem_limit_bytes=60 * 1024 * 1024
        ),
    )(
        *inputs,
        project_small,
        project_large,
        expert_gate,
        expert_up,
        expert_down,
    )


def solution(mesh):
    in_specs = (
        P(("grp", "sp", "tp"), None),
        P(("grp", "sp"), "tp"),
        P(("grp", "sp"), "tp"),
        P(None, ("grp", "sp")),
        P(None, ("grp", "sp")),
        P(None, ("grp", "sp")),
        P(None, ("grp", "sp")),
        P("tp", ("grp", "sp")),
        P("tp", ("grp", "sp")),
        P("tp", None),
        P("tp", None),
        P(),
        P(("sp", "tp"), None, None),
        P(("sp", "tp"), None, None),
        P(("sp", "tp"), None, None),
        P(("grp", "sp", "tp"), None),
        P(("grp", "sp", "tp"), None),
    )
    out_specs = P(("grp", "sp", "tp"), None)
    return jax.shard_map(shards, mesh=mesh, in_specs=in_specs, out_specs=out_specs, check_vma=False)
```

```python
import functools
import math

import jax
import jax.numpy as jnp
from jax import lax
from jax.experimental import pallas as pl
from jax.experimental.pallas import tpu as pltpu
from jax.sharding import PartitionSpec as P

MESH = pl.DeviceIdType.MESH
F32 = jnp.float32
BF16 = jnp.bfloat16


def layer_kernel(dims, *refs):
    given, refs = refs[:12], refs[12:]
    (
        project_small,
        project_large,
        expert_gate,
        expert_up,
        expert_down,
        out,
        residual_in,
        query_small,
        query_large,
        key_small,
        key_large,
        value_small,
        value_large,
        forget_small,
        forget_large,
        norm_gain,
        routing,
        route_weight,
        kv,
        gates,
        turned_q_small,
        turned_q_large,
        top_ref,
        total_ref,
        acc_small,
        acc_large,
        attn_t,
        attn,
        proj_w,
        gate_w,
        up_w,
        down_w,
        proj_f32,
        pair_out,
        pair_in,
        cross_out,
        cross_in,
        resid_ref,
        weight_sem,
        given_sem,
        kv_send,
        kv_recv,
        gate_send,
        gate_recv,
        share_send,
        pass_recv,
        pair_send,
        pair_recv,
        cross_send,
        cross_recv,
        *tail,
    ) = refs
    n_sp, n_tp, cap, col_len, lined = dims
    held = (
        residual_in,
        query_small,
        query_large,
        key_small,
        key_large,
        value_small,
        value_large,
        forget_small,
        forget_large,
        norm_gain,
        routing,
        route_weight,
    )
    fetches = [
        pltpu.make_async_copy(source, target, given_sem.at[i])
        for i, (source, target) in enumerate(zip(given, held))
    ]
    early, queries, late = (3, 4, 5, 6, 7, 8, 10, 11), (1, 2), (0, 9)
    for i in early + queries + late:
        fetches[i].start()
    experts = n_sp * n_tp
    seq = lax.axis_index("sp")
    ten = lax.axis_index("tp")
    me = seq * n_tp + ten
    parity = lax.rem(ten, 2)
    partner = ten + 1 - 2 * parity
    tokens = query_small.shape[0]
    size_small, size_large = key_small.shape[0], key_large.shape[0]
    heads_small, heads_large = forget_small.shape[0], forget_large.shape[0]
    width_small = heads_small * size_small
    rows, width = residual_in.shape
    piece_count = kv.shape[1]
    piece_small, piece_large = size_small // piece_count, size_large // piece_count
    cols = width // col_len
    half_groups = n_tp // 2
    my_group = lax.div(ten, 2)

    loads = [
        pltpu.make_async_copy(project_small, proj_w.at[pl.ds(0, width_small)], weight_sem.at[0]),
        pltpu.make_async_copy(
            project_large,
            proj_w.at[pl.ds(width_small, heads_large * size_large)],
            weight_sem.at[1],
        ),
        pltpu.make_async_copy(expert_gate.at[0], gate_w, weight_sem.at[2]),
        pltpu.make_async_copy(expert_up.at[0], up_w, weight_sem.at[3]),
        pltpu.make_async_copy(expert_down.at[0], down_w, weight_sem.at[4]),
    ]
    barrier = pltpu.get_barrier_semaphore()

    def greet(peer_sp, peer_tp):
        pl.semaphore_signal(
            barrier, inc=1, device_id={"sp": peer_sp, "tp": peer_tp}, device_id_type=MESH
        )

    def greet_all(i, carry):
        peer = lax.rem(me + i, experts)
        greet(lax.div(peer, n_tp), lax.rem(peer, n_tp))
        return carry

    lax.fori_loop(1, experts, greet_all, 0)
    for i in early:
        fetches[i].wait()

    for p in range(piece_count):
        base = 0
        for source, piece in (
            (key_small, piece_small),
            (key_large, piece_large),
            (value_small, piece_small),
            (value_large, piece_large),
        ):
            kv[seq, p, base : base + piece, :] = source[p * piece : (p + 1) * piece, :]
            base += piece
    top_count = routing.shape[0]
    gate_rows = gates.shape[1]
    gates[seq] = jnp.zeros(gates.shape[1:], F32)
    gates[seq, :heads_small, :tokens] = forget_small[...]
    gates[seq, heads_small : heads_small + heads_large, :tokens] = forget_large[...]
    gates[seq, :top_count, tokens : tokens + rows] = routing[...].astype(F32)

    pl.semaphore_wait(barrier, experts - 1)

    def kv_copy(source, target, slot):
        return pltpu.make_async_remote_copy(
            src_ref=kv.at[source, parity],
            dst_ref=kv.at[source, parity],
            send_sem=kv_send.at[slot],
            recv_sem=kv_recv.at[source],
            device_id={"sp": target, "tp": ten},
            device_id_type=MESH,
        )

    def gate_copy(source, target, slot):
        return pltpu.make_async_remote_copy(
            src_ref=gates.at[source],
            dst_ref=gates.at[source],
            send_sem=gate_send.at[slot],
            recv_sem=gate_recv.at[source],
            device_id={"sp": target, "tp": ten},
            device_id_type=MESH,
        )

    def pass_copy(source, piece):
        return pltpu.make_async_remote_copy(
            src_ref=kv.at[source, piece],
            dst_ref=kv.at[source, piece],
            send_sem=share_send.at[source],
            recv_sem=pass_recv.at[source],
            device_id={"sp": seq, "tp": partner},
            device_id_type=MESH,
        )

    def for_mates(action):
        for i in range(1, n_tp):
            action(lax.rem(ten + i, n_tp))

    def send_kv(target, carry):
        kv_copy(seq, target, target).start()
        return carry

    def send_gates(target, carry):
        gate_copy(seq, target, target).start()
        return carry

    lax.fori_loop(seq + 1, n_sp, send_gates, 0)
    lax.fori_loop(seq + 1, jnp.minimum(seq + 2, n_sp), send_kv, 0)
    if lined:
        lax.fori_loop(0, seq, send_gates, 0)
    for load in loads:
        load.start()

    lanes = lax.broadcasted_iota(jnp.int32, (rows, experts), 1)
    same = lax.broadcasted_iota(jnp.int32, (rows, rows), 0) == lax.broadcasted_iota(
        jnp.int32, (rows, rows), 1
    )

    def column(ref, k):
        return jnp.sum(
            jnp.where(same, ref[k : k + 1, :].astype(F32), 0.0), axis=1, keepdims=True
        )

    def route_places(routes):
        hot = [(route == lanes.astype(F32)).astype(F32) for route in routes]
        named = sum(hot).astype(BF16)
        below = (
            lax.broadcasted_iota(jnp.int32, (rows, rows), 0)
            > lax.broadcasted_iota(jnp.int32, (rows, rows), 1)
        ).astype(F32)
        earlier = jnp.dot(below.astype(BF16), named, preferred_element_type=F32)
        return [
            route * cap + jnp.sum(earlier * one, axis=1, keepdims=True)
            for route, one in zip(routes, hot)
        ]

    if lined:
        (
            pick_ref,
            choose,
            lane_rows,
            lane_scale,
            outgoing,
            arrived,
            scale_out,
            scale_in,
            result,
            returned,
            lane_send,
            lane_recv,
            disp_send,
            disp_recv,
            back_send,
            back_recv,
        ) = tail
        plane_slots = n_tp * cap
        slot_lane = lax.broadcasted_iota(jnp.int32, (rows, plane_slots), 1)

        def prepare(z):
            known = gates[z][:, tokens : tokens + rows]
            spots = (slot_lane + seq * plane_slots).astype(F32)
            both = jnp.zeros((rows, plane_slots), F32)
            for place in route_places([column(known, k) for k in range(top_count)]):
                both = both + (spots == place).astype(F32)
            choose[z] = both.T.astype(BF16)

        prepare(seq)
    else:
        (
            pick_ref,
            outgoing,
            arrived,
            scale_out,
            scale_in,
            result,
            returned,
            disp_send,
            disp_recv,
            back_send,
            back_recv,
        ) = tail

    spots = lax.broadcasted_iota(jnp.int32, (rows, experts * cap), 1).astype(F32)
    places = route_places([column(routing, k) for k in range(top_count)])
    for k in range(top_count):
        pick_ref[k * rows : (k + 1) * rows, :] = (spots == places[k]).astype(F32).astype(BF16)

    extra_rows = turned_q_small.shape[0] - size_small

    def fold(size):
        power = 2.0 ** math.floor(math.log2(size**-0.5))
        return power, size**-0.5 / power

    for i in queries:
        fetches[i].wait()
    extra_row = lax.broadcasted_iota(jnp.int32, (extra_rows, tokens), 0)
    for kind in range(2):
        heads, size, offset, source, q_ref = (
            (heads_small, size_small, 0, query_small, turned_q_small),
            (heads_large, size_large, heads_small, query_large, turned_q_large),
        )[kind]
        turned = (source[...] * fold(size)[0]).astype(BF16).T
        for h in range(heads):
            chosen = (lax.rem(extra_row, gate_rows) == offset + h) & (extra_row < 3 * gate_rows)
            span = slice(h * tokens, (h + 1) * tokens)
            q_ref[:size, span] = turned[h * size : (h + 1) * size, :]
            q_ref[size:, span] = jnp.where(chosen, 1.0, 0.0).astype(BF16)
    key_base = (0, piece_small)
    value_base = (piece_small + piece_large, 2 * piece_small + piece_large)

    def attend(block, diagonal):
        block_gates = gates[block][:, :tokens]

        def seen(heads):
            shape = (tokens, heads * tokens)
            k_pos = lax.broadcasted_iota(jnp.int32, shape, 0)
            q_pos = lax.rem(lax.broadcasted_iota(jnp.int32, shape, 1), tokens)
            return q_pos >= k_pos

        for kind in range(2):
            heads, size, piece, offset, q_ref, acc = (
                (heads_small, size_small, piece_small, 0, turned_q_small, acc_small),
                (heads_large, size_large, piece_large, heads_small, turned_q_large, acc_large),
            )[kind]
            kb, vb = key_base[kind], value_base[kind]
            rest = fold(size)[1]
            shift = block_gates * (-1.0 / rest)
            first = shift.astype(BF16).astype(F32)
            second = (shift - first).astype(BF16).astype(F32)
            pieces = [first, second, shift - first - second]
            if extra_rows > 3 * gate_rows:
                pieces.append(jnp.zeros((extra_rows - 3 * gate_rows, tokens), F32))
            keys = jnp.concatenate(
                [kv[block, p, kb : kb + piece, :] for p in range(piece_count)]
                + [jnp.concatenate(pieces, axis=0).astype(BF16)],
                axis=0,
            ).T
            values = jnp.concatenate(
                [kv[block, p, vb : vb + piece, :] for p in range(piece_count)], axis=0
            )
            side = slice(offset * tokens, (offset + heads) * tokens)
            scores = jnp.dot(keys, q_ref[...], preferred_element_type=F32)
            if diagonal:
                scores = jnp.where(seen(heads), scores, -jnp.inf)
            block_top = jnp.max(scores, axis=0, keepdims=True)
            top = block_top if diagonal else jnp.maximum(top_ref[:, side], block_top)
            below_top = scores - top
            weights = jnp.exp(below_top if rest == 1.0 else below_top * rest)
            total = jnp.sum(weights, axis=0, keepdims=True)
            mixed = jnp.dot(values, weights.astype(BF16), preferred_element_type=F32)
            if not diagonal:
                factor = jnp.exp((top_ref[:, side] - top) * rest)
                total = total_ref[:, side] * factor + total
                mixed = acc[...] * factor + mixed
            top_ref[:, side] = top
            total_ref[:, side] = total
            acc[...] = mixed

    def share_out(block):
        kv_copy(block, seq, block).wait_recv()
        pass_copy(block, parity).start()

    attend(seq, True)
    lax.fori_loop(seq + 2, n_sp, send_kv, 0)

    def learn(distances):
        if lined:
            for i in distances:
                z = lax.rem(seq + n_sp - i, n_sp)
                gate_copy(z, seq, z).wait_recv()
                prepare(z)

    learn(range(1, n_sp))

    def at_earlier(block):
        @pl.when(block >= 0)
        def _():
            share_out(block)

    at_earlier(seq - 1)

    def earlier_block(i, carry):
        block = seq - i
        pass_copy(block, 1 - parity).wait_recv()
        if not lined:
            gate_copy(block, seq, block).wait_recv()
        attend(block, False)

        @pl.when(jnp.logical_and(i == 1, seq > 1))
        def _():
            share_out(seq - 2)

        at_earlier(block - 2)
        return carry

    lax.fori_loop(1, seq + 1, earlier_block, 0)

    for h in range(heads_small):
        span = slice(h * tokens, (h + 1) * tokens)
        attn_t[h * size_small : (h + 1) * size_small, :] = (
            acc_small[:, span] * (1.0 / total_ref[:, span])
        ).astype(BF16)
    for h in range(heads_large):
        first = width_small + h * size_large
        span = slice(h * tokens, (h + 1) * tokens)
        side = slice((heads_small + h) * tokens, (heads_small + h + 1) * tokens)
        attn_t[first : first + size_large, :] = (
            acc_large[:, span] * (1.0 / total_ref[:, side])
        ).astype(BF16)
    attn[...] = attn_t[...].T

    def row_ds(group, par):
        return pl.ds(pl.multiple_of((2 * group + par) * rows, rows), rows)

    def pair_copy(c):
        return pltpu.make_async_remote_copy(
            src_ref=pair_out.at[c],
            dst_ref=pair_in.at[c],
            send_sem=pair_send.at[0],
            recv_sem=pair_recv.at[c],
            device_id={"sp": seq, "tp": partner},
            device_id_type=MESH,
        )

    def cross_copy(c, group, source, slot, part=None):
        return pltpu.make_async_remote_copy(
            src_ref=cross_out.at[c, group],
            dst_ref=cross_in.at[c, source],
            send_sem=cross_send.at[slot],
            recv_sem=cross_recv.at[c if part is None else part, source],
            device_id={"sp": seq, "tp": 2 * group + parity},
            device_id_type=MESH,
        )

    for load in loads[:2]:
        load.wait()
    for i in late:
        fetches[i].wait()
    for c in range(cols):
        part = jnp.dot(
            attn[...], proj_w[:, c * col_len : (c + 1) * col_len], preferred_element_type=F32
        )
        proj_f32[c] = part
        for group in range(half_groups):
            pair_out[c, group] = proj_f32[c, row_ds(group, 1 - parity), :].astype(BF16)
        pair_copy(c).start()
    for c in range(cols):
        pair_copy(c).wait_recv()
        for hop in range(1, half_groups):
            group = lax.rem(my_group + hop, half_groups)
            cross_out[c, group] = (
                proj_f32[c, row_ds(group, parity), :] + pair_in[c, group].astype(F32)
            ).astype(BF16)
            cross_copy(c, group, my_group, hop).start()
    def own_rows(c, span, squares):
        value = proj_f32[c, row_ds(my_group, parity), :] + pair_in[c, my_group].astype(F32)
        for hop in range(1, half_groups):
            source = lax.rem(my_group + hop, half_groups)
            cross_copy(c, source, source, hop).wait_recv()
            value = value + cross_in[c, source].astype(F32)
        value = value + residual_in[:, span].astype(F32)
        resid_ref[:, span] = value
        squares = squares + jnp.sum(value * value, axis=1, keepdims=True)
        return value, squares

    def finish():
        for c in range(cols):
            span = slice(c * col_len, (c + 1) * col_len)
            picked = jnp.dot(pick_ref[...], returned[:, span], preferred_element_type=F32)
            value = resid_ref[:, span]
            for k in range(top_count):
                value = value + picked[k * rows : (k + 1) * rows] * column(route_weight, k)
            out[:, span] = value.astype(BF16)

    def scale_parts(squares):
        scale = lax.rsqrt(squares * (1.0 / width) + 1e-06)
        first = scale.astype(BF16).astype(F32)
        second = (scale - first).astype(BF16).astype(F32)
        third = scale - first - second
        lane = lax.broadcasted_iota(jnp.int32, (rows, 128), 1)
        parts = jnp.where(lane == 0, first, 0.0)
        parts = jnp.where(lane == 1, second, parts)
        return jnp.where(lane == 2, third, parts).astype(BF16)

    if lined:

        def slot_ds(member):
            return pl.ds(pl.multiple_of(member * cap, cap), cap)

        def lane_copy(z, c, up):
            ref = lane_rows.at[z, c] if c < cols else lane_scale.at[z]
            return pltpu.make_async_remote_copy(
                src_ref=ref,
                dst_ref=ref,
                send_sem=lane_send.at[up, z, 1 if c == cols else 0],
                recv_sem=lane_recv.at[z, c],
                device_id={"sp": seq + 2 * up - 1, "tp": ten},
                device_id_type=MESH,
            )

        scale_out[...] = jnp.zeros(scale_out.shape, BF16)

        def disp_copy(z, c, peer, sender):
            source, target = (
                (outgoing.at[z, c], arrived.at[z, c])
                if c < cols
                else (scale_out.at[z], scale_in.at[z])
            )
            return pltpu.make_async_remote_copy(
                src_ref=source.at[slot_ds(peer)],
                dst_ref=target.at[slot_ds(sender)],
                send_sem=disp_send.at[z, 1 if c == cols else 0],
                recv_sem=disp_recv.at[z, 1 if c == cols else 0],
                device_id={"sp": seq, "tp": peer},
                device_id_type=MESH,
            )

        def back_copy(z, peer):
            return pltpu.make_async_remote_copy(
                src_ref=result.at[z, slot_ds(peer)],
                dst_ref=returned.at[slot_ds(me)],
                send_sem=back_send.at[0],
                recv_sem=back_recv.at[0],
                device_id={"sp": z, "tp": peer},
                device_id_type=MESH,
            )

        mates_rows = pl.ds(0, (n_tp - 1) * cap)
        next_mate = lax.rem(ten + 1, n_tp)

        def bulk(source, target, send_sem, recv_sem):
            return pltpu.make_async_remote_copy(
                src_ref=source,
                dst_ref=target,
                send_sem=send_sem,
                recv_sem=recv_sem,
                device_id={"sp": seq, "tp": next_mate},
                device_id_type=MESH,
            )

        def disp_came(z):
            ref = arrived.at[z, :, mates_rows]
            bulk(ref, ref, disp_send.at[z, 0], disp_recv.at[z, 0]).wait_recv()
            ref = scale_in.at[z, mates_rows]
            bulk(ref, ref, disp_send.at[z, 1], disp_recv.at[z, 1]).wait_recv()

        def sent_plane(z):
            ref = outgoing.at[z, :, mates_rows]
            bulk(ref, ref, disp_send.at[z, 0], disp_recv.at[z, 0]).wait_send()
            ref = scale_out.at[z, mates_rows]
            bulk(ref, ref, disp_send.at[z, 1], disp_recv.at[z, 0]).wait_send()

        def sent_lane(z, up):
            @pl.when(seq + 1 < n_sp if up else seq > 0)
            def _():
                bulk(
                    lane_rows.at[z], lane_rows.at[z], lane_send.at[up, z, 0], lane_recv.at[z, 0]
                ).wait_send()
                bulk(
                    lane_scale.at[z], lane_scale.at[z], lane_send.at[up, z, 1], lane_recv.at[z, 0]
                ).wait_send()

        def go_on(z, c, up):
            if up:

                @pl.when(seq + 1 < n_sp)
                def _():
                    lane_copy(z, c, 1).start()
            else:

                @pl.when(seq > 0)
                def _():
                    lane_copy(z, c, 0).start()

        def place_rows(z, c):
            if c < cols:
                outgoing[z, c] = jnp.dot(
                    choose[z], lane_rows[z, c], preferred_element_type=F32
                ).astype(BF16)
            else:
                parts = lane_scale[z, :, :rows].astype(F32).T.astype(BF16)
                scale_out[z, :, : parts.shape[1]] = jnp.dot(
                    choose[z], parts, preferred_element_type=F32
                ).astype(BF16)
            for_mates(lambda peer: disp_copy(z, c, peer, ten).start())
            if c < cols:
                arrived[z, c, slot_ds(ten), :] = outgoing[z, c, slot_ds(ten), :]
            else:
                scale_in[z, slot_ds(ten), :] = scale_out[z, slot_ds(ten), :]

        def at_pair(k, action, own):
            low, high = seq - k - 1, seq + k
            if k > 0:

                @pl.when(high < n_sp)
                def _():
                    action(high, 0)
            elif own is not None:
                own()

            @pl.when(low >= 0)
            def _():
                action(low, 1)

        def take(k, c):
            def one(z, up):
                lane_copy(z, c, up).wait_recv()
                go_on(z, c, up)
                place_rows(z, c)

            low, high = seq - k - 1, seq + k

            @pl.when(low >= 0)
            def _():
                one(low, 1)

            if k > 0:

                @pl.when(high < n_sp)
                def _():
                    one(high, 0)

        def serve(*blocks):
            for z in blocks:
                disp_came(z)
            came = jnp.concatenate(
                [
                    jnp.concatenate([arrived[z, c] for c in range(cols)], axis=1)
                    for z in blocks
                ],
                axis=0,
            )
            gate_part = jnp.dot(came, gate_w[...], preferred_element_type=F32)
            up_part = jnp.dot(came, up_w[...], preferred_element_type=F32)
            row_scale = jnp.concatenate(
                [
                    jnp.sum(
                        scale_in[z, :, : lane_scale.shape[1]].astype(F32), axis=1, keepdims=True
                    )
                    for z in blocks
                ],
                axis=0,
            )
            gate_part, up_part = gate_part * row_scale, up_part * row_scale
            hidden = (gate_part / (1.0 + jnp.exp(-gate_part)) * up_part).astype(BF16)
            for c in range(cols):
                span = slice(c * col_len, (c + 1) * col_len)
                made = jnp.dot(hidden, down_w[:, span], preferred_element_type=F32).astype(BF16)
                for i, z in enumerate(blocks):
                    result[z, :, span] = made[i * plane_slots : (i + 1) * plane_slots]

        def give(z, up):
            for_mates(lambda peer: back_copy(z, peer).start())
            back_copy(z, ten).start()

        def give_own():
            for_mates(lambda peer: back_copy(seq, peer).start())
            returned[slot_ds(me), :] = result[seq, slot_ds(ten), :]

        def serve_pair(k):
            low, high = seq - k - 1, seq + k
            both = jnp.logical_and(low >= 0, high < n_sp)

            if 2 * k + 1 < n_sp:

                @pl.when(both)
                def _():
                    serve(high, low)

            @pl.when(jnp.logical_not(both))
            def _():
                @pl.when(jnp.logical_or(low >= 0, high < n_sp))
                def _():
                    serve(jnp.where(low >= 0, low, high))

        squares = jnp.zeros((rows, 1), F32)
        gain = norm_gain[...].astype(F32).reshape(1, width)
        for c in range(cols):
            span = slice(c * col_len, (c + 1) * col_len)
            value, squares = own_rows(c, span, squares)
            lane_rows[seq, c] = (value * gain[:, span]).astype(BF16)
            go_on(seq, c, 0)
            go_on(seq, c, 1)
            place_rows(seq, c)
        lane_scale[seq] = jnp.zeros(lane_scale.shape[1:], BF16)
        turned_scale = scale_parts(squares).astype(F32).T
        lane_scale[seq, :, :rows] = turned_scale[: lane_scale.shape[1]].astype(BF16)
        go_on(seq, cols, 0)
        go_on(seq, cols, 1)
        place_rows(seq, cols)
        for c in range(cols + 1):
            take(0, c)
        for load in loads[2:]:
            load.wait()

        def sent_own():
            sent_plane(seq)
            sent_lane(seq, 0)
            sent_lane(seq, 1)

        def sent_block(z, up):
            sent_plane(z)
            sent_lane(z, up)

        at_end = seq == 0
        for step in range(1, n_sp + 2):
            moving = step < n_sp
            if step <= n_sp:

                @pl.when(at_end)
                def _():
                    serve_pair(step - 1)

            if moving:
                for c in range(cols + 1):
                    take(step, c)
            if step <= n_sp:

                @pl.when(jnp.logical_not(at_end))
                def _():
                    serve_pair(step - 1)

                if step == n_sp:
                    give_own()
                if step > 1:

                    @pl.when(seq + step - 1 < n_sp)
                    def _():
                        give(seq + step - 1, 0)

            for earlier in range(1, min(step, n_sp) + 1):
                due = jnp.maximum(earlier, n_sp - 1 - seq) == step

                @pl.when(jnp.logical_and(due, seq >= earlier))
                def _():
                    give(seq - earlier, 1)

            if step > 1:
                at_pair(step - 2, sent_block, sent_own)

        others = pl.ds(0, (experts - 1) * cap)
        bulk(
            returned.at[others], returned.at[others], back_send.at[0], back_recv.at[0]
        ).wait_recv()
        finish()
        bulk(
            returned.at[others], returned.at[others], back_send.at[0], back_recv.at[0]
        ).wait_send()
    else:
        def slot_ds(peer):
            return pl.ds(pl.multiple_of(peer * cap, cap), cap)

        def exchange(source_ref, target_ref, send, recv, peer, sender):
            return pltpu.make_async_remote_copy(
                src_ref=source_ref.at[slot_ds(peer)],
                dst_ref=target_ref.at[slot_ds(sender)],
                send_sem=send.at[peer],
                recv_sem=recv.at[sender],
                device_id={"sp": lax.div(peer, n_tp), "tp": lax.rem(peer, n_tp)},
                device_id_type=MESH,
            )

        def part_copy(c, peer, sender):
            if c < cols:
                source_ref, target_ref = outgoing.at[c], arrived.at[c]
            else:
                source_ref, target_ref = scale_out, scale_in
            return exchange(source_ref, target_ref, disp_send.at[c], disp_recv.at[c], peer, sender)

        def for_members(plane, action):
            def one(j, carry):
                peer = plane * n_tp + lax.rem(ten + j, n_tp)

                @pl.when(peer != me)
                def _():
                    action(peer)

                return carry

            lax.fori_loop(0, n_tp, one, 0)

        slots = experts * cap
        block_rows = min(256, slots)

        def place_rows(values, c):
            for b in range(slots // block_rows):
                span = slice(b * block_rows, (b + 1) * block_rows)
                chosen = pick_ref[:rows, span]
                for k in range(1, top_count):
                    chosen = chosen + pick_ref[k * rows : (k + 1) * rows, span]
                placed = lax.dot_general(
                    chosen, values, (((0,), (0,)), ((), ())), preferred_element_type=F32
                ).astype(BF16)
                if c < cols:
                    outgoing[c, span, :] = placed
                else:
                    scale_out[span, :] = placed

            def dispatch(i, carry):
                for_members(
                    lax.rem(seq + n_sp - i, n_sp), lambda peer: part_copy(c, peer, me).start()
                )
                return carry

            lax.fori_loop(0, n_sp, dispatch, 0)

        squares = jnp.zeros((rows, 1), F32)
        gain = norm_gain[...].astype(F32).reshape(1, width)
        for c in range(cols):
            span = slice(c * col_len, (c + 1) * col_len)
            value, squares = own_rows(c, span, squares)
            place_rows((value * gain[:, span]).astype(BF16), c)
        place_rows(scale_parts(squares), cols)
        for c in range(cols):
            arrived[c, slot_ds(me), :] = outgoing[c, slot_ds(me), :]
        scale_in[slot_ds(me), :] = scale_out[slot_ds(me), :]
        for load in loads[2:]:
            load.wait()

        group_rows = n_tp * cap

        def serve(i, carry):
            plane = lax.rem(seq + i, n_sp)
            span = pl.ds(pl.multiple_of(plane * group_rows, group_rows), group_rows)
            gate_part = jnp.zeros((group_rows, gate_w.shape[1]), F32)
            up_part = jnp.zeros((group_rows, gate_w.shape[1]), F32)
            for c in range(cols):
                for_members(plane, lambda peer: part_copy(c, me, peer).wait_recv())
                came = arrived[c, span, :]
                depth = slice(c * col_len, (c + 1) * col_len)
                gate_part = gate_part + jnp.dot(came, gate_w[depth, :], preferred_element_type=F32)
                up_part = up_part + jnp.dot(came, up_w[depth, :], preferred_element_type=F32)
            for_members(plane, lambda peer: part_copy(cols, me, peer).wait_recv())
            row_scale = jnp.sum(scale_in[span, :].astype(F32), axis=1, keepdims=True)
            gate_part, up_part = gate_part * row_scale, up_part * row_scale
            hidden = (gate_part / (1.0 + jnp.exp(-gate_part)) * up_part).astype(BF16)
            result[span, :] = jnp.dot(hidden, down_w[...], preferred_element_type=F32).astype(BF16)
            for_members(
                plane,
                lambda peer: exchange(result, returned, back_send, back_recv, peer, me).start(),
            )
            return carry

        lax.fori_loop(0, n_sp, serve, 0)
        returned[slot_ds(me), :] = result[slot_ds(me), :]

        def collect(i, carry):
            peer = lax.rem(me + i, experts)
            exchange(result, returned, back_send, back_recv, me, peer).wait_recv()
            return carry

        lax.fori_loop(1, experts, collect, 0)
        finish()

        def sent_rows(i, carry):
            peer = lax.rem(me + i, experts)
            for c in range(cols + 1):
                part_copy(c, peer, me).wait_send()
            exchange(result, returned, back_send, back_recv, peer, me).wait_send()
            return carry

        lax.fori_loop(1, experts, sent_rows, 0)

    def sent_kv(target, carry):
        gate_copy(seq, target, target).wait_send()
        kv_copy(seq, target, target).wait_send()
        return carry

    lax.fori_loop(seq + 1, n_sp, sent_kv, 0)
    if lined:

        def sent_gates(target, carry):
            gate_copy(seq, target, target).wait_send()
            return carry

        lax.fori_loop(0, seq, sent_gates, 0)

    def sent_fwd(block, carry):
        pass_copy(block, parity).wait_send()
        return carry

    lax.fori_loop(0, seq, sent_fwd, 0)
    pltpu.make_async_remote_copy(
        src_ref=pair_out,
        dst_ref=pair_in,
        send_sem=pair_send.at[0],
        recv_sem=pair_recv.at[0],
        device_id={"sp": seq, "tp": partner},
        device_id_type=MESH,
    ).wait_send()
    for hop in range(1, half_groups):
        cross_copy(pl.ds(0, cols), lax.rem(my_group + hop, half_groups), my_group, hop, 0).wait_send()


def shards(
    residual_in,
    query_small,
    query_large,
    key_small,
    key_large,
    value_small,
    value_large,
    forget_small,
    forget_large,
    project_small,
    project_large,
    norm_gain,
    expert_gate,
    expert_up,
    expert_down,
    routing,
    route_weight,
):
    n_sp, n_tp = lax.axis_size("sp"), lax.axis_size("tp")
    experts = n_sp * n_tp
    rows, width = residual_in.shape
    top_count = routing.shape[1]
    tokens = query_small.shape[0]
    size_small, size_large = key_small.shape[0], key_large.shape[0]
    heads_small, heads_large = forget_small.shape[0], forget_large.shape[0]
    heads = heads_small + heads_large
    gate_rows = -(-max(heads, 2 * top_count) // 8) * 8
    extra_rows = -(-3 * gate_rows // 16) * 16
    capacity = max(2, 2 * rows * top_count // experts)
    cap = -(-capacity // 16) * 16
    col_len = min(width, 512)
    cols = width // col_len
    hidden = expert_gate.shape[2]
    attn_width = heads_small * size_small + heads_large * size_large
    half_groups = n_tp // 2
    slots = experts * cap
    group = n_tp * cap
    lined = n_tp * capacity >= rows
    vmem, dma = pltpu.VMEM, pltpu.SemaphoreType.DMA
    inputs = (
        residual_in,
        query_small,
        query_large,
        key_small,
        key_large,
        value_small,
        value_large,
        forget_small,
        forget_large,
        norm_gain,
        routing.T,
        route_weight.T,
    )
    if lined:
        tail = [
            vmem((top_count * rows, slots), BF16),
            vmem((n_sp, group, rows), BF16),
            vmem((n_sp, cols, rows, col_len), BF16),
            vmem((n_sp, 16, -(-rows // 128) * 128), BF16),
            vmem((n_sp, cols, group, col_len), BF16),
            vmem((n_sp, cols, group, col_len), BF16),
            vmem((n_sp, group, 128), BF16),
            vmem((n_sp, group, 128), BF16),
            vmem((n_sp, group, width), BF16),
            vmem((slots, width), BF16),
            dma((2, n_sp, 2)),
            dma((n_sp, cols + 1)),
            dma((n_sp, 2)),
            dma((n_sp, 2)),
            dma((1,)),
            dma((1,)),
        ]
    else:
        tail = [
            vmem((top_count * rows, slots), BF16),
            vmem((cols, slots, col_len), BF16),
            vmem((cols, slots, col_len), BF16),
            vmem((slots, 128), BF16),
            vmem((slots, 128), BF16),
            vmem((slots, width), BF16),
            vmem((slots, width), BF16),
            dma((cols + 1, experts)),
            dma((cols + 1, experts)),
            dma((experts,)),
            dma((experts,)),
        ]
    return pl.pallas_call(
        functools.partial(layer_kernel, (n_sp, n_tp, cap, col_len, lined)),
        out_shape=pltpu.VMEM((rows, width), BF16),
        in_specs=[pl.BlockSpec(memory_space=pl.ANY)] * 17,
        out_specs=pl.BlockSpec(memory_space=pltpu.VMEM),
        scratch_shapes=[vmem(given.shape, given.dtype) for given in inputs]
        + [
            vmem((n_sp, 2, size_small + size_large, tokens), BF16),
            vmem((n_sp, gate_rows, tokens + -(-rows // 128) * 128), F32),
            vmem((size_small + extra_rows, heads_small * tokens), BF16),
            vmem((size_large + extra_rows, heads_large * tokens), BF16),
            vmem((1, heads * tokens), F32),
            vmem((1, heads * tokens), F32),
            vmem((size_small, heads_small * tokens), F32),
            vmem((size_large, heads_large * tokens), F32),
            vmem((attn_width, tokens), BF16),
            vmem((tokens, attn_width), BF16),
            vmem((attn_width, width), BF16),
            vmem((width, hidden), BF16),
            vmem((width, hidden), BF16),
            vmem((hidden, width), BF16),
            vmem((cols, tokens, col_len), F32),
            vmem((cols, half_groups, rows, col_len), BF16),
            vmem((cols, half_groups, rows, col_len), BF16),
            vmem((cols, half_groups, rows, col_len), BF16),
            vmem((cols, half_groups, rows, col_len), BF16),
            vmem((rows, width), F32),
            dma((5,)),
            dma((12,)),
            dma((n_sp,)),
            dma((n_sp,)),
            dma((n_sp,)),
            dma((n_sp,)),
            dma((n_sp,)),
            dma((n_sp,)),
            dma((1,)),
            dma((cols,)),
            dma((half_groups,)),
            dma((cols, half_groups)),
        ]
        + tail,
        compiler_params=pltpu.CompilerParams(
            collective_id=0, has_side_effects=True, vmem_limit_bytes=60 * 1024 * 1024
        ),
    )(
        *inputs,
        project_small,
        project_large,
        expert_gate,
        expert_up,
        expert_down,
    )


def solution(mesh):
    in_specs = (
        P(("grp", "sp", "tp"), None),
        P(("grp", "sp"), "tp"),
        P(("grp", "sp"), "tp"),
        P(None, ("grp", "sp")),
        P(None, ("grp", "sp")),
        P(None, ("grp", "sp")),
        P(None, ("grp", "sp")),
        P("tp", ("grp", "sp")),
        P("tp", ("grp", "sp")),
        P("tp", None),
        P("tp", None),
        P(),
        P(("sp", "tp"), None, None),
        P(("sp", "tp"), None, None),
        P(("sp", "tp"), None, None),
        P(("grp", "sp", "tp"), None),
        P(("grp", "sp", "tp"), None),
    )
    out_specs = P(("grp", "sp", "tp"), None)
    return jax.shard_map(shards, mesh=mesh, in_specs=in_specs, out_specs=out_specs, check_vma=False)
```
